128 devices in a mesh: rep: 4 (over x), fs: 2 (over core), tp: 16 (over z, y).
Axes of the slice: x: 4, y: 4, z: 4, core: 2. Of those that a mesh axis runs over, the one named last changes fastest.
Arguments:
- layer_input: bfloat16 [10240, 2048], P(('rep', 'fs'), 'tp'), may hold values from -6 to 6
- cotangent: bfloat16 [10240, 2048], P(('rep', 'fs'), 'tp'), may hold values from -8 to 8
- gate_pre: bfloat16 [10240, 3072], P('rep', 'fs'), may hold values from -8 to 8
- up_pre: bfloat16 [10240, 3072], P('rep', 'fs'), may hold values from -6 to 6
- gate_weight: bfloat16 [2048, 3072], P('tp', 'fs'), may hold values from -0.125 to 0.125
- up_weight: bfloat16 [2048, 3072], P('tp', 'fs'), may hold values from -0.125 to 0.125
- down_weight: bfloat16 [3072, 2048], P('fs', 'tp'), may hold values from -0.109375 to 0.109375
Outputs:
- input_grad: bfloat16 [10240, 2048], P(('rep', 'fs'), 'tp')
- gate_grad: float32 [2048, 3072], P('tp', 'fs')
- up_grad: float32 [2048, 3072], P('tp', 'fs')
- down_grad: float32 [3072, 2048], P('fs', 'tp')
- gate_rows_sq: float32 [2048], P('tp')
- up_rows_sq: float32 [2048], P('tp')
- down_rows_sq: float32 [3072], P('fs')
The draws below stay inside these ranges and needn't reach their ends.
All inputs are finite; a program needn't handle non-finite values.
Results may differ from the reference program's by a relative error of at most 0.019.
Values may be sent and summed in bfloat16 or wider, within the bound.
A program may use at most 128 MiB of HBM per device.

```python
import math
import jax
import jax.numpy as jnp
from jax import lax

D = 2048
FF = 3072
TOKENS = 10240
N_FS = 2


def with_spikes(values, own_key, source, target, blocks, factor):
    owner, partner = [(jnp.arange(values.shape[position]) // (values.shape[position] // blocks)).reshape([-1 if axis == position else 1 for axis in range(values.ndim)]) for position in (source, target)]
    chosen = jax.random.permutation(own_key, blocks)[partner]
    strong = (owner == chosen) | (owner == (partner + blocks // 2) % blocks)
    return jnp.where(strong, factor * values, values)


def steps_of(key, shape, pieces, smallest, top_value):
    loudness, own = 1.0, jax.random.fold_in(key, 6)
    for dim, blocks in pieces:
        heights = jnp.exp(jax.random.uniform(jax.random.fold_in(own, dim), (blocks,), jnp.float32, smallest / len(pieces), top_value / len(pieces)))
        loudness = loudness * jnp.repeat(heights, shape[dim] // blocks).reshape([-1 if axis == dim else 1 for axis in range(len(shape))])
    return loudness


def bell_draw(key, shape, deviation, most, shards=(), held_as=jnp.bfloat16):
    drawn = deviation * jax.random.normal(key, shape, jnp.float32)
    if shards:
        drawn = drawn * steps_of(key, shape, shards, -0.22, 0.18)
    return jnp.clip(drawn, -most, most).astype(held_as)


def heavy_noise(stream_key, extent, spread, limit, shards, heavy, kind=jnp.bfloat16):
    drawn = spread * jax.random.normal(stream_key, extent, jnp.float32)
    if shards:
        drawn = drawn * steps_of(stream_key, extent, shards, -0.22, 0.18)
    return jnp.clip(with_spikes(drawn, jax.random.fold_in(stream_key, 3), *heavy), -limit, limit).astype(kind)


def setup_inputs(seed: int = 0) -> dict:
    seeds = jax.random.split(jax.random.key(seed), 8)
    return {
        "layer_input": bell_draw(seeds[0], (TOKENS, D), 1.0, 6.0, ((0, 8), (1, 16))),
        "cotangent": heavy_noise(seeds[1], (TOKENS, D), 1.0, 8.0, ((0, 8), (1, 16)), (0, 1, 16, 2.0)),
        "gate_pre": bell_draw(seeds[2], (TOKENS, FF), 1.5, 8.0, ((0, 4), (1, 2))),
        "up_pre": bell_draw(seeds[3], (TOKENS, FF), 1.0, 6.0, ((0, 4), (1, 2))),
        "gate_weight": bell_draw(seeds[4], (D, FF), D ** -0.5, 0.125, ((0, 16), (1, 2))),
        "up_weight": bell_draw(seeds[5], (D, FF), D ** -0.5, 0.125, ((0, 16), (1, 2))),
        "down_weight": bell_draw(seeds[6], (FF, D), FF ** -0.5, 0.109375, ((0, 2), (1, 16))),
    }


def contract_rows(left_side, right_side):
    return lax.dot_general(left_side, right_side, (((0,), (0,)), ((), ())), preferred_element_type=jnp.float32)

def contract_cols(left_side, right_side):
    return lax.dot_general(left_side, right_side, (((1,), (1,)), ((), ())), preferred_element_type=jnp.float32)

def reference(layer_input, cotangent, gate_pre, up_pre, gate_weight, up_weight, down_weight):
    hidden_grad = contract_cols(cotangent, down_weight)
    gate_value = gate_pre.astype(jnp.float32)
    up_value = up_pre.astype(jnp.float32)
    sigmoid_gate = jax.nn.sigmoid(gate_value)
    activated = gate_value * sigmoid_gate
    hidden = (activated * up_value).astype(jnp.bfloat16)
    gate_delta = (hidden_grad * up_value * sigmoid_gate * (1.0 + gate_value * (1.0 - sigmoid_gate))).astype(jnp.bfloat16)
    up_delta = (hidden_grad * activated).astype(jnp.bfloat16)
    block = FF // N_FS
    input_sum = jnp.zeros((TOKENS, D), jnp.float32)
    for block_index in range(N_FS):
        first = block_index * block
        partial_sum = contract_cols(gate_delta[:, first:first + block], gate_weight[:, first:first + block])
        partial_sum = partial_sum + contract_cols(up_delta[:, first:first + block], up_weight[:, first:first + block])
        rounded = lax.optimization_barrier(partial_sum.astype(jnp.bfloat16))
        input_sum = input_sum + rounded.astype(jnp.float32)
    input_grad = input_sum.astype(jnp.bfloat16)
    grad_scale = 1.0 / math.sqrt(TOKENS)
    gate_grad = contract_rows(layer_input, gate_delta) * grad_scale
    up_grad = contract_rows(layer_input, up_delta) * grad_scale
    down_grad = contract_rows(hidden, cotangent) * grad_scale
    gate_rows_sq = lax.optimization_barrier(jnp.sum(gate_grad * gate_grad, axis=1))
    up_rows_sq = lax.optimization_barrier(jnp.sum(up_grad * up_grad, axis=1))
    down_rows_sq = lax.optimization_barrier(jnp.sum(down_grad * down_grad, axis=1))
    return (input_grad, gate_grad, up_grad, down_grad, gate_rows_sq, up_rows_sq, down_rows_sq)
```

```python
import math

import jax
import jax.numpy as jnp
from jax import lax
from jax.experimental import pallas as pl
from jax.experimental.pallas import tpu as pltpu
from jax.sharding import PartitionSpec as P

MESH = pl.DeviceIdType.MESH
BF = jnp.bfloat16
F32 = jnp.float32

TOK = 2560
HALF = 1280
FH = 1536
N = 256
CH = 256
NCH = FH // CH
NCOT = HALF // N
NPAY = NCOT + NCH
TM = 640
TP = 256


def body(
    x_hbm, cot_hbm, gate_hbm, up_hbm, gw_hbm, uw_hbm, dw_hbm,
    ig_out, gg_out, ug_out, dg_out, gsq_out, usq_out, dsq_out,
    allb, aa, cc, gbuf, ubuf, hid, xb, xt, dgt, ig, gw, uw,
    gacc, gs, rs, ag, ds, dr, dag, igs, igr, sqacc, sqs, sqr, dsqs, dsqr,
    send_sem, recv_sem, d2d_send, d2d_recv, loc_sem, tile_sem,
    rs_send, rs_recv, ag_send, ag_recv, q_send, q_recv, r_send, r_recv,
):
    rep = lax.axis_index("rep")
    fs = lax.axis_index("fs")
    tp = lax.axis_index("tp")
    z, y = tp // 4, tp % 4
    sib = 1 - fs
    scale = 1.0 / math.sqrt(TOK * 4)

    def blk(dz, dy):
        return ((z + dz) % 4) * 4 + (y + dy) % 4

    mine = pl.multiple_of(fs * HALF, HALF)
    theirs = pl.multiple_of(sib * HALF, HALF)

    own_cot = pltpu.make_async_copy(cot_hbm, allb.at[tp, pl.ds(mine, HALF)], loc_sem.at[0])
    own_dw = pltpu.make_async_copy(dw_hbm, allb.at[tp, pl.ds(TOK, FH)], loc_sem.at[1])
    own_x = pltpu.make_async_copy(x_hbm, xb.at[pl.ds(mine, HALF)], loc_sem.at[2])
    own_gw = pltpu.make_async_copy(gw_hbm, gw, loc_sem.at[3])
    own_uw = pltpu.make_async_copy(uw_hbm, uw, loc_sem.at[4])
    own_cot.start()
    own_x.start()
    own_dw.start()

    def tile_rows(i):
        return pl.multiple_of(((fs * 5 + i) % 10) * TP, TP)

    def loads(i):
        slot = i % 2
        r = tile_rows(i)
        return (
            pltpu.make_async_copy(gate_hbm.at[pl.ds(r, TP)], gbuf.at[slot], tile_sem.at[slot, 0]),
            pltpu.make_async_copy(up_hbm.at[pl.ds(r, TP)], ubuf.at[slot], tile_sem.at[slot, 1]),
        )

    for c in loads(0):
        c.start()
    for c in loads(1):
        c.start()
    own_gw.start()
    own_uw.start()

    barrier = pltpu.get_barrier_semaphore()
    for d in range(1, 16):
        pl.semaphore_signal(barrier, inc=1, device_id={"tp": (tp + d) % 16}, device_id_type=MESH)
    for d in range(1, 4):
        pl.semaphore_signal(barrier, inc=1, device_id={"rep": (rep + d) % 4}, device_id_type=MESH)
    pl.semaphore_signal(barrier, inc=1, device_id={"fs": sib}, device_id_type=MESH)
    pl.semaphore_wait(barrier, 19)

    def row0(p):
        w = (p + 11) // 16
        return 256 * p + HALF * (w + fs * (1 - w))

    def put(p, b, off, n, dz, dy, g):
        rows = pl.ds(pl.multiple_of(row0(p) + off, 64), n)
        ref = allb.at[b, rows]
        pltpu.make_async_remote_copy(
            src_ref=ref,
            dst_ref=ref,
            send_sem=send_sem.at[p],
            recv_sem=recv_sem.at[p, g],
            device_id={"tp": blk(dz, dy)},
            device_id_type=MESH,
        ).start()

    def take(sem, k):
        ref = allb.at[pl.ds(0, k), pl.ds(0, N)]
        pltpu.make_async_copy(ref, ref, sem).wait()

    H, Q = N // 2, N // 4
    OA, OB = 0, H

    def both_y(p, b, g):
        put(p, b, OA, H, 0, 1, g)
        put(p, b, OA, H, 0, -1, g)

    def both_z(p, b, g):
        put(p, b, OB, H, 1, 0, g)
        put(p, b, OB, H, -1, 0, g)

    def r0(p):
        put(p, tp, OA, H, 1, 0, 0)
        put(p, tp, OA, H, -1, 0, 0)
        put(p, tp, OB, H, 0, 1, 0)
        put(p, tp, OB, H, 0, -1, 0)
        both_y(p, tp, 2)
        both_z(p, tp, 2)

    def r1(p):
        take(recv_sem.at[p, 0], 2)
        put(p, blk(-1, 0), OA, Q, 1, 0, 1)
        put(p, blk(1, 0), OA + Q, Q, -1, 0, 1)
        put(p, blk(0, -1), OB, Q, 0, 1, 1)
        put(p, blk(0, 1), OB + Q, Q, 0, -1, 1)
        for d in (-1, 1):
            both_y(p, blk(d, 0), 2)
            both_z(p, blk(0, d), 2)

    def r2(p):
        take(recv_sem.at[p, 1], 1)
        both_y(p, blk(2, 0), 3)
        both_z(p, blk(0, 2), 3)

    def onward(p, d, g):
        put(p, blk(d, -1), OA, Q, 0, 1, g)
        put(p, blk(d, 1), OA + Q, Q, 0, -1, g)
        put(p, blk(-1, d), OB, Q, 1, 0, g)
        put(p, blk(1, d), OB + Q, Q, -1, 0, g)

    def r3(p):
        take(recv_sem.at[p, 2], 6)
        for d in (0, -1, 1):
            onward(p, d, 4)

    def r4(p):
        take(recv_sem.at[p, 3], 2)
        onward(p, 2, 5)

    def r5(p):
        take(recv_sem.at[p, 4], 3)
        take(recv_sem.at[p, 5], 1)

    def to_sibling(p):
        rows = pl.ds(pl.multiple_of(fs * HALF + N * p, N), N)
        for d in range(1, 16):
            ref = allb.at[(tp + d) % 16, rows]
            pltpu.make_async_remote_copy(
                src_ref=ref,
                dst_ref=ref,
                send_sem=d2d_send.at[p],
                recv_sem=d2d_recv.at[p],
                device_id={"fs": sib},
                device_id_type=MESH,
            ).start()

    def d2d(src, dst, k):
        return pltpu.make_async_remote_copy(
            src_ref=src,
            dst_ref=dst,
            send_sem=r_send.at[k],
            recv_sem=r_recv.at[k],
            device_id={"fs": sib},
            device_id_type=MESH,
        )

    own_cot.wait()
    r0(0)
    cot_pair = d2d(allb.at[tp, pl.ds(mine, HALF)], allb.at[tp, pl.ds(mine, HALF)], 0)
    cot_pair.start()
    own_x.wait()
    x_pair = d2d(xb.at[pl.ds(mine, HALF)], xb.at[pl.ds(mine, HALF)], 1)
    x_pair.start()
    own_dw.wait()
    own_gw.wait()
    own_uw.wait()
    dgt[...] = jnp.zeros_like(dgt)
    ig[...] = jnp.zeros_like(ig)
    sqacc[...] = jnp.zeros_like(sqacc)
    cot_pair.wait_recv()
    x_pair.wait_recv()
    r1(0)

    def transpose_x(i, carry):
        r = pl.multiple_of(i * 128, 128)
        v = xb[pl.ds(r, 128), :].astype(F32)
        xt[i // 5, :, pl.ds(pl.multiple_of((i % 5) * 128, 128), 128)] = v.T.astype(BF)
        return carry

    lax.fori_loop(0, TOK // 128, transpose_x, 0)

    def tile(i):
        slot = i % 2
        r = tile_rows(i)
        for c in loads(i):
            c.wait()

        def sub(k, carry):
            q = pl.multiple_of(k * 32, 32)
            for j in range(NCH):
                g = gbuf[slot, pl.ds(q, 32), j * CH : (j + 1) * CH].astype(F32)
                u = ubuf[slot, pl.ds(q, 32), j * CH : (j + 1) * CH].astype(F32)
                s = 1.0 / (1.0 + jnp.exp(-g))
                a = g * s
                hid[pl.ds(q, 32), j * CH : (j + 1) * CH] = (a * u).astype(BF)
                aa[j, pl.ds(pl.multiple_of(r + q, 32), 32), :] = a.astype(BF)
                cc[j, pl.ds(pl.multiple_of(r + q, 32), 32), :] = (
                    u * s * (1.0 + g * (1.0 - s))
                ).astype(BF)
            return carry

        lax.fori_loop(0, TP // 32, sub, 0)

        @pl.when(i < 8)
        def _():
            for c in loads(i + 2):
                c.start()

        ct = allb[tp, pl.ds(r, TP), :].astype(F32).T.astype(BF)
        dgt[...] += jnp.dot(ct, hid[...], preferred_element_type=F32)

    def first(p, carry):
        r2(p)
        r0(p + 1)

        @pl.when(p >= 1)
        def _():
            r5(p - 1)
            to_sibling(p - 1)

        tile(2 * p)
        r3(p)
        r1(p + 1)
        tile(2 * p + 1)
        r4(p)
        return carry

    lax.fori_loop(0, NCOT, first, 0)

    def scatter(src, dst, s_sem, r_sem):
        for d in range(1, 4):
            peer = (rep + d) % 4
            pltpu.make_async_remote_copy(
                src_ref=src.at[peer],
                dst_ref=dst.at[rep],
                send_sem=s_sem,
                recv_sem=r_sem,
                device_id={"rep": peer},
                device_id_type=MESH,
            ).start()

    def spread(buf, s_sem, r_sem):
        for d in range(1, 4):
            pltpu.make_async_remote_copy(
                src_ref=buf.at[rep],
                dst_ref=buf.at[rep],
                send_sem=s_sem,
                recv_sem=r_sem,
                device_id={"rep": (rep + d) % 4},
                device_id_type=MESH,
            ).start()

    def three(buf, sem):
        ref = buf.at[pl.ds(0, 3)]
        pltpu.make_async_copy(ref, ref, sem).wait()

    p = NCOT
    r2(p)
    r0(p + 1)
    r5(p - 1)
    to_sibling(p - 1)
    for j in range(4):
        ds[j] = (dgt[32 * j : 32 * j + 32, :] * scale).astype(BF)
    dr[rep] = ds[rep]
    r3(p)
    scatter(ds, dr, rs_send.at[NCH], rs_recv.at[NCH])
    r1(p + 1)
    r4(p)
    for k in range(NCOT):
        take(d2d_recv.at[k], 15)

    def main_tile(c, j):
        t = (sib * 2 + j) % 4
        rows = pl.ds(pl.multiple_of(t * TM, TM), TM)
        fr = pl.ds(pl.multiple_of(TOK + c * CH, CH), CH)
        lhs = jnp.concatenate([allb[k, rows, :] for k in range(16)], axis=1)
        rhs = jnp.concatenate([allb[k, fr, :] for k in range(16)], axis=1)
        hg = lax.dot_general(lhs, rhs, (((1,), (1,)), ((), ())), preferred_element_type=F32)
        gd = (hg * cc[c, rows, :].astype(F32)).astype(BF)
        ud = (hg * aa[c, rows, :].astype(F32)).astype(BF)
        cols = pl.ds(pl.multiple_of(c * CH, CH), CH)
        both = jnp.concatenate([gd, ud], axis=1)
        wts = jnp.concatenate([gw[:, cols], uw[:, cols]], axis=1)
        ig[rows, :] += lax.dot_general(
            both, wts, (((1,), (1,)), ((), ())), preferred_element_type=F32
        )
        gu = jnp.dot(xt[t], both, preferred_element_type=F32)
        if j == 0:
            gacc[...] = gu
        else:
            gacc[...] += gu

    def send_grads(c):
        for j in range(4):
            gs[c, j, 0:32, :] = (gacc[32 * j : 32 * j + 32, 0:CH] * scale).astype(BF)
            gs[c, j, 32:64, :] = (gacc[32 * j : 32 * j + 32, CH : 2 * CH] * scale).astype(BF)
        rs[c, rep] = gs[c, rep]
        scatter(gs.at[c], rs.at[c], rs_send.at[c], rs_recv.at[c])

    def reduce_grads(c):
        three(rs.at[c], rs_recv.at[c])
        v = rs[c, 0].astype(F32) + rs[c, 1].astype(F32)
        v = v + rs[c, 2].astype(F32) + rs[c, 3].astype(F32)
        ag[c, rep] = v.astype(BF)
        spread(ag.at[c], ag_send.at[c], ag_recv.at[c])

    def finish_grads(c):
        three(ag.at[c], ag_recv.at[c])
        cols = pl.ds(pl.multiple_of(c * CH, CH), CH)
        for j in range(4):
            v = ag[c, j].astype(F32)
            gg_out[32 * j : 32 * j + 32, cols] = v[0:32]
            ug_out[32 * j : 32 * j + 32, cols] = v[32:64]
            w = v * v
            w = w[:, 0:128] + w[:, 128:256]
            sqacc[32 * j : 32 * j + 32, :] += w[0:32]
            sqacc[128 + 32 * j : 160 + 32 * j, :] += w[32:64]

    def reduce_down():
        three(dr, rs_recv.at[NCH])
        v = dr[0].astype(F32) + dr[1].astype(F32)
        v = v + dr[2].astype(F32) + dr[3].astype(F32)
        dag[rep] = v.astype(BF)
        spread(dag, ag_send.at[NCH], ag_recv.at[NCH])

    def finish_down():
        three(dag, ag_recv.at[NCH])
        for k in range(FH // 128):
            v = jnp.concatenate(
                [dag[j, :, 128 * k : 128 * k + 128].astype(F32) for j in range(4)], axis=0
            )
            dg_out[128 * k : 128 * k + 128, :] = v.T
            dsqs[:, 128 * k : 128 * k + 128] = jnp.sum(v * v, axis=0, keepdims=True)

    def send_down_sq():
        dsqr[tp] = dsqs[...]
        for d in range(1, 16):
            pltpu.make_async_remote_copy(
                src_ref=dsqs,
                dst_ref=dsqr.at[tp],
                send_sem=q_send,
                recv_sem=q_recv,
                device_id={"tp": (tp + d) % 16},
                device_id_type=MESH,
            ).start()

    ig_pair = d2d(igs, igr, 2)

    def chunk(c, carry):
        p = NCOT + 1 + c

        @pl.when(p < NPAY)
        def _():
            r2(p)

        @pl.when(p + 1 < NPAY)
        def _():
            r0(p + 1)

        r5(p - 1)
        main_tile(c, 0)

        @pl.when(p < NPAY)
        def _():
            r3(p)

        @pl.when(c == 0)
        def _():
            reduce_down()

        main_tile(c, 1)

        @pl.when(p + 1 < NPAY)
        def _():
            r1(p + 1)

        @pl.when(c >= 1)
        def _():
            reduce_grads(c - 1)

        @pl.when(c == NCH - 1)
        def _():
            igs[...] = ig[pl.ds(theirs, HALF), :].astype(BF)

        main_tile(c, 2)

        @pl.when(c == NCH - 1)
        def _():
            ig_pair.start()

        @pl.when(p < NPAY)
        def _():
            r4(p)

        @pl.when(c >= 2)
        def _():
            finish_grads(c - 2)

        @pl.when(c == 1)
        def _():
            finish_down()

        main_tile(c, 3)

        @pl.when(c == 1)
        def _():
            send_down_sq()

        send_grads(c)
        return carry

    lax.fori_loop(0, NCH, chunk, 0)

    finish_grads(NCH - 2)
    ig_pair.wait_recv()
    mine_part = ig[pl.ds(mine, HALF), :].astype(BF).astype(F32)
    ig_out[...] = (mine_part + igr[...].astype(F32)).astype(BF)
    reduce_grads(NCH - 1)
    all15 = dsqr.at[pl.ds(0, 15)]
    pltpu.make_async_copy(all15, all15, q_recv).wait()
    total = dsqr[0]
    for k in range(1, 16):
        total = total + dsqr[k]
    dsq_out[...] = total
    finish_grads(NCH - 1)
    sqs[...] = jnp.sum(sqacc[...].T, axis=0, keepdims=True)
    sq_pair = d2d(sqs, sqr, 3)
    sq_pair.start()

    for p in range(NPAY):
        take(send_sem.at[p], 15)
    for k in range(NCOT):
        take(d2d_send.at[k], 15)
    for k in range(NCH):
        three(gs.at[k], rs_send.at[k])
        three(ag.at[k], ag_send.at[k])
    three(ds, rs_send.at[NCH])
    three(dag, ag_send.at[NCH])
    pltpu.make_async_copy(all15, all15, q_send).wait()
    cot_pair.wait_send()
    x_pair.wait_send()
    ig_pair.wait_send()
    sq_pair.wait()
    both_sq = sqs[...] + sqr[...]
    gsq_out[...] = both_sq[:, 0:128]
    usq_out[...] = both_sq[:, 128:256]


def on_device(layer_input, cotangent, gate_pre, up_pre, gate_weight, up_weight, down_weight):
    anyspec = pl.BlockSpec(memory_space=pl.ANY)
    vm = pl.BlockSpec(memory_space=pltpu.VMEM)
    dma = pltpu.SemaphoreType.DMA
    outs = pl.pallas_call(
        body,
        out_shape=(
            jax.ShapeDtypeStruct((HALF, 128), BF),
            jax.ShapeDtypeStruct((128, FH), F32),
            jax.ShapeDtypeStruct((128, FH), F32),
            jax.ShapeDtypeStruct((FH, 128), F32),
            jax.ShapeDtypeStruct((1, 128), F32),
            jax.ShapeDtypeStruct((1, 128), F32),
            jax.ShapeDtypeStruct((1, FH), F32),
        ),
        in_specs=[anyspec] * 7,
        out_specs=(vm,) * 7,
        scratch_shapes=[
            pltpu.VMEM((16, TOK + FH, 128), BF),
            pltpu.VMEM((NCH, TOK, CH), BF),
            pltpu.VMEM((NCH, TOK, CH), BF),
            pltpu.VMEM((2, TP, FH), BF),
            pltpu.VMEM((2, TP, FH), BF),
            pltpu.VMEM((TP, FH), BF),
            pltpu.VMEM((TOK, 128), BF),
            pltpu.VMEM((4, 128, TM), BF),
            pltpu.VMEM((128, FH), F32),
            pltpu.VMEM((TOK, 128), F32),
            pltpu.VMEM((128, FH), BF),
            pltpu.VMEM((128, FH), BF),
            pltpu.VMEM((128, 2 * CH), F32),
            pltpu.VMEM((NCH, 4, 64, CH), BF),
            pltpu.VMEM((NCH, 4, 64, CH), BF),
            pltpu.VMEM((NCH, 4, 64, CH), BF),
            pltpu.VMEM((4, 32, FH), BF),
            pltpu.VMEM((4, 32, FH), BF),
            pltpu.VMEM((4, 32, FH), BF),
            pltpu.VMEM((HALF, 128), BF),
            pltpu.VMEM((HALF, 128), BF),
            pltpu.VMEM((256, 128), F32),
            pltpu.VMEM((1, 256), F32),
            pltpu.VMEM((1, 256), F32),
            pltpu.VMEM((1, FH), F32),
            pltpu.VMEM((16, 1, FH), F32),
            dma((NPAY,)),
            dma((NPAY, 6)),
            dma((NCOT,)),
            dma((NCOT,)),
            dma((5,)),
            dma((2, 2)),
            dma((NCH + 1,)),
            dma((NCH + 1,)),
            dma((NCH + 1,)),
            dma((NCH + 1,)),
            dma,
            dma,
            dma((4,)),
            dma((4,)),
        ],
        compiler_params=pltpu.CompilerParams(
            collective_id=0, has_side_effects=True, vmem_limit_bytes=64000000
        ),
        name="backward",
    )(layer_input, cotangent, gate_pre, up_pre, gate_weight, up_weight, down_weight)
    ig, gg, ug, dg, gsq, usq, dsq = outs
    return ig, gg, ug, dg, gsq.reshape(128), usq.reshape(128), dsq.reshape(FH)


def solution(mesh):
    return jax.shard_map(
        on_device,
        mesh=mesh,
        in_specs=(
            P(("rep", "fs"), "tp"),
            P(("rep", "fs"), "tp"),
            P("rep", "fs"),
            P("rep", "fs"),
            P("tp", "fs"),
            P("tp", "fs"),
            P("fs", "tp"),
        ),
        out_specs=(
            P(("rep", "fs"), "tp"),
            P("tp", "fs"),
            P("tp", "fs"),
            P("fs", "tp"),
            P("tp"),
            P("tp"),
            P("fs"),
        ),
        check_vma=False,
    )
```

```python
import math

import jax
import jax.numpy as jnp
from jax import lax
from jax.experimental import pallas as pl
from jax.experimental.pallas import tpu as pltpu
from jax.sharding import PartitionSpec as P

MESH = pl.DeviceIdType.MESH
BF = jnp.bfloat16
F32 = jnp.float32

TOK = 2560
HALF = 1280
FH = 1536
N = 256
CH = 256
NCH = FH // CH
NCOT = HALF // N
NPAY = NCOT + NCH
TM = 640
TP = 256


def body(
    x_hbm, cot_hbm, gate_hbm, up_hbm, gw_hbm, uw_hbm, dw_hbm,
    ig_out, ag, dag, sq_out, dsq_out,
    allb, aa, cc, gbuf, ubuf, hid, xb, xt, dgt, ig, gw, uw,
    gb, gacc, gs, rs, ds, dr, igs, igr, sqacc, sqs, sqr, dsqs, dsqr,
    send_sem, recv_sem, d2d_send, d2d_recv, loc_sem, tile_sem,
    rs_send, rs_recv, ag_send, ag_recv, q_send, q_recv, r_send, r_recv,
):
    rep = lax.axis_index("rep")
    fs = lax.axis_index("fs")
    tp = lax.axis_index("tp")
    z, y = tp // 4, tp % 4
    sib = 1 - fs
    scale = 1.0 / math.sqrt(TOK * 4)

    def blk(dz, dy):
        return ((z + dz) % 4) * 4 + (y + dy) % 4

    mine = pl.multiple_of(fs * HALF, HALF)
    theirs = pl.multiple_of(sib * HALF, HALF)

    own_cot = pltpu.make_async_copy(cot_hbm, allb.at[tp, pl.ds(mine, HALF)], loc_sem.at[0])
    own_dw = pltpu.make_async_copy(dw_hbm, allb.at[tp, pl.ds(TOK, FH)], loc_sem.at[1])
    own_x = pltpu.make_async_copy(x_hbm, xb.at[pl.ds(mine, HALF)], loc_sem.at[2])
    own_gw = pltpu.make_async_copy(gw_hbm, gw, loc_sem.at[3])
    own_uw = pltpu.make_async_copy(uw_hbm, uw, loc_sem.at[4])
    own_cot.start()
    own_x.start()
    own_dw.start()

    def tile_rows(i):
        return pl.multiple_of(((fs * 5 + i) % 10) * TP, TP)

    def loads(i):
        slot = i % 2
        r = tile_rows(i)
        return (
            pltpu.make_async_copy(gate_hbm.at[pl.ds(r, TP)], gbuf.at[slot], tile_sem.at[slot, 0]),
            pltpu.make_async_copy(up_hbm.at[pl.ds(r, TP)], ubuf.at[slot], tile_sem.at[slot, 1]),
        )

    for c in loads(0):
        c.start()
    for c in loads(1):
        c.start()
    own_gw.start()
    own_uw.start()

    barrier = pltpu.get_barrier_semaphore()
    for d in range(1, 16):
        pl.semaphore_signal(barrier, inc=1, device_id={"tp": (tp + d) % 16}, device_id_type=MESH)
    for d in range(1, 4):
        peer = (rep + d) % 4
        pl.semaphore_signal(barrier, inc=1, device_id={"rep": peer}, device_id_type=MESH)
        pl.semaphore_signal(barrier, inc=1, device_id={"rep": peer, "fs": sib}, device_id_type=MESH)
    pl.semaphore_signal(barrier, inc=1, device_id={"fs": sib}, device_id_type=MESH)
    pl.semaphore_wait(barrier, 22)

    def row0(p):
        w = (p + 11) // 16
        return 256 * p + HALF * (w + fs * (1 - w))

    def put(p, b, off, n, dz, dy, g):
        rows = pl.ds(pl.multiple_of(row0(p) + off, 64), n)
        ref = allb.at[b, rows]
        pltpu.make_async_remote_copy(
            src_ref=ref,
            dst_ref=ref,
            send_sem=send_sem.at[p],
            recv_sem=recv_sem.at[p, g],
            device_id={"tp": blk(dz, dy)},
            device_id_type=MESH,
        ).start()

    def take(sem, k):
        ref = allb.at[pl.ds(0, k), pl.ds(0, N)]
        pltpu.make_async_copy(ref, ref, sem).wait()

    H, Q = N // 2, N // 4
    OA, OB = 0, H

    def both_y(p, b, g):
        put(p, b, OA, H, 0, 1, g)
        put(p, b, OA, H, 0, -1, g)

    def both_z(p, b, g):
        put(p, b, OB, H, 1, 0, g)
        put(p, b, OB, H, -1, 0, g)

    def r0(p):
        put(p, tp, OA, H, 1, 0, 0)
        put(p, tp, OA, H, -1, 0, 0)
        put(p, tp, OB, H, 0, 1, 0)
        put(p, tp, OB, H, 0, -1, 0)
        both_y(p, tp, 2)
        both_z(p, tp, 2)

    def r1(p):
        take(recv_sem.at[p, 0], 2)
        put(p, blk(-1, 0), OA, Q, 1, 0, 1)
        put(p, blk(1, 0), OA + Q, Q, -1, 0, 1)
        put(p, blk(0, -1), OB, Q, 0, 1, 1)
        put(p, blk(0, 1), OB + Q, Q, 0, -1, 1)
        for d in (-1, 1):
            both_y(p, blk(d, 0), 2)
            both_z(p, blk(0, d), 2)

    def r2(p):
        take(recv_sem.at[p, 1], 1)
        both_y(p, blk(2, 0), 3)
        both_z(p, blk(0, 2), 3)

    def onward(p, d, g):
        put(p, blk(d, -1), OA, Q, 0, 1, g)
        put(p, blk(d, 1), OA + Q, Q, 0, -1, g)
        put(p, blk(-1, d), OB, Q, 1, 0, g)
        put(p, blk(1, d), OB + Q, Q, -1, 0, g)

    def r3(p):
        take(recv_sem.at[p, 2], 6)
        for d in (0, -1, 1):
            onward(p, d, 4)

    def r4(p):
        take(recv_sem.at[p, 3], 2)
        onward(p, 2, 5)

    def r5(p):
        take(recv_sem.at[p, 4], 3)
        take(recv_sem.at[p, 5], 1)

    def to_sibling(p):
        rows = pl.ds(pl.multiple_of(fs * HALF + N * p, N), N)
        for d in range(1, 16):
            ref = allb.at[(tp + d) % 16, rows]
            pltpu.make_async_remote_copy(
                src_ref=ref,
                dst_ref=ref,
                send_sem=d2d_send.at[p],
                recv_sem=d2d_recv.at[p],
                device_id={"fs": sib},
                device_id_type=MESH,
            ).start()

    def d2d(src, dst, k):
        return pltpu.make_async_remote_copy(
            src_ref=src,
            dst_ref=dst,
            send_sem=r_send.at[k],
            recv_sem=r_recv.at[k],
            device_id={"fs": sib},
            device_id_type=MESH,
        )

    own_cot.wait()
    r0(0)
    r0(1)
    cot_pair = d2d(allb.at[tp, pl.ds(mine, HALF)], allb.at[tp, pl.ds(mine, HALF)], 0)
    cot_pair.start()
    own_x.wait()
    x_pair = d2d(xb.at[pl.ds(mine, HALF)], xb.at[pl.ds(mine, HALF)], 1)
    x_pair.start()
    own_dw.wait()
    own_gw.wait()
    own_uw.wait()
    dgt[...] = jnp.zeros_like(dgt)
    ig[...] = jnp.zeros_like(ig)
    sqacc[...] = jnp.zeros_like(sqacc)
    r1(0)
    cot_pair.wait_recv()
    x_pair.wait_recv()

    def transpose_x(i, carry):
        r = pl.multiple_of(i * 128, 128)
        v = xb[pl.ds(r, 128), :].astype(F32)
        xt[:, pl.ds(r, 128)] = v.T.astype(BF)
        return carry

    lax.fori_loop(0, TOK // 128, transpose_x, 0)

    def tile(i):
        slot = i % 2
        r = tile_rows(i)
        for c in loads(i):
            c.wait()

        def sub(k, carry):
            q = pl.multiple_of(k * 32, 32)
            for j in range(NCH):
                g = gbuf[slot, pl.ds(q, 32), j * CH : (j + 1) * CH].astype(F32)
                u = ubuf[slot, pl.ds(q, 32), j * CH : (j + 1) * CH].astype(F32)
                s = 1.0 / (1.0 + jnp.exp(-g))
                a = g * s
                hid[pl.ds(q, 32), j * CH : (j + 1) * CH] = (a * u).astype(BF)
                aa[j, pl.ds(pl.multiple_of(r + q, 32), 32), :] = a.astype(BF)
                cc[j, pl.ds(pl.multiple_of(r + q, 32), 32), :] = (
                    u * s * (1.0 + g * (1.0 - s))
                ).astype(BF)
            return carry

        lax.fori_loop(0, TP // 32, sub, 0)

        @pl.when(i < 8)
        def _():
            for c in loads(i + 2):
                c.start()

        ct = allb[tp, pl.ds(r, TP), :].astype(F32).T.astype(BF)
        dgt[...] += jnp.dot(ct, hid[...], preferred_element_type=F32)

    def first(k, carry):
        r2(k)
        r1(k + 1)
        tile(2 * k)
        r3(k)

        @pl.when(k >= 1)
        def _():
            r4(k - 1)

        r0(k + 2)
        tile(2 * k + 1)

        @pl.when(k >= 2)
        def _():
            r5(k - 2)
            to_sibling(k - 2)

        return carry

    lax.fori_loop(0, NCOT, first, 0)

    def scatter(src, dst, s_sem, r_sem):
        for d in range(1, 4):
            peer = (rep + d) % 4
            pltpu.make_async_remote_copy(
                src_ref=src.at[peer],
                dst_ref=dst.at[rep],
                send_sem=s_sem,
                recv_sem=r_sem,
                device_id={"rep": peer},
                device_id_type=MESH,
            ).start()

    def spread(buf, s_sem, r_sem):
        for d in range(1, 4):
            pltpu.make_async_remote_copy(
                src_ref=buf.at[rep],
                dst_ref=buf.at[rep],
                send_sem=s_sem,
                recv_sem=r_sem,
                device_id={"rep": (rep + d) % 4},
                device_id_type=MESH,
            ).start()

    def three(buf, sem):
        ref = buf.at[pl.ds(0, 3)]
        pltpu.make_async_copy(ref, ref, sem).wait()

    for k in range(NCOT, NCOT + 2):
        r2(k)
        r1(k + 1)
        if k == NCOT:
            for j in range(4):
                ds[j] = (dgt[32 * j : 32 * j + 32, :] * scale).astype(BF)
            dr[rep] = ds[rep]
        r3(k)
        if k == NCOT:
            scatter(ds, dr, rs_send.at[NCH], rs_recv.at[NCH])
        r4(k - 1)
        r0(k + 2)
        r5(k - 2)
        to_sibling(k - 2)
    for k in range(NCOT):
        take(d2d_recv.at[k], 15)

    def main_tile(c, j):
        rows = pl.ds(j * TM, TM)
        fr = pl.ds(pl.multiple_of(TOK + c * CH, CH), CH)
        lhs = jnp.concatenate([allb[k, rows, :] for k in range(16)], axis=1)
        rhs = jnp.concatenate([allb[k, fr, :] for k in range(16)], axis=1)
        hg = lax.dot_general(lhs, rhs, (((1,), (1,)), ((), ())), preferred_element_type=F32)
        gd = (hg * cc[c, rows, :].astype(F32)).astype(BF)
        ud = (hg * aa[c, rows, :].astype(F32)).astype(BF)
        gb[rows, 0:CH] = gd
        gb[rows, CH : 2 * CH] = ud

    def main_grads():
        gacc[...] = jnp.dot(xt[...], gb[...], preferred_element_type=F32)

    def main_input(c):
        cols = pl.ds(pl.multiple_of(c * CH, CH), CH)
        wts = jnp.concatenate([gw[:, cols], uw[:, cols]], axis=1)
        ig[...] += lax.dot_general(
            gb[...], wts, (((1,), (1,)), ((), ())), preferred_element_type=F32
        )

    def send_grads(c):
        for j in range(4):
            gs[c, j, 0:32, :] = (gacc[32 * j : 32 * j + 32, 0:CH] * scale).astype(BF)
            gs[c, j, 32:64, :] = (gacc[32 * j : 32 * j + 32, CH : 2 * CH] * scale).astype(BF)
        rs[c, rep] = gs[c, rep]
        scatter(gs.at[c], rs.at[c], rs_send.at[c], rs_recv.at[c])

    def reduce_grads(c):
        three(rs.at[c], rs_recv.at[c])
        v = rs[c, 0].astype(F32) + rs[c, 1].astype(F32)
        v = v + rs[c, 2].astype(F32) + rs[c, 3].astype(F32)
        ag[c, rep] = v.astype(BF)
        spread(ag.at[c], ag_send.at[c], ag_recv.at[c])
        w = v * v
        w = w[:, 0:128] + w[:, 128:256]
        sqacc[pl.ds(pl.multiple_of(32 * rep, 32), 32), :] += w[0:32]
        sqacc[pl.ds(pl.multiple_of(128 + 32 * rep, 32), 32), :] += w[32:64]

    def reduce_down():
        three(dr, rs_recv.at[NCH])
        v = dr[0].astype(F32) + dr[1].astype(F32)
        v = v + dr[2].astype(F32) + dr[3].astype(F32)
        dag[rep] = v.astype(BF)
        spread(dag, ag_send.at[NCH], ag_recv.at[NCH])

    def finish_down():
        three(dag, ag_recv.at[NCH])
        for k in range(FH // 128):
            v = jnp.concatenate(
                [dag[j, :, 128 * k : 128 * k + 128].astype(F32) for j in range(4)], axis=0
            )
            dsqs[:, 128 * k : 128 * k + 128] = jnp.sum(v * v, axis=0, keepdims=True)

    def send_down_sq():
        dsqr[tp] = dsqs[...]
        for d in range(1, 16):
            pltpu.make_async_remote_copy(
                src_ref=dsqs,
                dst_ref=dsqr.at[tp],
                send_sem=q_send,
                recv_sem=q_recv,
                device_id={"tp": (tp + d) % 16},
                device_id_type=MESH,
            ).start()

    ig_pair = d2d(igs, igr, 2)

    def chunk(c, carry):
        k = NCOT + 2 + c

        @pl.when(k < NPAY)
        def _():
            r2(k)

        @pl.when(k + 1 < NPAY)
        def _():
            r1(k + 1)

        r5(k - 2)
        main_tile(c, 0)

        @pl.when(k < NPAY)
        def _():
            r3(k)

        @pl.when(c == 0)
        def _():
            reduce_down()

        main_tile(c, 1)

        @pl.when(k - 1 < NPAY)
        def _():
            r4(k - 1)

        @pl.when(c >= 1)
        def _():
            reduce_grads(c - 1)

        main_tile(c, 2)

        @pl.when(k + 2 < NPAY)
        def _():
            r0(k + 2)

        @pl.when(c == 1)
        def _():
            finish_down()

        main_tile(c, 3)

        @pl.when(c == 1)
        def _():
            send_down_sq()

        main_grads()
        send_grads(c)
        main_input(c)
        return carry

    lax.fori_loop(0, NCH, chunk, 0)

    igs[...] = ig[pl.ds(theirs, HALF), :].astype(BF)
    mine_part = ig[pl.ds(mine, HALF), :].astype(BF).astype(F32)
    ig[pl.ds(mine, HALF), :] = mine_part
    ig_pair.start()
    reduce_grads(NCH - 1)
    sqs[...] = jnp.sum(sqacc[...].T, axis=0, keepdims=True)
    sqr[rep * 2 + fs] = sqs[...]
    for d in range(1, 8):
        other = {"rep": (rep + d // 2) % 4, "fs": (fs + d) % 2}
        pltpu.make_async_remote_copy(
            src_ref=sqs,
            dst_ref=sqr.at[rep * 2 + fs],
            send_sem=r_send.at[3],
            recv_sem=r_recv.at[3],
            device_id=other,
            device_id_type=MESH,
        ).start()
    ig_pair.wait_recv()
    ig_out[...] = (ig[pl.ds(mine, HALF), :] + igr[...].astype(F32)).astype(BF)
    all15 = dsqr.at[pl.ds(0, 15)]
    pltpu.make_async_copy(all15, all15, q_recv).wait()
    total = dsqr[0]
    for k in range(1, 16):
        total = total + dsqr[k]
    dsq_out[...] = total

    for p in range(NPAY):
        take(send_sem.at[p], 15)
    for k in range(NCOT):
        take(d2d_send.at[k], 15)
    for k in range(NCH):
        three(gs.at[k], rs_send.at[k])
        three(ag.at[k], ag_send.at[k])
    three(ds, rs_send.at[NCH])
    three(dag, ag_send.at[NCH])
    pltpu.make_async_copy(all15, all15, q_send).wait()
    cot_pair.wait_send()
    x_pair.wait_send()
    ig_pair.wait_send()
    for k in range(NCH):
        three(ag.at[k], ag_recv.at[k])
    all7 = sqr.at[pl.ds(0, 7)]
    pltpu.make_async_copy(all7, all7, r_send.at[3]).wait()
    pltpu.make_async_copy(all7, all7, r_recv.at[3]).wait()
    total = sqr[0]
    for k in range(1, 8):
        total = total + sqr[k]
    sq_out[...] = total


def finish(ig, ag, dag, sq, dsq, ig_out, gg_out, ug_out, dg_out, gsq_out, usq_out, dsq_out):
    ig_out[...] = ig[...]
    for c in range(NCH):
        for j in range(4):
            v = ag[c, j].astype(F32)
            gg_out[32 * j : 32 * j + 32, c * CH : (c + 1) * CH] = v[0:32]
            ug_out[32 * j : 32 * j + 32, c * CH : (c + 1) * CH] = v[32:64]
    for k in range(FH // 128):
        v = jnp.concatenate(
            [dag[j, :, 128 * k : 128 * k + 128].astype(F32) for j in range(4)], axis=0
        )
        dg_out[128 * k : 128 * k + 128, :] = v.T
    gsq_out[...] = sq[0, 0:128]
    usq_out[...] = sq[0, 128:256]
    dsq_out[...] = dsq[0, :]


def on_device(layer_input, cotangent, gate_pre, up_pre, gate_weight, up_weight, down_weight):
    anyspec = pl.BlockSpec(memory_space=pl.ANY)
    vm = pl.BlockSpec(memory_space=pltpu.VMEM)
    dma = pltpu.SemaphoreType.DMA
    outs = pl.pallas_call(
        body,
        out_shape=(
            jax.ShapeDtypeStruct((HALF, 128), BF),
            jax.ShapeDtypeStruct((NCH, 4, 64, CH), BF),
            jax.ShapeDtypeStruct((4, 32, FH), BF),
            jax.ShapeDtypeStruct((1, 256), F32),
            jax.ShapeDtypeStruct((1, FH), F32),
        ),
        in_specs=[anyspec] * 7,
        out_specs=(vm,) * 5,
        scratch_shapes=[
            pltpu.VMEM((16, TOK + FH, 128), BF),
            pltpu.VMEM((NCH, TOK, CH), BF),
            pltpu.VMEM((NCH, TOK, CH), BF),
            pltpu.VMEM((2, TP, FH), BF),
            pltpu.VMEM((2, TP, FH), BF),
            pltpu.VMEM((TP, FH), BF),
            pltpu.VMEM((TOK, 128), BF),
            pltpu.VMEM((128, TOK), BF),
            pltpu.VMEM((128, FH), F32),
            pltpu.VMEM((TOK, 128), F32),
            pltpu.VMEM((128, FH), BF),
            pltpu.VMEM((128, FH), BF),
            pltpu.VMEM((TOK, 2 * CH), BF),
            pltpu.VMEM((128, 2 * CH), F32),
            pltpu.VMEM((NCH, 4, 64, CH), BF),
            pltpu.VMEM((NCH, 4, 64, CH), BF),
            pltpu.VMEM((4, 32, FH), BF),
            pltpu.VMEM((4, 32, FH), BF),
            pltpu.VMEM((HALF, 128), BF),
            pltpu.VMEM((HALF, 128), BF),
            pltpu.VMEM((256, 128), F32),
            pltpu.VMEM((1, 256), F32),
            pltpu.VMEM((8, 1, 256), F32),
            pltpu.VMEM((1, FH), F32),
            pltpu.VMEM((16, 1, FH), F32),
            dma((NPAY,)),
            dma((NPAY, 6)),
            dma((NCOT,)),
            dma((NCOT,)),
            dma((5,)),
            dma((2, 2)),
            dma((NCH + 1,)),
            dma((NCH + 1,)),
            dma((NCH + 1,)),
            dma((NCH + 1,)),
            dma,
            dma,
            dma((4,)),
            dma((4,)),
        ],
        compiler_params=pltpu.CompilerParams(
            collective_id=0, has_side_effects=True, vmem_limit_bytes=64000000
        ),
        name="backward",
    )(layer_input, cotangent, gate_pre, up_pre, gate_weight, up_weight, down_weight)
    return pl.pallas_call(
        finish,
        out_shape=(
            jax.ShapeDtypeStruct((HALF, 128), BF),
            jax.ShapeDtypeStruct((128, FH), F32),
            jax.ShapeDtypeStruct((128, FH), F32),
            jax.ShapeDtypeStruct((FH, 128), F32),
            jax.ShapeDtypeStruct((128,), F32),
            jax.ShapeDtypeStruct((128,), F32),
            jax.ShapeDtypeStruct((FH,), F32),
        ),
        in_specs=[vm] * 5,
        out_specs=(vm,) * 7,
        name="outputs",
    )(*outs)


def solution(mesh):
    return jax.shard_map(
        on_device,
        mesh=mesh,
        in_specs=(
            P(("rep", "fs"), "tp"),
            P(("rep", "fs"), "tp"),
            P("rep", "fs"),
            P("rep", "fs"),
            P("tp", "fs"),
            P("tp", "fs"),
            P("fs", "tp"),
        ),
        out_specs=(
            P(("rep", "fs"), "tp"),
            P("tp", "fs"),
            P("tp", "fs"),
            P("fs", "tp"),
            P("tp"),
            P("tp"),
            P("fs"),
        ),
        check_vma=False,
    )
```

```python
import math

import jax
import jax.numpy as jnp
from jax import lax
from jax.experimental import pallas as pl
from jax.experimental.pallas import tpu as pltpu
from jax.sharding import PartitionSpec as P

MESH = pl.DeviceIdType.MESH
BF = jnp.bfloat16
F32 = jnp.float32

TOK = 2560
HALF = 1280
FH = 1536
N = 256
CH = 256
NCH = FH // CH
NCOT = HALF // N
NPAY = NCOT + NCH
TM = 640
TP = 256


def body(
    x_hbm, cot_hbm, gate_hbm, up_hbm, gw_hbm, uw_hbm, dw_hbm,
    ig_out, ag, dag, sq_out, dsq_out,
    allb, aa, cc, gbuf, ubuf, hid, xb, xt, dgt, ig, gw, uw,
    gb, wt, gacc, gs, rs, ds, dr, igs, igr, sqacc, sqs, sqr, dsqs, dsqr,
    send_sem, recv_sem, d2d_send, d2d_recv, loc_sem, tile_sem,
    rs_send, rs_recv, ag_send, ag_recv, q_send, q_recv, r_send, r_recv,
):
    rep = lax.axis_index("rep")
    fs = lax.axis_index("fs")
    tp = lax.axis_index("tp")
    z, y = tp // 4, tp % 4
    sib = 1 - fs
    scale = 1.0 / math.sqrt(TOK * 4)

    def blk(dz, dy):
        return ((z + dz) % 4) * 4 + (y + dy) % 4

    mine = pl.multiple_of(fs * HALF, HALF)
    theirs = pl.multiple_of(sib * HALF, HALF)

    own_cot = pltpu.make_async_copy(cot_hbm, allb.at[tp, pl.ds(mine, HALF)], loc_sem.at[0])
    own_dw = pltpu.make_async_copy(dw_hbm, allb.at[tp, pl.ds(TOK, FH)], loc_sem.at[1])
    own_x = pltpu.make_async_copy(x_hbm, xb.at[pl.ds(mine, HALF)], loc_sem.at[2])
    own_gw = pltpu.make_async_copy(gw_hbm, gw, loc_sem.at[3])
    own_uw = pltpu.make_async_copy(uw_hbm, uw, loc_sem.at[4])
    own_cot.start()
    own_x.start()
    own_dw.start()

    def tile_rows(i):
        return pl.multiple_of(((fs * 5 + i) % 10) * TP, TP)

    def loads(i):
        slot = i % 2
        r = tile_rows(i)
        return (
            pltpu.make_async_copy(gate_hbm.at[pl.ds(r, TP)], gbuf.at[slot], tile_sem.at[slot, 0]),
            pltpu.make_async_copy(up_hbm.at[pl.ds(r, TP)], ubuf.at[slot], tile_sem.at[slot, 1]),
        )

    for c in loads(0):
        c.start()
    for c in loads(1):
        c.start()
    own_gw.start()
    own_uw.start()

    barrier = pltpu.get_barrier_semaphore()
    for d in range(1, 16):
        pl.semaphore_signal(barrier, inc=1, device_id={"tp": (tp + d) % 16}, device_id_type=MESH)
    for d in range(1, 4):
        peer = (rep + d) % 4
        pl.semaphore_signal(barrier, inc=1, device_id={"rep": peer}, device_id_type=MESH)
        pl.semaphore_signal(barrier, inc=1, device_id={"rep": peer, "fs": sib}, device_id_type=MESH)
    pl.semaphore_signal(barrier, inc=1, device_id={"fs": sib}, device_id_type=MESH)
    pl.semaphore_wait(barrier, 22)

    def row0(p):
        w = (p + 11) // 16
        return 256 * p + HALF * (w + fs * (1 - w))

    def put(p, b, off, n, dz, dy, g):
        rows = pl.ds(pl.multiple_of(row0(p) + off, 64), n)
        ref = allb.at[b, rows]
        pltpu.make_async_remote_copy(
            src_ref=ref,
            dst_ref=ref,
            send_sem=send_sem.at[p],
            recv_sem=recv_sem.at[p, g],
            device_id={"tp": blk(dz, dy)},
            device_id_type=MESH,
        ).start()

    def take(sem, k):
        ref = allb.at[pl.ds(0, k), pl.ds(0, N)]
        pltpu.make_async_copy(ref, ref, sem).wait()

    H, Q = N // 2, N // 4
    OA, OB = 0, H

    def both_y(p, b, g):
        put(p, b, OA, H, 0, 1, g)
        put(p, b, OA, H, 0, -1, g)

    def both_z(p, b, g):
        put(p, b, OB, H, 1, 0, g)
        put(p, b, OB, H, -1, 0, g)

    def r0(p):
        put(p, tp, OA, H, 1, 0, 0)
        put(p, tp, OA, H, -1, 0, 0)
        put(p, tp, OB, H, 0, 1, 0)
        put(p, tp, OB, H, 0, -1, 0)
        both_y(p, tp, 2)
        both_z(p, tp, 2)

    def r1(p):
        take(recv_sem.at[p, 0], 2)
        put(p, blk(-1, 0), OA, Q, 1, 0, 1)
        put(p, blk(1, 0), OA + Q, Q, -1, 0, 1)
        put(p, blk(0, -1), OB, Q, 0, 1, 1)
        put(p, blk(0, 1), OB + Q, Q, 0, -1, 1)
        for d in (-1, 1):
            both_y(p, blk(d, 0), 2)
            both_z(p, blk(0, d), 2)

    def r2(p):
        take(recv_sem.at[p, 1], 1)
        both_y(p, blk(2, 0), 3)
        both_z(p, blk(0, 2), 3)

    def onward(p, d, g):
        put(p, blk(d, -1), OA, Q, 0, 1, g)
        put(p, blk(d, 1), OA + Q, Q, 0, -1, g)
        put(p, blk(-1, d), OB, Q, 1, 0, g)
        put(p, blk(1, d), OB + Q, Q, -1, 0, g)

    def r3(p):
        take(recv_sem.at[p, 2], 6)
        for d in (0, -1, 1):
            onward(p, d, 4)

    def r4(p):
        take(recv_sem.at[p, 3], 2)
        onward(p, 2, 5)

    def r5(p):
        take(recv_sem.at[p, 4], 3)
        take(recv_sem.at[p, 5], 1)

    def to_sibling(p):
        rows = pl.ds(pl.multiple_of(fs * HALF + N * p, N), N)
        for d in range(1, 16):
            ref = allb.at[(tp + d) % 16, rows]
            pltpu.make_async_remote_copy(
                src_ref=ref,
                dst_ref=ref,
                send_sem=d2d_send.at[p],
                recv_sem=d2d_recv.at[p],
                device_id={"fs": sib},
                device_id_type=MESH,
            ).start()

    def d2d(src, dst, k):
        return pltpu.make_async_remote_copy(
            src_ref=src,
            dst_ref=dst,
            send_sem=r_send.at[k],
            recv_sem=r_recv.at[k],
            device_id={"fs": sib},
            device_id_type=MESH,
        )

    own_cot.wait()
    r0(0)
    r0(1)
    r0(2)
    cot_pair = d2d(allb.at[tp, pl.ds(mine, HALF)], allb.at[tp, pl.ds(mine, HALF)], 0)
    cot_pair.start()
    own_x.wait()
    x_pair = d2d(xb.at[pl.ds(mine, HALF)], xb.at[pl.ds(mine, HALF)], 1)
    x_pair.start()
    own_dw.wait()
    own_gw.wait()
    own_uw.wait()
    dgt[...] = jnp.zeros_like(dgt)
    ig[...] = jnp.zeros_like(ig)
    sqacc[...] = jnp.zeros_like(sqacc)
    r1(0)
    cot_pair.wait_recv()
    x_pair.wait_recv()

    def transpose_x(i, carry):
        r = pl.multiple_of(i * 128, 128)
        v = xb[pl.ds(r, 128), :].astype(F32)
        xt[:, pl.ds(r, 128)] = v.T.astype(BF)
        return carry

    lax.fori_loop(0, TOK // 128, transpose_x, 0)

    def tile(i):
        slot = i % 2
        r = tile_rows(i)
        for c in loads(i):
            c.wait()

        def sub(k, carry):
            q = pl.multiple_of(k * 32, 32)
            for j in range(NCH):
                g = gbuf[slot, pl.ds(q, 32), j * CH : (j + 1) * CH].astype(F32)
                u = ubuf[slot, pl.ds(q, 32), j * CH : (j + 1) * CH].astype(F32)
                s = 1.0 / (1.0 + jnp.exp(-g))
                a = g * s
                hid[pl.ds(q, 32), j * CH : (j + 1) * CH] = (a * u).astype(BF)
                aa[j, pl.ds(pl.multiple_of(r + q, 32), 32), :] = a.astype(BF)
                cc[j, pl.ds(pl.multiple_of(r + q, 32), 32), :] = (
                    u * s * (1.0 + g * (1.0 - s))
                ).astype(BF)
            return carry

        lax.fori_loop(0, TP // 32, sub, 0)

        @pl.when(i < 8)
        def _():
            for c in loads(i + 2):
                c.start()

        ct = allb[tp, pl.ds(r, TP), :].astype(F32).T.astype(BF)
        dgt[...] += jnp.dot(ct, hid[...], preferred_element_type=F32)

    def first(k, carry):
        r2(k)
        r1(k + 1)
        tile(2 * k)
        r3(k)

        @pl.when(k >= 1)
        def _():
            r4(k - 1)

        r0(k + 3)
        tile(2 * k + 1)

        @pl.when(k >= 2)
        def _():
            r5(k - 2)
            to_sibling(k - 2)

        return carry

    lax.fori_loop(0, NCOT, first, 0)

    def scatter(src, dst, s_sem, r_sem):
        for d in range(1, 4):
            peer = (rep + d) % 4
            pltpu.make_async_remote_copy(
                src_ref=src.at[peer],
                dst_ref=dst.at[rep],
                send_sem=s_sem,
                recv_sem=r_sem,
                device_id={"rep": peer},
                device_id_type=MESH,
            ).start()

    def spread(buf, s_sem, r_sem):
        for d in range(1, 4):
            pltpu.make_async_remote_copy(
                src_ref=buf.at[rep],
                dst_ref=buf.at[rep],
                send_sem=s_sem,
                recv_sem=r_sem,
                device_id={"rep": (rep + d) % 4},
                device_id_type=MESH,
            ).start()

    def three(buf, sem):
        ref = buf.at[pl.ds(0, 3)]
        pltpu.make_async_copy(ref, ref, sem).wait()

    for k in range(NCOT, NCOT + 2):
        r2(k)
        r1(k + 1)
        if k == NCOT:
            for j in range(4):
                ds[j] = (dgt[32 * j : 32 * j + 32, :] * scale).astype(BF)
            dr[rep] = ds[rep]
        r3(k)
        if k == NCOT:
            scatter(ds, dr, rs_send.at[NCH], rs_recv.at[NCH])
        r4(k - 1)
        r0(k + 3)
        r5(k - 2)
        to_sibling(k - 2)
    for k in range(NCOT):
        take(d2d_recv.at[k], 15)

    def main_weight(c):
        fr = pl.ds(pl.multiple_of(TOK + c * CH, CH), CH)
        for k in range(16):
            wt[128 * k : 128 * k + 128, :] = allb[k, fr, :].astype(F32).T.astype(BF)

    def main_tile(c, j):
        for i in range(2):
            rows = pl.ds(j * TM + i * (TM // 2), TM // 2)
            lhs = jnp.concatenate([allb[k, rows, :] for k in range(16)], axis=1)
            hg = jnp.dot(lhs, wt[...], preferred_element_type=F32)
            gb[rows, 0:CH] = (hg * cc[c, rows, :].astype(F32)).astype(BF)
            gb[rows, CH : 2 * CH] = (hg * aa[c, rows, :].astype(F32)).astype(BF)

    def main_grads():
        gacc[...] = jnp.dot(xt[...], gb[...], preferred_element_type=F32)

    def main_input(c):
        cols = pl.ds(pl.multiple_of(c * CH, CH), CH)
        wts = jnp.concatenate([gw[:, cols], uw[:, cols]], axis=1)
        ig[...] += lax.dot_general(
            gb[...], wts, (((1,), (1,)), ((), ())), preferred_element_type=F32
        )

    def send_grads(c):
        for j in range(4):
            gs[c, j, 0:32, :] = (gacc[32 * j : 32 * j + 32, 0:CH] * scale).astype(BF)
            gs[c, j, 32:64, :] = (gacc[32 * j : 32 * j + 32, CH : 2 * CH] * scale).astype(BF)
        rs[c, rep] = gs[c, rep]
        scatter(gs.at[c], rs.at[c], rs_send.at[c], rs_recv.at[c])

    def reduce_grads(c):
        three(rs.at[c], rs_recv.at[c])
        v = rs[c, 0].astype(F32) + rs[c, 1].astype(F32)
        v = v + rs[c, 2].astype(F32) + rs[c, 3].astype(F32)
        ag[c, rep] = v.astype(BF)
        w = v * v
        w = w[:, 0:128] + w[:, 128:256]
        sqacc[pl.ds(pl.multiple_of(32 * rep, 32), 32), :] += w[0:32]
        sqacc[pl.ds(pl.multiple_of(128 + 32 * rep, 32), 32), :] += w[32:64]
        spread(ag.at[c], ag_send.at[c], ag_recv.at[c])

    def reduce_down():
        three(dr, rs_recv.at[NCH])
        v = dr[0].astype(F32) + dr[1].astype(F32)
        v = v + dr[2].astype(F32) + dr[3].astype(F32)
        dag[rep] = v.astype(BF)
        spread(dag, ag_send.at[NCH], ag_recv.at[NCH])

    def finish_down():
        three(dag, ag_recv.at[NCH])
        for k in range(FH // 128):
            v = jnp.concatenate(
                [dag[j, :, 128 * k : 128 * k + 128].astype(F32) for j in range(4)], axis=0
            )
            dsqs[:, 128 * k : 128 * k + 128] = jnp.sum(v * v, axis=0, keepdims=True)

    def send_down_sq():
        dsqr[tp] = dsqs[...]
        for d in range(1, 16):
            pltpu.make_async_remote_copy(
                src_ref=dsqs,
                dst_ref=dsqr.at[tp],
                send_sem=q_send,
                recv_sem=q_recv,
                device_id={"tp": (tp + d) % 16},
                device_id_type=MESH,
            ).start()

    ig_pair = d2d(igs, igr, 2)

    def chunk(c, carry):
        k = NCOT + 2 + c

        @pl.when(k < NPAY)
        def _():
            r2(k)

        @pl.when(k + 1 < NPAY)
        def _():
            r1(k + 1)

        r5(k - 2)
        main_weight(c)
        main_tile(c, 0)

        @pl.when(k < NPAY)
        def _():
            r3(k)

        @pl.when(c == 0)
        def _():
            reduce_down()

        main_tile(c, 1)

        @pl.when(k - 1 < NPAY)
        def _():
            r4(k - 1)

        main_tile(c, 2)

        @pl.when(k + 3 < NPAY)
        def _():
            r0(k + 3)

        @pl.when(c == 1)
        def _():
            finish_down()

        main_tile(c, 3)

        @pl.when(c == 1)
        def _():
            send_down_sq()

        @pl.when(c >= 1)
        def _():
            reduce_grads(c - 1)

        main_grads()
        send_grads(c)
        main_input(c)
        return carry

    lax.fori_loop(0, NCH, chunk, 0)

    igs[...] = ig[pl.ds(theirs, HALF), :].astype(BF)
    mine_part = ig[pl.ds(mine, HALF), :].astype(BF).astype(F32)
    ig[pl.ds(mine, HALF), :] = mine_part
    ig_pair.start()
    reduce_grads(NCH - 1)
    sqs[...] = jnp.sum(sqacc[...].T, axis=0, keepdims=True)
    sqr[rep * 2 + fs] = sqs[...]
    for d in range(1, 8):
        other = {"rep": (rep + d // 2) % 4, "fs": (fs + d) % 2}
        pltpu.make_async_remote_copy(
            src_ref=sqs,
            dst_ref=sqr.at[rep * 2 + fs],
            send_sem=r_send.at[3],
            recv_sem=r_recv.at[3],
            device_id=other,
            device_id_type=MESH,
        ).start()
    ig_pair.wait_recv()
    ig_out[...] = (ig[pl.ds(mine, HALF), :] + igr[...].astype(F32)).astype(BF)
    all15 = dsqr.at[pl.ds(0, 15)]
    pltpu.make_async_copy(all15, all15, q_recv).wait()
    total = dsqr[0]
    for k in range(1, 16):
        total = total + dsqr[k]
    dsq_out[...] = total

    for p in range(NPAY):
        take(send_sem.at[p], 15)
    for k in range(NCOT):
        take(d2d_send.at[k], 15)
    for k in range(NCH):
        three(gs.at[k], rs_send.at[k])
        three(ag.at[k], ag_send.at[k])
    three(ds, rs_send.at[NCH])
    three(dag, ag_send.at[NCH])
    pltpu.make_async_copy(all15, all15, q_send).wait()
    cot_pair.wait_send()
    x_pair.wait_send()
    ig_pair.wait_send()
    for k in range(NCH):
        three(ag.at[k], ag_recv.at[k])
    all7 = sqr.at[pl.ds(0, 7)]
    pltpu.make_async_copy(all7, all7, r_send.at[3]).wait()
    pltpu.make_async_copy(all7, all7, r_recv.at[3]).wait()
    total = sqr[0]
    for k in range(1, 8):
        total = total + sqr[k]
    sq_out[...] = total


def finish(ig, ag, dag, sq, dsq, ig_out, gg_out, ug_out, dg_out, gsq_out, usq_out, dsq_out):
    ig_out[...] = ig[...]
    for c in range(NCH):
        for j in range(4):
            v = ag[c, j].astype(F32)
            gg_out[32 * j : 32 * j + 32, c * CH : (c + 1) * CH] = v[0:32]
            ug_out[32 * j : 32 * j + 32, c * CH : (c + 1) * CH] = v[32:64]
    for k in range(FH // 128):
        v = jnp.concatenate(
            [dag[j, :, 128 * k : 128 * k + 128].astype(F32) for j in range(4)], axis=0
        )
        dg_out[128 * k : 128 * k + 128, :] = v.T
    gsq_out[...] = sq[0, 0:128]
    usq_out[...] = sq[0, 128:256]
    dsq_out[...] = dsq[0, :]


def on_device(layer_input, cotangent, gate_pre, up_pre, gate_weight, up_weight, down_weight):
    anyspec = pl.BlockSpec(memory_space=pl.ANY)
    vm = pl.BlockSpec(memory_space=pltpu.VMEM)
    dma = pltpu.SemaphoreType.DMA
    outs = pl.pallas_call(
        body,
        out_shape=(
            jax.ShapeDtypeStruct((HALF, 128), BF),
            jax.ShapeDtypeStruct((NCH, 4, 64, CH), BF),
            jax.ShapeDtypeStruct((4, 32, FH), BF),
            jax.ShapeDtypeStruct((1, 256), F32),
            jax.ShapeDtypeStruct((1, FH), F32),
        ),
        in_specs=[anyspec] * 7,
        out_specs=(vm,) * 5,
        scratch_shapes=[
            pltpu.VMEM((16, TOK + FH, 128), BF),
            pltpu.VMEM((NCH, TOK, CH), BF),
            pltpu.VMEM((NCH, TOK, CH), BF),
            pltpu.VMEM((2, TP, FH), BF),
            pltpu.VMEM((2, TP, FH), BF),
            pltpu.VMEM((TP, FH), BF),
            pltpu.VMEM((TOK, 128), BF),
            pltpu.VMEM((128, TOK), BF),
            pltpu.VMEM((128, FH), F32),
            pltpu.VMEM((TOK, 128), F32),
            pltpu.VMEM((128, FH), BF),
            pltpu.VMEM((128, FH), BF),
            pltpu.VMEM((TOK, 2 * CH), BF),
            pltpu.VMEM((2048, CH), BF),
            pltpu.VMEM((128, 2 * CH), F32),
            pltpu.VMEM((NCH, 4, 64, CH), BF),
            pltpu.VMEM((NCH, 4, 64, CH), BF),
            pltpu.VMEM((4, 32, FH), BF),
            pltpu.VMEM((4, 32, FH), BF),
            pltpu.VMEM((HALF, 128), BF),
            pltpu.VMEM((HALF, 128), BF),
            pltpu.VMEM((256, 128), F32),
            pltpu.VMEM((1, 256), F32),
            pltpu.VMEM((8, 1, 256), F32),
            pltpu.VMEM((1, FH), F32),
            pltpu.VMEM((16, 1, FH), F32),
            dma((NPAY,)),
            dma((NPAY, 6)),
            dma((NCOT,)),
            dma((NCOT,)),
            dma((5,)),
            dma((2, 2)),
            dma((NCH + 1,)),
            dma((NCH + 1,)),
            dma((NCH + 1,)),
            dma((NCH + 1,)),
            dma,
            dma,
            dma((4,)),
            dma((4,)),
        ],
        compiler_params=pltpu.CompilerParams(
            collective_id=0, has_side_effects=True, vmem_limit_bytes=64000000
        ),
        name="backward",
    )(layer_input, cotangent, gate_pre, up_pre, gate_weight, up_weight, down_weight)
    return pl.pallas_call(
        finish,
        out_shape=(
            jax.ShapeDtypeStruct((HALF, 128), BF),
            jax.ShapeDtypeStruct((128, FH), F32),
            jax.ShapeDtypeStruct((128, FH), F32),
            jax.ShapeDtypeStruct((FH, 128), F32),
            jax.ShapeDtypeStruct((128,), F32),
            jax.ShapeDtypeStruct((128,), F32),
            jax.ShapeDtypeStruct((FH,), F32),
        ),
        in_specs=[vm] * 5,
        out_specs=(vm,) * 7,
        name="outputs",
    )(*outs)


def solution(mesh):
    return jax.shard_map(
        on_device,
        mesh=mesh,
        in_specs=(
            P(("rep", "fs"), "tp"),
            P(("rep", "fs"), "tp"),
            P("rep", "fs"),
            P("rep", "fs"),
            P("tp", "fs"),
            P("tp", "fs"),
            P("fs", "tp"),
        ),
        out_specs=(
            P(("rep", "fs"), "tp"),
            P("tp", "fs"),
            P("tp", "fs"),
            P("fs", "tp"),
            P("tp"),
            P("tp"),
            P("fs"),
        ),
        check_vma=False,
    )
```

```python
import math

import jax
import jax.numpy as jnp
from jax import lax
from jax.experimental import pallas as pl
from jax.experimental.pallas import tpu as pltpu
from jax.sharding import PartitionSpec as P

MESH = pl.DeviceIdType.MESH
BF = jnp.bfloat16
F32 = jnp.float32

TOK = 2560
HALF = 1280
FH = 1536
N = 256
CH = 256
NCH = FH // CH
NCOT = HALF // N
SH = CH // 4
NXC = 2
NPAY = NCOT + NCH - NXC
TM = 640
TP = 256


def body(
    x_hbm, cot_hbm, gate_hbm, up_hbm, gw_hbm, uw_hbm, dw_hbm,
    ig_out, ag, dag, sq_out, dsq_out,
    allb, aa, cc, gbuf, ubuf, hid, xb, xt, dgt, ig, gw, uw,
    wt, gacc, gs, rs, ds, dr, igs, igr, sqacc, sqs, sqr, dsqs, dsqr,
    send_sem, recv_sem, x_send, x_recv, d2d_send, d2d_recv, loc_sem, tile_sem,
    rs_send, rs_recv, ag_send, ag_recv, q_send, q_recv, r_send, r_recv,
):
    rep = lax.axis_index("rep")
    fs = lax.axis_index("fs")
    tp = lax.axis_index("tp")
    z, y = tp // 4, tp % 4
    sib = 1 - fs
    scale = 1.0 / math.sqrt(TOK * 4)

    def blk(dz, dy):
        return ((z + dz) % 4) * 4 + (y + dy) % 4

    mine = pl.multiple_of(fs * HALF, HALF)
    theirs = pl.multiple_of(sib * HALF, HALF)

    own_cot = pltpu.make_async_copy(cot_hbm, allb.at[tp, pl.ds(mine, HALF)], loc_sem.at[0])
    own_rows = [(CH * i + SH * rep, SH, 5 + i) for i in range(NXC)] + [(NXC * CH, FH - NXC * CH, 1)]
    own_dw = [
        pltpu.make_async_copy(
            dw_hbm.at[pl.ds(pl.multiple_of(r, SH), n)],
            allb.at[tp, pl.ds(pl.multiple_of(TOK + r, SH), n)],
            loc_sem.at[k],
        )
        for r, n, k in own_rows
    ]
    own_x = pltpu.make_async_copy(x_hbm, xb.at[pl.ds(mine, HALF)], loc_sem.at[2])
    own_gw = pltpu.make_async_copy(gw_hbm, gw, loc_sem.at[3])
    own_uw = pltpu.make_async_copy(uw_hbm, uw, loc_sem.at[4])
    own_cot.start()
    own_x.start()
    for c in own_dw:
        c.start()

    def tile_rows(i):
        return pl.multiple_of(((fs * 5 + i) % 10) * TP, TP)

    def loads(i):
        slot = i % 2
        r = tile_rows(i)
        return (
            pltpu.make_async_copy(gate_hbm.at[pl.ds(r, TP)], gbuf.at[slot], tile_sem.at[slot, 0]),
            pltpu.make_async_copy(up_hbm.at[pl.ds(r, TP)], ubuf.at[slot], tile_sem.at[slot, 1]),
        )

    for c in loads(0):
        c.start()
    for c in loads(1):
        c.start()
    own_gw.start()
    own_uw.start()

    barrier = pltpu.get_barrier_semaphore()
    for d in range(1, 16):
        pl.semaphore_signal(barrier, inc=1, device_id={"tp": (tp + d) % 16}, device_id_type=MESH)
    for d in range(1, 4):
        peer = (rep + d) % 4
        pl.semaphore_signal(barrier, inc=1, device_id={"rep": peer}, device_id_type=MESH)
        pl.semaphore_signal(barrier, inc=1, device_id={"rep": peer, "fs": sib}, device_id_type=MESH)
    pl.semaphore_signal(barrier, inc=1, device_id={"fs": sib}, device_id_type=MESH)
    pl.semaphore_wait(barrier, 22)

    def row0(p):
        w = (p + 11) // 16
        return 256 * p + w * (NXC * CH + HALF) + (1 - w) * fs * HALF

    def whole(p):
        return p, row0(p), N

    def share(i):
        return NPAY + i, TOK + CH * i + SH * rep, SH

    def put(pay, b, first, num, dz, dy, g):
        p, row, n = pay
        q = n // 4
        rows = pl.ds(pl.multiple_of(row + first * q, 16), num * q)
        ref = allb.at[b, rows]
        pltpu.make_async_remote_copy(
            src_ref=ref,
            dst_ref=ref,
            send_sem=send_sem.at[p],
            recv_sem=recv_sem.at[p, g],
            device_id={"tp": blk(dz, dy)},
            device_id_type=MESH,
        ).start()

    def take(sem, k, n=N):
        ref = allb.at[pl.ds(0, k), pl.ds(0, n)]
        pltpu.make_async_copy(ref, ref, sem).wait()

    def got(pay, g, k):
        take(recv_sem.at[pay[0], g], k, pay[2])

    def both_y(pay, b, g):
        put(pay, b, 0, 2, 0, 1, g)
        put(pay, b, 0, 2, 0, -1, g)

    def both_z(pay, b, g):
        put(pay, b, 2, 2, 1, 0, g)
        put(pay, b, 2, 2, -1, 0, g)

    def r0(pay):
        put(pay, tp, 0, 2, 1, 0, 0)
        put(pay, tp, 0, 2, -1, 0, 0)
        put(pay, tp, 2, 2, 0, 1, 0)
        put(pay, tp, 2, 2, 0, -1, 0)
        both_y(pay, tp, 2)
        both_z(pay, tp, 2)

    def r1(pay):
        got(pay, 0, 2)
        put(pay, blk(-1, 0), 0, 1, 1, 0, 1)
        put(pay, blk(1, 0), 1, 1, -1, 0, 1)
        put(pay, blk(0, -1), 2, 1, 0, 1, 1)
        put(pay, blk(0, 1), 3, 1, 0, -1, 1)
        for d in (-1, 1):
            both_y(pay, blk(d, 0), 2)
            both_z(pay, blk(0, d), 2)

    def r2(pay):
        got(pay, 1, 1)
        both_y(pay, blk(2, 0), 3)
        both_z(pay, blk(0, 2), 3)

    def onward(pay, d, g):
        put(pay, blk(d, -1), 0, 1, 0, 1, g)
        put(pay, blk(d, 1), 1, 1, 0, -1, g)
        put(pay, blk(-1, d), 2, 1, 1, 0, g)
        put(pay, blk(1, d), 3, 1, -1, 0, g)

    def r3(pay):
        got(pay, 2, 6)
        for d in (0, -1, 1):
            onward(pay, d, 4)

    def r4(pay):
        got(pay, 3, 2)
        onward(pay, 2, 5)

    def r5(pay):
        got(pay, 4, 3)
        got(pay, 5, 1)

    def over_rep(i):
        rows = pl.ds(pl.multiple_of(TOK + CH * i + SH * rep, SH), SH)
        ref = allb.at[pl.ds(0, 16), rows]
        for d in (1, 3, 2):
            pltpu.make_async_remote_copy(
                src_ref=ref,
                dst_ref=ref,
                send_sem=x_send.at[i],
                recv_sem=x_recv.at[i],
                device_id={"rep": (rep + d) % 4},
                device_id_type=MESH,
            ).start()

    NEAR = [(dz, dy) for dz in (0, 1, -1) for dy in (0, 1, -1) if (dz, dy) != (0, 0)]
    FAR = [(2, dy) for dy in (0, 1, -1, 2)] + [(dz, 2) for dz in (0, 1, -1)]

    def to_sibling(p, blocks):
        rows = pl.ds(pl.multiple_of(fs * HALF + N * p, N), N)
        for dz, dy in blocks:
            ref = allb.at[blk(dz, dy), rows]
            pltpu.make_async_remote_copy(
                src_ref=ref,
                dst_ref=ref,
                send_sem=d2d_send.at[p],
                recv_sem=d2d_recv.at[p],
                device_id={"fs": sib},
                device_id_type=MESH,
            ).start()

    def d2d(src, dst, k):
        return pltpu.make_async_remote_copy(
            src_ref=src,
            dst_ref=dst,
            send_sem=r_send.at[k],
            recv_sem=r_recv.at[k],
            device_id={"fs": sib},
            device_id_type=MESH,
        )

    for c in own_dw:
        c.wait()
    shares = [share(i) for i in range(NXC)]
    for h in shares:
        r0(h)
    own_cot.wait()
    r0(whole(0))
    r0(whole(1))
    cot_pair = d2d(allb.at[tp, pl.ds(mine, HALF)], allb.at[tp, pl.ds(mine, HALF)], 0)
    cot_pair.start()
    own_x.wait()
    x_pair = d2d(xb.at[pl.ds(mine, HALF)], xb.at[pl.ds(mine, HALF)], 1)
    x_pair.start()
    own_gw.wait()
    own_uw.wait()
    dgt[...] = jnp.zeros_like(dgt)
    sqacc[...] = jnp.zeros_like(sqacc)
    for h in shares:
        r1(h)
    r0(whole(2))
    r1(whole(0))
    cot_pair.wait_recv()
    x_pair.wait_recv()

    def transpose_x(i, carry):
        r = pl.multiple_of(i * 128, 128)
        v = xb[pl.ds(r, 128), :].astype(F32)
        xt[:, pl.ds(r, 128)] = v.T.astype(BF)
        return carry

    for h in shares:
        r2(h)
    for h in shares:
        r3(h)
    r0(whole(3))
    r1(whole(1))
    lax.fori_loop(0, TOK // 128, transpose_x, 0)
    for h in shares:
        r4(h)
    r0(whole(4))

    def tile(i):
        slot = i % 2
        r = tile_rows(i)
        for c in loads(i):
            c.wait()

        def sub(k, carry):
            q = pl.multiple_of(k * 32, 32)
            for j in range(NCH):
                g = gbuf[slot, pl.ds(q, 32), j * CH : (j + 1) * CH].astype(F32)
                u = ubuf[slot, pl.ds(q, 32), j * CH : (j + 1) * CH].astype(F32)
                s = 1.0 / (1.0 + jnp.exp(-g))
                a = g * s
                hid[pl.ds(q, 32), j * CH : (j + 1) * CH] = (a * u).astype(BF)
                aa[j, pl.ds(pl.multiple_of(r + q, 32), 32), :] = a.astype(BF)
                cc[j, pl.ds(pl.multiple_of(r + q, 32), 32), :] = (
                    u * s * (1.0 + g * (1.0 - s))
                ).astype(BF)
            return carry

        lax.fori_loop(0, TP // 32, sub, 0)

        @pl.when(i < 8)
        def _():
            for c in loads(i + 2):
                c.start()

        ct = allb[tp, pl.ds(r, TP), :].astype(F32).T.astype(BF)
        dgt[...] += jnp.dot(ct, hid[...], preferred_element_type=F32)

    def first(k, carry):
        r2(whole(k))

        @pl.when(k + 2 < NCOT)
        def _():
            r1(whole(k + 2))

        tile(2 * k)

        @pl.when(k == 0)
        def _():
            for i, h in enumerate(shares):
                r5(h)
                over_rep(i)

        r3(whole(k))
        to_sibling(k, NEAR)

        @pl.when(k >= 1)
        def _():
            r4(whole(k - 1))

        tile(2 * k + 1)

        @pl.when(k >= 2)
        def _():
            r5(whole(k - 2))
            to_sibling(k - 2, FAR)

        return carry

    lax.fori_loop(0, NCOT - 1, first, 0)

    def scatter(src, dst, s_sem, r_sem):
        for d in range(1, 4):
            peer = (rep + d) % 4
            pltpu.make_async_remote_copy(
                src_ref=src.at[peer],
                dst_ref=dst.at[rep],
                send_sem=s_sem,
                recv_sem=r_sem,
                device_id={"rep": peer},
                device_id_type=MESH,
            ).start()

    def spread(buf, s_sem, r_sem):
        for d in range(1, 4):
            pltpu.make_async_remote_copy(
                src_ref=buf.at[rep],
                dst_ref=buf.at[rep],
                send_sem=s_sem,
                recv_sem=r_sem,
                device_id={"rep": (rep + d) % 4},
                device_id_type=MESH,
            ).start()

    def three(buf, sem):
        ref = buf.at[pl.ds(0, 3)]
        pltpu.make_async_copy(ref, ref, sem).wait()

    k = NCOT - 1
    r2(whole(k))
    tile(2 * k)
    r3(whole(k))
    to_sibling(k, NEAR)
    r4(whole(k - 1))
    r0(whole(k + 1))
    tile(2 * k + 1)
    r5(whole(k - 2))
    to_sibling(k - 2, FAR)
    for j in range(4):
        ds[j] = (dgt[32 * j : 32 * j + 32, :] * scale).astype(BF)
    dr[rep] = ds[rep]
    r4(whole(k))
    r5(whole(k - 1))
    to_sibling(k - 1, FAR)
    r0(whole(k + 2))
    r1(whole(k + 1))
    scatter(ds, dr, rs_send.at[NCH], rs_recv.at[NCH])
    r5(whole(k))
    to_sibling(k, FAR)
    r0(whole(k + 3))
    take(x_recv.at[0], 12)
    for k in range(NCOT):
        take(d2d_recv.at[k], 15)

    def main_weight(c):
        fr = pl.ds(pl.multiple_of(TOK + c * CH, CH), CH)
        for k in range(16):
            wt[128 * k : 128 * k + 128, :] = allb[k, fr, :].astype(F32).T.astype(BF)

    def main_tile(c, j):
        for i in range(2):
            rows = pl.ds(j * TM + i * (TM // 2), TM // 2)
            lhs = jnp.concatenate([allb[k, rows, :] for k in range(16)], axis=1)
            hg = jnp.dot(lhs, wt[...], preferred_element_type=F32)
            cc[c, rows, :] = (hg * cc[c, rows, :].astype(F32)).astype(BF)
            aa[c, rows, :] = (hg * aa[c, rows, :].astype(F32)).astype(BF)

    def main_grads(c):
        gacc[:, 0:CH] = jnp.dot(xt[...], cc[c], preferred_element_type=F32)
        gacc[:, CH : 2 * CH] = jnp.dot(xt[...], aa[c], preferred_element_type=F32)

    def input_part(start):
        wts = jnp.concatenate([gw[...], uw[...]], axis=1)
        parts = []
        for i in range(2):
            rows = pl.ds(pl.multiple_of(start + i * TM, TM), TM)
            lhs = jnp.concatenate(
                [cc[c, rows, :] for c in range(NCH)] + [aa[c, rows, :] for c in range(NCH)],
                axis=1,
            )
            parts.append(
                lax.dot_general(lhs, wts, (((1,), (1,)), ((), ())), preferred_element_type=F32)
            )
        return parts

    def send_grads(c):
        for j in range(4):
            gs[c, j, 0:32, :] = (gacc[32 * j : 32 * j + 32, 0:CH] * scale).astype(BF)
            gs[c, j, 32:64, :] = (gacc[32 * j : 32 * j + 32, CH : 2 * CH] * scale).astype(BF)
        rs[c, rep] = gs[c, rep]
        scatter(gs.at[c], rs.at[c], rs_send.at[c], rs_recv.at[c])

    def reduce_grads(c):
        three(rs.at[c], rs_recv.at[c])
        v = rs[c, 0].astype(F32) + rs[c, 1].astype(F32)
        v = v + rs[c, 2].astype(F32) + rs[c, 3].astype(F32)
        ag[c, rep] = v.astype(BF)
        w = v * v
        w = w[:, 0:128] + w[:, 128:256]
        sqacc[pl.ds(pl.multiple_of(32 * rep, 32), 32), :] += w[0:32]
        sqacc[pl.ds(pl.multiple_of(128 + 32 * rep, 32), 32), :] += w[32:64]
        spread(ag.at[c], ag_send.at[c], ag_recv.at[c])

    def reduce_down():
        three(dr, rs_recv.at[NCH])
        v = dr[0].astype(F32) + dr[1].astype(F32)
        v = v + dr[2].astype(F32) + dr[3].astype(F32)
        dag[rep] = v.astype(BF)
        spread(dag, ag_send.at[NCH], ag_recv.at[NCH])

    def finish_down():
        three(dag, ag_recv.at[NCH])
        for k in range(FH // 128):
            v = jnp.concatenate(
                [dag[j, :, 128 * k : 128 * k + 128].astype(F32) for j in range(4)], axis=0
            )
            dsqs[:, 128 * k : 128 * k + 128] = jnp.sum(v * v, axis=0, keepdims=True)

    def send_down_sq():
        dsqr[tp] = dsqs[...]
        for d in range(1, 16):
            pltpu.make_async_remote_copy(
                src_ref=dsqs,
                dst_ref=dsqr.at[tp],
                send_sem=q_send,
                recv_sem=q_recv,
                device_id={"tp": (tp + d) % 16},
                device_id_type=MESH,
            ).start()

    ig_pair = d2d(igs, igr, 2)

    def chunk(c, carry):
        k = NCOT + c

        @pl.when(c == 1)
        def _():
            take(x_recv.at[1], 12)

        main_weight(c)
        main_tile(c, 0)

        @pl.when((c >= 1) & (k - 1 < NPAY))
        def _():
            r4(whole(k - 1))

        @pl.when(c == 0)
        def _():
            r0(whole(NPAY - 1))

        main_tile(c, 1)

        @pl.when(k < NPAY)
        def _():
            r2(whole(k))

        @pl.when(k + 1 < NPAY)
        def _():
            r1(whole(k + 1))

        main_tile(c, 2)

        @pl.when(k < NPAY)
        def _():
            r3(whole(k))

        @pl.when(c == 2)
        def _():
            reduce_down()

        @pl.when(c == 4)
        def _():
            finish_down()

        main_tile(c, 3)

        @pl.when(c == 4)
        def _():
            send_down_sq()

        @pl.when(c >= 2)
        def _():
            reduce_grads(c - 2)

        @pl.when((c >= 1) & (k - 1 < NPAY))
        def _():
            r5(whole(k - 1))

        main_grads(c)
        send_grads(c)
        return carry

    lax.fori_loop(0, NCH, chunk, 0)

    reduce_grads(NCH - 2)
    for i, v in enumerate(input_part(theirs)):
        igs[i * TM : (i + 1) * TM, :] = v.astype(BF)
    reduce_grads(NCH - 1)
    ig_pair.start()
    sqs[...] = jnp.sum(sqacc[...].T, axis=0, keepdims=True)
    sqr[rep * 2 + fs] = sqs[...]
    for d in range(1, 8):
        other = {"rep": (rep + d // 2) % 4, "fs": (fs + d) % 2}
        pltpu.make_async_remote_copy(
            src_ref=sqs,
            dst_ref=sqr.at[rep * 2 + fs],
            send_sem=r_send.at[3],
            recv_sem=r_recv.at[3],
            device_id=other,
            device_id_type=MESH,
        ).start()
    for i, v in enumerate(input_part(mine)):
        ig[i * TM : (i + 1) * TM, :] = v.astype(BF).astype(F32)
    ig_pair.wait_recv()
    ig_out[...] = (ig[...] + igr[...].astype(F32)).astype(BF)
    all15 = dsqr.at[pl.ds(0, 15)]
    pltpu.make_async_copy(all15, all15, q_recv).wait()
    total = dsqr[0]
    for k in range(1, 16):
        total = total + dsqr[k]
    dsq_out[...] = total

    for p in range(NPAY):
        take(send_sem.at[p], 15)
    for i in range(NXC):
        take(send_sem.at[NPAY + i], 15, SH)
        take(x_send.at[i], 12)
    for k in range(NCOT):
        take(d2d_send.at[k], 15)
    for k in range(NCH):
        three(gs.at[k], rs_send.at[k])
        three(ag.at[k], ag_send.at[k])
    three(ds, rs_send.at[NCH])
    three(dag, ag_send.at[NCH])
    pltpu.make_async_copy(all15, all15, q_send).wait()
    cot_pair.wait_send()
    x_pair.wait_send()
    ig_pair.wait_send()
    for k in range(NCH):
        three(ag.at[k], ag_recv.at[k])
    all7 = sqr.at[pl.ds(0, 7)]
    pltpu.make_async_copy(all7, all7, r_send.at[3]).wait()
    pltpu.make_async_copy(all7, all7, r_recv.at[3]).wait()
    total = sqr[0]
    for k in range(1, 8):
        total = total + sqr[k]
    sq_out[...] = total


def finish(ig, ag, dag, sq, dsq, ig_out, gg_out, ug_out, dg_out, gsq_out, usq_out, dsq_out):
    ig_out[...] = ig[...]
    for c in range(NCH):
        for j in range(4):
            v = ag[c, j].astype(F32)
            gg_out[32 * j : 32 * j + 32, c * CH : (c + 1) * CH] = v[0:32]
            ug_out[32 * j : 32 * j + 32, c * CH : (c + 1) * CH] = v[32:64]
    for k in range(FH // 128):
        v = jnp.concatenate(
            [dag[j, :, 128 * k : 128 * k + 128].astype(F32) for j in range(4)], axis=0
        )
        dg_out[128 * k : 128 * k + 128, :] = v.T
    gsq_out[...] = sq[0, 0:128]
    usq_out[...] = sq[0, 128:256]
    dsq_out[...] = dsq[0, :]


def on_device(layer_input, cotangent, gate_pre, up_pre, gate_weight, up_weight, down_weight):
    anyspec = pl.BlockSpec(memory_space=pl.ANY)
    vm = pl.BlockSpec(memory_space=pltpu.VMEM)
    dma = pltpu.SemaphoreType.DMA
    outs = pl.pallas_call(
        body,
        out_shape=(
            jax.ShapeDtypeStruct((HALF, 128), BF),
            jax.ShapeDtypeStruct((NCH, 4, 64, CH), BF),
            jax.ShapeDtypeStruct((4, 32, FH), BF),
            jax.ShapeDtypeStruct((1, 256), F32),
            jax.ShapeDtypeStruct((1, FH), F32),
        ),
        in_specs=[anyspec] * 7,
        out_specs=(vm,) * 5,
        scratch_shapes=[
            pltpu.VMEM((16, TOK + FH, 128), BF),
            pltpu.VMEM((NCH, TOK, CH), BF),
            pltpu.VMEM((NCH, TOK, CH), BF),
            pltpu.VMEM((2, TP, FH), BF),
            pltpu.VMEM((2, TP, FH), BF),
            pltpu.VMEM((TP, FH), BF),
            pltpu.VMEM((TOK, 128), BF),
            pltpu.VMEM((128, TOK), BF),
            pltpu.VMEM((128, FH), F32),
            pltpu.VMEM((HALF, 128), F32),
            pltpu.VMEM((128, FH), BF),
            pltpu.VMEM((128, FH), BF),
            pltpu.VMEM((2048, CH), BF),
            pltpu.VMEM((128, 2 * CH), F32),
            pltpu.VMEM((NCH, 4, 64, CH), BF),
            pltpu.VMEM((NCH, 4, 64, CH), BF),
            pltpu.VMEM((4, 32, FH), BF),
            pltpu.VMEM((4, 32, FH), BF),
            pltpu.VMEM((HALF, 128), BF),
            pltpu.VMEM((HALF, 128), BF),
            pltpu.VMEM((256, 128), F32),
            pltpu.VMEM((1, 256), F32),
            pltpu.VMEM((8, 1, 256), F32),
            pltpu.VMEM((1, FH), F32),
            pltpu.VMEM((16, 1, FH), F32),
            dma((NPAY + NXC,)),
            dma((NPAY + NXC, 6)),
            dma((NXC,)),
            dma((NXC,)),
            dma((NCOT,)),
            dma((NCOT,)),
            dma((5 + NXC,)),
            dma((2, 2)),
            dma((NCH + 1,)),
            dma((NCH + 1,)),
            dma((NCH + 1,)),
            dma((NCH + 1,)),
            dma,
            dma,
            dma((4,)),
            dma((4,)),
        ],
        compiler_params=pltpu.CompilerParams(
            collective_id=0, has_side_effects=True, vmem_limit_bytes=64000000
        ),
        name="backward",
    )(layer_input, cotangent, gate_pre, up_pre, gate_weight, up_weight, down_weight)
    return pl.pallas_call(
        finish,
        out_shape=(
            jax.ShapeDtypeStruct((HALF, 128), BF),
            jax.ShapeDtypeStruct((128, FH), F32),
            jax.ShapeDtypeStruct((128, FH), F32),
            jax.ShapeDtypeStruct((FH, 128), F32),
            jax.ShapeDtypeStruct((128,), F32),
            jax.ShapeDtypeStruct((128,), F32),
            jax.ShapeDtypeStruct((FH,), F32),
        ),
        in_specs=[vm] * 5,
        out_specs=(vm,) * 7,
        name="outputs",
    )(*outs)


def solution(mesh):
    return jax.shard_map(
        on_device,
        mesh=mesh,
        in_specs=(
            P(("rep", "fs"), "tp"),
            P(("rep", "fs"), "tp"),
            P("rep", "fs"),
            P("rep", "fs"),
            P("tp", "fs"),
            P("tp", "fs"),
            P("fs", "tp"),
        ),
        out_specs=(
            P(("rep", "fs"), "tp"),
            P("tp", "fs"),
            P("tp", "fs"),
            P("fs", "tp"),
            P("tp"),
            P("tp"),
            P("fs"),
        ),
        check_vma=False,
    )
```

```python
import math

import jax
import jax.numpy as jnp
from jax import lax
from jax.experimental import pallas as pl
from jax.experimental.pallas import tpu as pltpu
from jax.sharding import PartitionSpec as P

MESH = pl.DeviceIdType.MESH
BF = jnp.bfloat16
F32 = jnp.float32

TOK = 2560
HALF = 1280
FH = 1536
N = 256
CH = 256
NCH = FH // CH
NCOT = HALF // N
SH = CH // 4
NXC = 2
NPAY = NCOT + NCH - NXC
TM = 640
TP = 256


def body(
    x_hbm, cot_hbm, gate_hbm, up_hbm, gw_hbm, uw_hbm, dw_hbm,
    ig_hbm, ag_hbm, dag_hbm, sq_hbm, dsq_hbm,
    sq_out, dsq_out, ig_out, ag, dag, out_sem, allb, aa, cc, gbuf, ubuf, hid, xb, xt, dgt, ig, gw, uw,
    wt, gacc, gs, rs, ds, dr, igs, igr, sqacc, sqs, sqr, dsqs, dsqr,
    send_sem, recv_sem, x_send, x_recv, d2d_send, d2d_recv, loc_sem, tile_sem,
    rs_send, rs_recv, ag_send, ag_recv, q_send, q_recv, r_send, r_recv,
):
    rep = lax.axis_index("rep")
    fs = lax.axis_index("fs")
    tp = lax.axis_index("tp")
    z, y = tp // 4, tp % 4
    sib = 1 - fs
    scale = 1.0 / math.sqrt(TOK * 4)

    def blk(dz, dy):
        return ((z + dz) % 4) * 4 + (y + dy) % 4

    mine = pl.multiple_of(fs * HALF, HALF)
    theirs = pl.multiple_of(sib * HALF, HALF)

    own_cot = pltpu.make_async_copy(cot_hbm, allb.at[tp, pl.ds(mine, HALF)], loc_sem.at[0])
    own_rows = [(CH * i + SH * rep, SH, 5 + i) for i in range(NXC)] + [(NXC * CH, FH - NXC * CH, 1)]
    own_dw = [
        pltpu.make_async_copy(
            dw_hbm.at[pl.ds(pl.multiple_of(r, SH), n)],
            allb.at[tp, pl.ds(pl.multiple_of(TOK + r, SH), n)],
            loc_sem.at[k],
        )
        for r, n, k in own_rows
    ]
    own_x = pltpu.make_async_copy(x_hbm, xb.at[pl.ds(mine, HALF)], loc_sem.at[2])
    own_gw = pltpu.make_async_copy(gw_hbm, gw, loc_sem.at[3])
    own_uw = pltpu.make_async_copy(uw_hbm, uw, loc_sem.at[4])
    own_cot.start()
    own_x.start()
    for c in own_dw:
        c.start()

    def tile_rows(i):
        return pl.multiple_of(((fs * 5 + i) % 10) * TP, TP)

    def loads(i):
        slot = i % 2
        r = tile_rows(i)
        return (
            pltpu.make_async_copy(gate_hbm.at[pl.ds(r, TP)], gbuf.at[slot], tile_sem.at[slot, 0]),
            pltpu.make_async_copy(up_hbm.at[pl.ds(r, TP)], ubuf.at[slot], tile_sem.at[slot, 1]),
        )

    for c in loads(0):
        c.start()
    for c in loads(1):
        c.start()
    own_gw.start()
    own_uw.start()

    barrier = pltpu.get_barrier_semaphore()
    for d in ((0, 1), (0, -1), (1, 0), (-1, 0)):
        pl.semaphore_signal(barrier, inc=1, device_id={"tp": blk(*d)}, device_id_type=MESH)
    for d in range(1, 4):
        peer = (rep + d) % 4
        pl.semaphore_signal(barrier, inc=1, device_id={"rep": peer}, device_id_type=MESH)
        pl.semaphore_signal(barrier, inc=1, device_id={"rep": peer, "fs": sib}, device_id_type=MESH)
    pl.semaphore_signal(barrier, inc=1, device_id={"fs": sib}, device_id_type=MESH)
    pl.semaphore_wait(barrier, 11)

    def row0(p):
        w = (p + 11) // 16
        return 256 * p + w * (NXC * CH + HALF) + (1 - w) * fs * HALF

    def whole(p):
        return p, row0(p), N

    def share(i):
        return NPAY + i, TOK + CH * i + SH * rep, SH

    def put(pay, b, first, num, dz, dy, g):
        p, row, n = pay
        q = n // 4
        rows = pl.ds(pl.multiple_of(row + first * q, 16), num * q)
        ref = allb.at[b, rows]
        pltpu.make_async_remote_copy(
            src_ref=ref,
            dst_ref=ref,
            send_sem=send_sem.at[p],
            recv_sem=recv_sem.at[p, g],
            device_id={"tp": blk(dz, dy)},
            device_id_type=MESH,
        ).start()

    def take(sem, k, n=N):
        ref = allb.at[pl.ds(0, k), pl.ds(0, n)]
        pltpu.make_async_copy(ref, ref, sem).wait()

    def got(pay, g, k):
        take(recv_sem.at[pay[0], g], k, pay[2])

    def both_y(pay, b, g):
        put(pay, b, 0, 2, 0, 1, g)
        put(pay, b, 0, 2, 0, -1, g)

    def both_z(pay, b, g):
        put(pay, b, 2, 2, 1, 0, g)
        put(pay, b, 2, 2, -1, 0, g)

    def r0(pay):
        put(pay, tp, 0, 2, 1, 0, 0)
        put(pay, tp, 0, 2, -1, 0, 0)
        put(pay, tp, 2, 2, 0, 1, 0)
        put(pay, tp, 2, 2, 0, -1, 0)
        both_y(pay, tp, 2)
        both_z(pay, tp, 2)

    def r1(pay):
        got(pay, 0, 2)
        put(pay, blk(-1, 0), 0, 1, 1, 0, 1)
        put(pay, blk(1, 0), 1, 1, -1, 0, 1)
        put(pay, blk(0, -1), 2, 1, 0, 1, 1)
        put(pay, blk(0, 1), 3, 1, 0, -1, 1)
        for d in (-1, 1):
            both_y(pay, blk(d, 0), 2)
            both_z(pay, blk(0, d), 2)

    def r2(pay):
        got(pay, 1, 1)
        both_y(pay, blk(2, 0), 3)
        both_z(pay, blk(0, 2), 3)

    def onward(pay, d, g):
        put(pay, blk(d, -1), 0, 1, 0, 1, g)
        put(pay, blk(d, 1), 1, 1, 0, -1, g)
        put(pay, blk(-1, d), 2, 1, 1, 0, g)
        put(pay, blk(1, d), 3, 1, -1, 0, g)

    def r3(pay):
        got(pay, 2, 6)
        for d in (0, -1, 1):
            onward(pay, d, 4)

    def r4(pay):
        got(pay, 3, 2)
        onward(pay, 2, 5)

    def r5(pay):
        got(pay, 4, 3)
        got(pay, 5, 1)

    def over_rep(i):
        rows = pl.ds(pl.multiple_of(TOK + CH * i + SH * rep, SH), SH)
        ref = allb.at[pl.ds(0, 16), rows]
        for d in (1, 3, 2):
            pltpu.make_async_remote_copy(
                src_ref=ref,
                dst_ref=ref,
                send_sem=x_send.at[i],
                recv_sem=x_recv.at[i],
                device_id={"rep": (rep + d) % 4},
                device_id_type=MESH,
            ).start()

    NEAR = [(dz, dy) for dz in (0, 1, -1) for dy in (0, 1, -1) if (dz, dy) != (0, 0)]
    FAR = [(2, dy) for dy in (0, 1, -1, 2)] + [(dz, 2) for dz in (0, 1, -1)]

    def to_sibling(p, blocks):
        rows = pl.ds(pl.multiple_of(fs * HALF + N * p, N), N)
        for dz, dy in blocks:
            ref = allb.at[blk(dz, dy), rows]
            pltpu.make_async_remote_copy(
                src_ref=ref,
                dst_ref=ref,
                send_sem=d2d_send.at[p],
                recv_sem=d2d_recv.at[p],
                device_id={"fs": sib},
                device_id_type=MESH,
            ).start()

    def d2d(src, dst, k):
        return pltpu.make_async_remote_copy(
            src_ref=src,
            dst_ref=dst,
            send_sem=r_send.at[k],
            recv_sem=r_recv.at[k],
            device_id={"fs": sib},
            device_id_type=MESH,
        )

    def tile(i):
        slot = i % 2
        r = tile_rows(i)
        for c in loads(i):
            c.wait()

        def sub(k, carry):
            q = pl.multiple_of(k * 32, 32)
            for j in range(NCH):
                g = gbuf[slot, pl.ds(q, 32), j * CH : (j + 1) * CH].astype(F32)
                u = ubuf[slot, pl.ds(q, 32), j * CH : (j + 1) * CH].astype(F32)
                s = 1.0 / (1.0 + jnp.exp(-g))
                a = g * s
                hid[pl.ds(q, 32), j * CH : (j + 1) * CH] = (a * u).astype(BF)
                aa[j, pl.ds(pl.multiple_of(r + q, 32), 32), :] = a.astype(BF)
                cc[j, pl.ds(pl.multiple_of(r + q, 32), 32), :] = (
                    u * s * (1.0 + g * (1.0 - s))
                ).astype(BF)
            return carry

        lax.fori_loop(0, TP // 32, sub, 0)

        @pl.when(i < 8)
        def _():
            for c in loads(i + 2):
                c.start()

        ct = allb[tp, pl.ds(r, TP), :].astype(F32).T.astype(BF)
        dgt[...] += jnp.dot(ct, hid[...], preferred_element_type=F32)

    def transpose_x(i, carry):
        r = pl.multiple_of(i * 128, 128)
        v = xb[pl.ds(r, 128), :].astype(F32)
        xt[:, pl.ds(r, 128)] = v.T.astype(BF)
        return carry

    for c in own_dw:
        c.wait()
    shares = [share(i) for i in range(NXC)]
    for h in shares:
        r0(h)
    own_cot.wait()
    r0(whole(0))
    r0(whole(1))
    cot_pair = d2d(allb.at[tp, pl.ds(mine, HALF)], allb.at[tp, pl.ds(mine, HALF)], 0)
    cot_pair.start()
    own_x.wait()
    x_pair = d2d(xb.at[pl.ds(mine, HALF)], xb.at[pl.ds(mine, HALF)], 1)
    x_pair.start()
    own_gw.wait()
    own_uw.wait()
    dgt[...] = jnp.zeros_like(dgt)
    sqacc[...] = jnp.zeros_like(sqacc)
    tile(0)
    for h in shares:
        r1(h)
    r0(whole(2))
    r1(whole(0))
    tile(1)
    for h in shares:
        r2(h)
    for h in shares:
        r3(h)
    r0(whole(3))
    r1(whole(1))
    cot_pair.wait_recv()
    x_pair.wait_recv()
    lax.fori_loop(0, TOK // 128, transpose_x, 0)
    for h in shares:
        r4(h)
    r0(whole(4))
    tile(2)

    def first(k, carry):
        r2(whole(k))

        @pl.when(k + 2 < NCOT)
        def _():
            r1(whole(k + 2))

        tile(k + 3 + k // 3)

        @pl.when(k == 0)
        def _():
            for i, h in enumerate(shares):
                r5(h)
                over_rep(i)

        r3(whole(k))
        to_sibling(k, NEAR)

        @pl.when(k >= 1)
        def _():
            r4(whole(k - 1))

        @pl.when(k >= 2)
        def _():
            tile(2 * k + 2)
            r5(whole(k - 2))
            to_sibling(k - 2, FAR)

        return carry

    lax.fori_loop(0, NCOT - 1, first, 0)

    def scatter(src, dst, s_sem, r_sem):
        for d in (2, 1, 3):
            peer = (rep + d) % 4
            pltpu.make_async_remote_copy(
                src_ref=src.at[peer],
                dst_ref=dst.at[rep],
                send_sem=s_sem,
                recv_sem=r_sem,
                device_id={"rep": peer},
                device_id_type=MESH,
            ).start()

    def spread(buf, s_sem, r_sem):
        for d in (2, 1, 3):
            pltpu.make_async_remote_copy(
                src_ref=buf.at[rep],
                dst_ref=buf.at[rep],
                send_sem=s_sem,
                recv_sem=r_sem,
                device_id={"rep": (rep + d) % 4},
                device_id_type=MESH,
            ).start()

    def three(buf, sem):
        ref = buf.at[pl.ds(0, 3)]
        pltpu.make_async_copy(ref, ref, sem).wait()

    k = NCOT - 1
    r2(whole(k))
    tile(9)
    r3(whole(k))
    to_sibling(k, NEAR)
    r4(whole(k - 1))
    r0(whole(k + 1))
    r5(whole(k - 2))
    to_sibling(k - 2, FAR)
    r4(whole(k))
    r5(whole(k - 1))
    to_sibling(k - 1, FAR)
    r0(whole(k + 2))
    r1(whole(k + 1))
    r5(whole(k))
    to_sibling(k, FAR)
    r0(whole(k + 3))
    for j in range(4):
        ds[j] = (dgt[32 * j : 32 * j + 32, :] * scale).astype(BF)
    dr[rep] = ds[rep]
    scatter(ds, dr, rs_send.at[NCH], rs_recv.at[NCH])
    take(x_recv.at[0], 12)
    for k in range(NCOT):
        take(d2d_recv.at[k], 15)

    def main_weight(c):
        fr = pl.ds(pl.multiple_of(TOK + c * CH, CH), CH)
        for k in range(16):
            wt[128 * k : 128 * k + 128, :] = allb[k, fr, :].astype(F32).T.astype(BF)

    def main_tile(c, j):
        for i in range(4):
            rows = pl.ds(j * 2 * TM + i * (TM // 2), TM // 2)
            lhs = jnp.concatenate([allb[k, rows, :] for k in range(16)], axis=1)
            hg = jnp.dot(lhs, wt[...], preferred_element_type=F32)
            cc[c, rows, :] = (hg * cc[c, rows, :].astype(F32)).astype(BF)
            aa[c, rows, :] = (hg * aa[c, rows, :].astype(F32)).astype(BF)

    def main_grads(c):
        gacc[:, 0:CH] = jnp.dot(xt[...], cc[c], preferred_element_type=F32)
        gacc[:, CH : 2 * CH] = jnp.dot(xt[...], aa[c], preferred_element_type=F32)

    def input_part(start):
        wts = jnp.concatenate([gw[...], uw[...]], axis=1)
        parts = []
        for i in range(2):
            rows = pl.ds(pl.multiple_of(start + i * TM, TM), TM)
            lhs = jnp.concatenate(
                [cc[c, rows, :] for c in range(NCH)] + [aa[c, rows, :] for c in range(NCH)],
                axis=1,
            )
            parts.append(
                lax.dot_general(lhs, wts, (((1,), (1,)), ((), ())), preferred_element_type=F32)
            )
        return parts

    def send_grads(c):
        for j in range(4):
            gs[c, j, 0:32, :] = (gacc[32 * j : 32 * j + 32, 0:CH] * scale).astype(BF)
            gs[c, j, 32:64, :] = (gacc[32 * j : 32 * j + 32, CH : 2 * CH] * scale).astype(BF)
        rs[c, rep] = gs[c, rep]
        scatter(gs.at[c], rs.at[c], rs_send.at[c], rs_recv.at[c])

    def reduce_grads(c):
        three(rs.at[c], rs_recv.at[c])
        v = rs[c, 0].astype(F32) + rs[c, 1].astype(F32)
        v = v + rs[c, 2].astype(F32) + rs[c, 3].astype(F32)
        ag[c, rep] = v.astype(BF)
        w = v * v
        w = w[:, 0:128] + w[:, 128:256]
        sqacc[pl.ds(pl.multiple_of(32 * rep, 32), 32), :] += w[0:32]
        sqacc[pl.ds(pl.multiple_of(128 + 32 * rep, 32), 32), :] += w[32:64]
        spread(ag.at[c], ag_send.at[c], ag_recv.at[c])

    def reduce_down():
        three(dr, rs_recv.at[NCH])
        v = dr[0].astype(F32) + dr[1].astype(F32)
        v = v + dr[2].astype(F32) + dr[3].astype(F32)
        dag[rep] = v.astype(BF)
        spread(dag, ag_send.at[NCH], ag_recv.at[NCH])

    def finish_down():
        three(dag, ag_recv.at[NCH])
        for k in range(FH // 128):
            v = jnp.concatenate(
                [dag[j, :, 128 * k : 128 * k + 128].astype(F32) for j in range(4)], axis=0
            )
            dsqs[:, 128 * k : 128 * k + 128] = jnp.sum(v * v, axis=0, keepdims=True)

    def send_down_sq():
        dsqr[tp] = dsqs[...]
        for d in range(1, 16):
            pltpu.make_async_remote_copy(
                src_ref=dsqs,
                dst_ref=dsqr.at[tp],
                send_sem=q_send,
                recv_sem=q_recv,
                device_id={"tp": (tp + d) % 16},
                device_id_type=MESH,
            ).start()

    ig_pair = d2d(igs, igr, 2)

    def chunk(c, carry):
        k = NCOT + c

        @pl.when(c == 1)
        def _():
            take(x_recv.at[1], 12)

        @pl.when(c >= 1)
        def _():
            @pl.when(k - 1 < NPAY)
            def _():
                r4(whole(k - 1))

            @pl.when(k < NPAY)
            def _():
                r2(whole(k))

            @pl.when(k + 1 < NPAY)
            def _():
                r1(whole(k + 1))

        main_weight(c)
        main_tile(c, 0)

        @pl.when(c == 0)
        def _():
            r2(whole(NCOT))
            r1(whole(NCOT + 1))
            r0(whole(NPAY - 1))

        @pl.when((c >= 1) & (k < NPAY))
        def _():
            r3(whole(k))

        @pl.when(c == 2)
        def _():
            reduce_down()

        @pl.when(c == 4)
        def _():
            finish_down()

        main_tile(c, 1)

        @pl.when(c == 0)
        def _():
            r3(whole(NCOT))

        @pl.when(c == 4)
        def _():
            send_down_sq()

        @pl.when(c >= 2)
        def _():
            reduce_grads(c - 2)

        @pl.when((c >= 1) & (k - 1 < NPAY))
        def _():
            r5(whole(k - 1))

        main_grads(c)
        send_grads(c)
        return carry

    lax.fori_loop(0, NCH, chunk, 0)

    reduce_grads(NCH - 2)
    for i, v in enumerate(input_part(theirs)):
        igs[i * TM : (i + 1) * TM, :] = v.astype(BF)
    reduce_grads(NCH - 1)
    ig_pair.start()
    sqs[...] = jnp.sum(sqacc[...].T, axis=0, keepdims=True)
    sqr[rep * 2 + fs] = sqs[...]
    for d in range(1, 8):
        other = {"rep": (rep + d // 2) % 4, "fs": (fs + d) % 2}
        pltpu.make_async_remote_copy(
            src_ref=sqs,
            dst_ref=sqr.at[rep * 2 + fs],
            send_sem=r_send.at[3],
            recv_sem=r_recv.at[3],
            device_id=other,
            device_id_type=MESH,
        ).start()
    leave = [pltpu.make_async_copy(ag.at[k], ag_hbm.at[k], out_sem.at[k]) for k in range(NCH)]
    leave.append(pltpu.make_async_copy(dag, dag_hbm, out_sem.at[NCH]))
    leave.append(pltpu.make_async_copy(ig_out, ig_hbm, out_sem.at[NCH + 1]))
    leave[NCH].start()
    for k in range(NCH - 2):
        three(ag.at[k], ag_recv.at[k])
        leave[k].start()
    for i, v in enumerate(input_part(mine)):
        ig[i * TM : (i + 1) * TM, :] = v.astype(BF).astype(F32)
    ig_pair.wait_recv()
    ig_out[...] = (ig[...] + igr[...].astype(F32)).astype(BF)
    three(ag.at[NCH - 2], ag_recv.at[NCH - 2])
    leave[NCH - 2].start()
    leave[NCH + 1].start()
    all15 = dsqr.at[pl.ds(0, 15)]
    pltpu.make_async_copy(all15, all15, q_recv).wait()
    total = dsqr[0]
    for k in range(1, 16):
        total = total + dsqr[k]
    dsq_out[...] = total
    leave.append(pltpu.make_async_copy(dsq_out, dsq_hbm, out_sem.at[NCH + 2]))
    leave.append(pltpu.make_async_copy(sq_out, sq_hbm, out_sem.at[NCH + 3]))
    leave[NCH + 2].start()

    for p in range(NPAY):
        take(send_sem.at[p], 15)
    for i in range(NXC):
        take(send_sem.at[NPAY + i], 15, SH)
        take(x_send.at[i], 12)
    for k in range(NCOT):
        take(d2d_send.at[k], 15)
    for k in range(NCH):
        three(gs.at[k], rs_send.at[k])
        three(ag.at[k], ag_send.at[k])
    three(ds, rs_send.at[NCH])
    three(dag, ag_send.at[NCH])
    pltpu.make_async_copy(all15, all15, q_send).wait()
    cot_pair.wait_send()
    x_pair.wait_send()
    ig_pair.wait_send()
    three(ag.at[NCH - 1], ag_recv.at[NCH - 1])
    leave[NCH - 1].start()
    all7 = sqr.at[pl.ds(0, 7)]
    pltpu.make_async_copy(all7, all7, r_send.at[3]).wait()
    pltpu.make_async_copy(all7, all7, r_recv.at[3]).wait()
    total = sqr[0]
    for k in range(1, 8):
        total = total + sqr[k]
    sq_out[...] = total
    leave[NCH + 3].start()
    for c in leave:
        c.wait()


def finish(ig, ag, dag, sq, dsq, ig_out, gg_out, ug_out, dg_out, gsq_out, usq_out, dsq_out):
    ig_out[...] = ig[...]
    for c in range(NCH):
        for j in range(4):
            v = ag[c, j].astype(F32)
            gg_out[32 * j : 32 * j + 32, c * CH : (c + 1) * CH] = v[0:32]
            ug_out[32 * j : 32 * j + 32, c * CH : (c + 1) * CH] = v[32:64]
    for k in range(FH // 128):
        v = jnp.concatenate(
            [dag[j, :, 128 * k : 128 * k + 128].astype(F32) for j in range(4)], axis=0
        )
        dg_out[128 * k : 128 * k + 128, :] = v.T
    gsq_out[...] = sq[0, 0:128]
    usq_out[...] = sq[0, 128:256]
    dsq_out[...] = dsq[0, :]


def on_device(layer_input, cotangent, gate_pre, up_pre, gate_weight, up_weight, down_weight):
    anyspec = pl.BlockSpec(memory_space=pl.ANY)
    vm = pl.BlockSpec(memory_space=pltpu.VMEM)
    dma = pltpu.SemaphoreType.DMA
    outs = pl.pallas_call(
        body,
        out_shape=(
            jax.ShapeDtypeStruct((HALF, 128), BF),
            jax.ShapeDtypeStruct((NCH, 4, 64, CH), BF),
            jax.ShapeDtypeStruct((4, 32, FH), BF),
            jax.ShapeDtypeStruct((1, 256), F32),
            jax.ShapeDtypeStruct((1, FH), F32),
        ),
        in_specs=[anyspec] * 7,
        out_specs=(anyspec,) * 5,
        scratch_shapes=[
            pltpu.VMEM((1, 256), F32),
            pltpu.VMEM((1, FH), F32),
            pltpu.VMEM((HALF, 128), BF),
            pltpu.VMEM((NCH, 4, 64, CH), BF),
            pltpu.VMEM((4, 32, FH), BF),
            dma((NCH + 4,)),
            pltpu.VMEM((16, TOK + FH, 128), BF),
            pltpu.VMEM((NCH, TOK, CH), BF),
            pltpu.VMEM((NCH, TOK, CH), BF),
            pltpu.VMEM((2, TP, FH), BF),
            pltpu.VMEM((2, TP, FH), BF),
            pltpu.VMEM((TP, FH), BF),
            pltpu.VMEM((TOK, 128), BF),
            pltpu.VMEM((128, TOK), BF),
            pltpu.VMEM((128, FH), F32),
            pltpu.VMEM((HALF, 128), F32),
            pltpu.VMEM((128, FH), BF),
            pltpu.VMEM((128, FH), BF),
            pltpu.VMEM((2048, CH), BF),
            pltpu.VMEM((128, 2 * CH), F32),
            pltpu.VMEM((NCH, 4, 64, CH), BF),
            pltpu.VMEM((NCH, 4, 64, CH), BF),
            pltpu.VMEM((4, 32, FH), BF),
            pltpu.VMEM((4, 32, FH), BF),
            pltpu.VMEM((HALF, 128), BF),
            pltpu.VMEM((HALF, 128), BF),
            pltpu.VMEM((256, 128), F32),
            pltpu.VMEM((1, 256), F32),
            pltpu.VMEM((8, 1, 256), F32),
            pltpu.VMEM((1, FH), F32),
            pltpu.VMEM((16, 1, FH), F32),
            dma((NPAY + NXC,)),
            dma((NPAY + NXC, 6)),
            dma((NXC,)),
            dma((NXC,)),
            dma((NCOT,)),
            dma((NCOT,)),
            dma((5 + NXC,)),
            dma((2, 2)),
            dma((NCH + 1,)),
            dma((NCH + 1,)),
            dma((NCH + 1,)),
            dma((NCH + 1,)),
            dma,
            dma,
            dma((4,)),
            dma((4,)),
        ],
        compiler_params=pltpu.CompilerParams(
            collective_id=0, has_side_effects=True, vmem_limit_bytes=64000000
        ),
        name="backward",
    )(layer_input, cotangent, gate_pre, up_pre, gate_weight, up_weight, down_weight)
    return pl.pallas_call(
        finish,
        out_shape=(
            jax.ShapeDtypeStruct((HALF, 128), BF),
            jax.ShapeDtypeStruct((128, FH), F32),
            jax.ShapeDtypeStruct((128, FH), F32),
            jax.ShapeDtypeStruct((FH, 128), F32),
            jax.ShapeDtypeStruct((128,), F32),
            jax.ShapeDtypeStruct((128,), F32),
            jax.ShapeDtypeStruct((FH,), F32),
        ),
        in_specs=[vm] * 5,
        out_specs=(vm,) * 7,
        name="outputs",
    )(*outs)


def solution(mesh):
    return jax.shard_map(
        on_device,
        mesh=mesh,
        in_specs=(
            P(("rep", "fs"), "tp"),
            P(("rep", "fs"), "tp"),
            P("rep", "fs"),
            P("rep", "fs"),
            P("tp", "fs"),
            P("tp", "fs"),
            P("fs", "tp"),
        ),
        out_specs=(
            P(("rep", "fs"), "tp"),
            P("tp", "fs"),
            P("tp", "fs"),
            P("fs", "tp"),
            P("tp"),
            P("tp"),
            P("fs"),
        ),
        check_vma=False,
    )
```

```python
import math

import jax
import jax.numpy as jnp
from jax import lax
from jax.experimental import pallas as pl
from jax.experimental.pallas import tpu as pltpu
from jax.sharding import PartitionSpec as P

MESH = pl.DeviceIdType.MESH
BF = jnp.bfloat16
F32 = jnp.float32

TOK = 2560
HALF = 1280
FH = 1536
N = 256
CH = 256
NCH = FH // CH
NCOT = HALF // N
SH = CH // 4
NXC = 2
NPAY = NCOT + NCH - NXC
TM = 640
TP = 256


def body(
    x_hbm, cot_hbm, gate_hbm, up_hbm, gw_hbm, uw_hbm, dw_hbm,
    ig_hbm, ag_hbm, dag_hbm, sq_hbm, dsq_hbm,
    sq_out, dsq_out, ig_out, ag, dag, out_sem, allb, aa, cc, gbuf, ubuf, hid, xb, xt, dgt, ig, gw, uw,
    gacc, gs, rs, ds, dr, igs, igr, sqacc, sqs, sqr, dsqs, dsqr,
    send_sem, recv_sem, x_send, x_recv, d2d_send, d2d_recv, loc_sem, tile_sem,
    rs_send, rs_recv, ag_send, ag_recv, q_send, q_recv, r_send, r_recv,
):
    rep = lax.axis_index("rep")
    fs = lax.axis_index("fs")
    tp = lax.axis_index("tp")
    z, y = tp // 4, tp % 4
    sib = 1 - fs
    scale = 1.0 / math.sqrt(TOK * 4)

    def blk(dz, dy):
        return ((z + dz) % 4) * 4 + (y + dy) % 4

    mine = pl.multiple_of(fs * HALF, HALF)
    theirs = pl.multiple_of(sib * HALF, HALF)

    own_cot = pltpu.make_async_copy(cot_hbm, allb.at[tp, pl.ds(mine, HALF)], loc_sem.at[0])
    own_rows = [(CH * i + SH * rep, SH, 5 + i) for i in range(NXC)] + [(NXC * CH, FH - NXC * CH, 1)]
    own_dw = [
        pltpu.make_async_copy(
            dw_hbm.at[pl.ds(pl.multiple_of(r, SH), n)],
            allb.at[tp, pl.ds(pl.multiple_of(TOK + r, SH), n)],
            loc_sem.at[k],
        )
        for r, n, k in own_rows
    ]
    own_x = pltpu.make_async_copy(x_hbm, xb.at[pl.ds(mine, HALF)], loc_sem.at[2])
    own_gw = pltpu.make_async_copy(gw_hbm, gw, loc_sem.at[3])
    own_uw = pltpu.make_async_copy(uw_hbm, uw, loc_sem.at[4])
    own_cot.start()
    own_x.start()
    for c in own_dw:
        c.start()

    def tile_rows(i):
        return pl.multiple_of(((fs * 5 + i) % 10) * TP, TP)

    def loads(i):
        slot = i % 2
        r = tile_rows(i)
        return (
            pltpu.make_async_copy(gate_hbm.at[pl.ds(r, TP)], gbuf.at[slot], tile_sem.at[slot, 0]),
            pltpu.make_async_copy(up_hbm.at[pl.ds(r, TP)], ubuf.at[slot], tile_sem.at[slot, 1]),
        )

    for c in loads(0):
        c.start()
    for c in loads(1):
        c.start()
    own_gw.start()
    own_uw.start()

    barrier = pltpu.get_barrier_semaphore()
    for d in ((0, 1), (0, -1), (1, 0), (-1, 0)):
        pl.semaphore_signal(barrier, inc=1, device_id={"tp": blk(*d)}, device_id_type=MESH)
    for d in range(1, 4):
        peer = (rep + d) % 4
        pl.semaphore_signal(barrier, inc=1, device_id={"rep": peer}, device_id_type=MESH)
    pl.semaphore_signal(barrier, inc=1, device_id={"fs": sib}, device_id_type=MESH)
    pl.semaphore_wait(barrier, 8)

    def row0(p):
        w = (p + 11) // 16
        return 256 * p + w * (NXC * CH + HALF) + (1 - w) * fs * HALF

    def whole(p):
        return p, row0(p), N

    def share(i):
        return NPAY + i, TOK + CH * i + SH * rep, SH

    def put(pay, b, first, num, dz, dy, g):
        p, row, n = pay
        q = n // 4
        rows = pl.ds(pl.multiple_of(row + first * q, 16), num * q)
        ref = allb.at[b, rows]
        pltpu.make_async_remote_copy(
            src_ref=ref,
            dst_ref=ref,
            send_sem=send_sem.at[p],
            recv_sem=recv_sem.at[p, g],
            device_id={"tp": blk(dz, dy)},
            device_id_type=MESH,
        ).start()

    def take(sem, k, n=N):
        ref = allb.at[pl.ds(0, k), pl.ds(0, n)]
        pltpu.make_async_copy(ref, ref, sem).wait()

    def got(pay, g, k):
        take(recv_sem.at[pay[0], g], k, pay[2])

    def both_y(pay, b, g):
        put(pay, b, 0, 2, 0, 1, g)
        put(pay, b, 0, 2, 0, -1, g)

    def both_z(pay, b, g):
        put(pay, b, 2, 2, 1, 0, g)
        put(pay, b, 2, 2, -1, 0, g)

    def r0(pay):
        put(pay, tp, 0, 2, 1, 0, 0)
        put(pay, tp, 0, 2, -1, 0, 0)
        put(pay, tp, 2, 2, 0, 1, 0)
        put(pay, tp, 2, 2, 0, -1, 0)
        both_y(pay, tp, 2)
        both_z(pay, tp, 2)

    def r1(pay):
        got(pay, 0, 2)
        put(pay, blk(-1, 0), 0, 1, 1, 0, 1)
        put(pay, blk(1, 0), 1, 1, -1, 0, 1)
        put(pay, blk(0, -1), 2, 1, 0, 1, 1)
        put(pay, blk(0, 1), 3, 1, 0, -1, 1)
        for d in (-1, 1):
            both_y(pay, blk(d, 0), 2)
            both_z(pay, blk(0, d), 2)

    def r2(pay):
        got(pay, 1, 1)
        both_y(pay, blk(2, 0), 3)
        both_z(pay, blk(0, 2), 3)

    def onward(pay, d, g):
        put(pay, blk(d, -1), 0, 1, 0, 1, g)
        put(pay, blk(d, 1), 1, 1, 0, -1, g)
        put(pay, blk(-1, d), 2, 1, 1, 0, g)
        put(pay, blk(1, d), 3, 1, -1, 0, g)

    def r3(pay):
        got(pay, 2, 6)
        for d in (0, -1, 1):
            onward(pay, d, 4)

    def r4(pay):
        got(pay, 3, 2)
        onward(pay, 2, 5)

    def r5(pay):
        got(pay, 4, 3)
        got(pay, 5, 1)

    def over_rep(i):
        rows = pl.ds(pl.multiple_of(TOK + CH * i + SH * rep, SH), SH)
        ref = allb.at[pl.ds(0, 16), rows]
        for d in (1, 3, 2):
            pltpu.make_async_remote_copy(
                src_ref=ref,
                dst_ref=ref,
                send_sem=x_send.at[i],
                recv_sem=x_recv.at[i],
                device_id={"rep": (rep + d) % 4},
                device_id_type=MESH,
            ).start()

    NEAR = [(dz, dy) for dz in (0, 1, -1) for dy in (0, 1, -1) if (dz, dy) != (0, 0)]
    FAR = [(2, dy) for dy in (0, 1, -1, 2)] + [(dz, 2) for dz in (0, 1, -1)]

    def to_sibling(p, blocks):
        rows = pl.ds(pl.multiple_of(fs * HALF + N * p, N), N)
        for dz, dy in blocks:
            ref = allb.at[blk(dz, dy), rows]
            pltpu.make_async_remote_copy(
                src_ref=ref,
                dst_ref=ref,
                send_sem=d2d_send.at[p],
                recv_sem=d2d_recv.at[p],
                device_id={"fs": sib},
                device_id_type=MESH,
            ).start()

    def d2d(src, dst, k):
        return pltpu.make_async_remote_copy(
            src_ref=src,
            dst_ref=dst,
            send_sem=r_send.at[k],
            recv_sem=r_recv.at[k],
            device_id={"fs": sib},
            device_id_type=MESH,
        )

    def tile(i):
        slot = i % 2
        r = tile_rows(i)
        for c in loads(i):
            c.wait()

        def sub(k, carry):
            q = pl.multiple_of(k * 32, 32)
            for j in range(NCH):
                g = gbuf[slot, pl.ds(q, 32), j * CH : (j + 1) * CH].astype(F32)
                u = ubuf[slot, pl.ds(q, 32), j * CH : (j + 1) * CH].astype(F32)
                s = 1.0 / (1.0 + jnp.exp(-g))
                a = g * s
                hid[pl.ds(q, 32), j * CH : (j + 1) * CH] = (a * u).astype(BF)
                aa[j, pl.ds(pl.multiple_of(r + q, 32), 32), :] = a.astype(BF)
                cc[j, pl.ds(pl.multiple_of(r + q, 32), 32), :] = (
                    u * s * (1.0 + g * (1.0 - s))
                ).astype(BF)
            return carry

        lax.fori_loop(0, TP // 32, sub, 0)

        @pl.when(i < 8)
        def _():
            for c in loads(i + 2):
                c.start()

        ct = allb[tp, pl.ds(r, TP), :].astype(F32).T.astype(BF)
        dgt[...] += jnp.dot(ct, hid[...], preferred_element_type=F32)

    def transpose_x(i, carry):
        r = pl.multiple_of(i * 128, 128)
        v = xb[pl.ds(r, 128), :].astype(F32)
        xt[:, pl.ds(r, 128)] = v.T.astype(BF)
        return carry

    for c in own_dw:
        c.wait()
    shares = [share(i) for i in range(NXC)]
    for h in shares:
        r0(h)
    own_cot.wait()
    r0(whole(0))
    r0(whole(1))
    cot_pair = d2d(allb.at[tp, pl.ds(mine, HALF)], allb.at[tp, pl.ds(mine, HALF)], 0)
    cot_pair.start()
    own_x.wait()
    x_pair = d2d(xb.at[pl.ds(mine, HALF)], xb.at[pl.ds(mine, HALF)], 1)
    x_pair.start()
    own_gw.wait()
    own_uw.wait()
    dgt[...] = jnp.zeros_like(dgt)
    sqacc[...] = jnp.zeros_like(sqacc)
    tile(0)
    for h in shares:
        r1(h)
    r0(whole(2))
    r1(whole(0))
    tile(1)
    for h in shares:
        r2(h)
    for h in shares:
        r3(h)
    r0(whole(3))
    r1(whole(1))
    cot_pair.wait_recv()
    x_pair.wait_recv()
    lax.fori_loop(0, TOK // 128, transpose_x, 0)
    for h in shares:
        r4(h)
    r0(whole(4))
    tile(2)

    def first(k, carry):
        r2(whole(k))

        @pl.when(k + 2 < NCOT)
        def _():
            r1(whole(k + 2))

        tile(k + 3 + k // 3)

        @pl.when(k == 0)
        def _():
            for i, h in enumerate(shares):
                r5(h)
                over_rep(i)

        r3(whole(k))
        to_sibling(k, NEAR)

        @pl.when(k >= 1)
        def _():
            r4(whole(k - 1))

        @pl.when(k >= 2)
        def _():
            tile(2 * k + 2)
            r5(whole(k - 2))
            to_sibling(k - 2, FAR)

        return carry

    lax.fori_loop(0, NCOT - 1, first, 0)

    def scatter(src, dst, s_sem, r_sem):
        for d in (2, 1, 3):
            peer = (rep + d) % 4
            pltpu.make_async_remote_copy(
                src_ref=src.at[peer],
                dst_ref=dst.at[rep],
                send_sem=s_sem,
                recv_sem=r_sem,
                device_id={"rep": peer},
                device_id_type=MESH,
            ).start()

    def spread(buf, s_sem, r_sem):
        for d in (2, 1, 3):
            pltpu.make_async_remote_copy(
                src_ref=buf.at[rep],
                dst_ref=buf.at[rep],
                send_sem=s_sem,
                recv_sem=r_sem,
                device_id={"rep": (rep + d) % 4},
                device_id_type=MESH,
            ).start()

    def three(buf, sem):
        ref = buf.at[pl.ds(0, 3)]
        pltpu.make_async_copy(ref, ref, sem).wait()

    k = NCOT - 1
    r2(whole(k))
    tile(9)
    r3(whole(k))
    to_sibling(k, NEAR)
    r4(whole(k - 1))
    r0(whole(k + 1))
    r5(whole(k - 2))
    to_sibling(k - 2, FAR)
    r4(whole(k))
    r5(whole(k - 1))
    to_sibling(k - 1, FAR)
    r0(whole(k + 2))
    r1(whole(k + 1))
    r5(whole(k))
    to_sibling(k, FAR)
    r0(whole(k + 3))
    for j in range(4):
        ds[j] = (dgt[32 * j : 32 * j + 32, :] * scale).astype(BF)
    dr[rep] = ds[rep]
    scatter(ds, dr, rs_send.at[NCH], rs_recv.at[NCH])
    take(x_recv.at[0], 12)
    for k in range(NCOT):
        take(d2d_recv.at[k], 15)

    def main_tile(c, j):
        fr = pl.ds(pl.multiple_of(TOK + c * CH, CH), CH)
        for i in range(4):
            rows = pl.ds(j * 2 * TM + i * (TM // 2), TM // 2)
            lhs = jnp.concatenate([allb[k, rows, :] for k in range(16)], axis=1)
            rhs = jnp.concatenate([allb[k, fr, :] for k in range(16)], axis=1)
            hg = lax.dot_general(
                lhs, rhs, (((1,), (1,)), ((), ())), preferred_element_type=F32
            )
            cc[c, rows, :] = (hg * cc[c, rows, :].astype(F32)).astype(BF)
            aa[c, rows, :] = (hg * aa[c, rows, :].astype(F32)).astype(BF)

    def main_grads(c):
        gacc[:, 0:CH] = jnp.dot(xt[...], cc[c], preferred_element_type=F32)
        gacc[:, CH : 2 * CH] = jnp.dot(xt[...], aa[c], preferred_element_type=F32)

    def input_part(start):
        wts = jnp.concatenate([gw[...], uw[...]], axis=1)
        parts = []
        for i in range(2):
            rows = pl.ds(pl.multiple_of(start + i * TM, TM), TM)
            lhs = jnp.concatenate(
                [cc[c, rows, :] for c in range(NCH)] + [aa[c, rows, :] for c in range(NCH)],
                axis=1,
            )
            parts.append(
                lax.dot_general(lhs, wts, (((1,), (1,)), ((), ())), preferred_element_type=F32)
            )
        return parts

    def send_grads(c):
        for j in range(4):
            gs[c, j, 0:32, :] = (gacc[32 * j : 32 * j + 32, 0:CH] * scale).astype(BF)
            gs[c, j, 32:64, :] = (gacc[32 * j : 32 * j + 32, CH : 2 * CH] * scale).astype(BF)
        rs[c, rep] = gs[c, rep]
        scatter(gs.at[c], rs.at[c], rs_send.at[c], rs_recv.at[c])

    def reduce_grads(c):
        three(rs.at[c], rs_recv.at[c])
        v = rs[c, 0].astype(F32) + rs[c, 1].astype(F32)
        v = v + rs[c, 2].astype(F32) + rs[c, 3].astype(F32)
        ag[c, rep] = v.astype(BF)
        w = v * v
        w = w[:, 0:128] + w[:, 128:256]
        sqacc[pl.ds(pl.multiple_of(32 * rep, 32), 32), :] += w[0:32]
        sqacc[pl.ds(pl.multiple_of(128 + 32 * rep, 32), 32), :] += w[32:64]
    def spread_grads(c):
        spread(ag.at[c], ag_send.at[c], ag_recv.at[c])

    def reduce_down():
        three(dr, rs_recv.at[NCH])
        v = dr[0].astype(F32) + dr[1].astype(F32)
        v = v + dr[2].astype(F32) + dr[3].astype(F32)
        dag[rep] = v.astype(BF)
        spread(dag, ag_send.at[NCH], ag_recv.at[NCH])

    def finish_down():
        three(dag, ag_recv.at[NCH])
        for k in range(FH // 128):
            v = jnp.concatenate(
                [dag[j, :, 128 * k : 128 * k + 128].astype(F32) for j in range(4)], axis=0
            )
            dsqs[:, 128 * k : 128 * k + 128] = jnp.sum(v * v, axis=0, keepdims=True)

    def send_down_sq():
        dsqr[tp] = dsqs[...]
        for d in range(1, 16):
            pltpu.make_async_remote_copy(
                src_ref=dsqs,
                dst_ref=dsqr.at[tp],
                send_sem=q_send,
                recv_sem=q_recv,
                device_id={"tp": (tp + d) % 16},
                device_id_type=MESH,
            ).start()

    ig_pair = d2d(igs, igr, 2)

    def chunk(c, carry):
        k = NCOT + c

        @pl.when(c == 1)
        def _():
            take(x_recv.at[1], 12)

        @pl.when(c >= 1)
        def _():
            @pl.when(k - 1 < NPAY)
            def _():
                r4(whole(k - 1))

            @pl.when(k < NPAY)
            def _():
                r2(whole(k))

            @pl.when(k + 1 < NPAY)
            def _():
                r1(whole(k + 1))

        main_tile(c, 0)

        @pl.when(c == 0)
        def _():
            r2(whole(NCOT))
            r1(whole(NCOT + 1))
            r0(whole(NPAY - 1))

        @pl.when((c >= 1) & (k < NPAY))
        def _():
            r3(whole(k))

        @pl.when(c == 2)
        def _():
            reduce_down()

        @pl.when(c == 4)
        def _():
            finish_down()

        main_tile(c, 1)

        @pl.when(c == 0)
        def _():
            r3(whole(NCOT))

        @pl.when(c == 4)
        def _():
            send_down_sq()

        @pl.when(c >= 2)
        def _():
            reduce_grads(c - 2)
            spread_grads(c - 2)

        @pl.when((c >= 1) & (k - 1 < NPAY))
        def _():
            r5(whole(k - 1))

        main_grads(c)
        send_grads(c)
        return carry

    lax.fori_loop(0, NCH, chunk, 0)

    reduce_grads(NCH - 2)
    spread_grads(NCH - 2)
    for i, v in enumerate(input_part(theirs)):
        igs[i * TM : (i + 1) * TM, :] = v.astype(BF)
    reduce_grads(NCH - 1)
    sqs[...] = jnp.sum(sqacc[...].T, axis=0, keepdims=True)
    sqr[rep * 2 + fs] = sqs[...]
    for d in range(1, 8):
        other = {"rep": (rep + d // 2) % 4, "fs": (fs + d) % 2}
        pltpu.make_async_remote_copy(
            src_ref=sqs,
            dst_ref=sqr.at[rep * 2 + fs],
            send_sem=r_send.at[3],
            recv_sem=r_recv.at[3],
            device_id=other,
            device_id_type=MESH,
        ).start()
    spread_grads(NCH - 1)
    ig_pair.start()
    leave = [pltpu.make_async_copy(ag.at[k], ag_hbm.at[k], out_sem.at[k]) for k in range(NCH)]
    leave.append(pltpu.make_async_copy(dag, dag_hbm, out_sem.at[NCH]))
    leave.append(pltpu.make_async_copy(ig_out, ig_hbm, out_sem.at[NCH + 1]))
    leave[NCH].start()
    for k in range(NCH - 2):
        three(ag.at[k], ag_recv.at[k])
        leave[k].start()
    for i, v in enumerate(input_part(mine)):
        ig[i * TM : (i + 1) * TM, :] = v.astype(BF).astype(F32)
    ig_pair.wait_recv()
    ig_out[...] = (ig[...] + igr[...].astype(F32)).astype(BF)
    three(ag.at[NCH - 2], ag_recv.at[NCH - 2])
    leave[NCH - 2].start()
    leave[NCH + 1].start()
    all15 = dsqr.at[pl.ds(0, 15)]
    pltpu.make_async_copy(all15, all15, q_recv).wait()
    total = dsqr[0]
    for k in range(1, 16):
        total = total + dsqr[k]
    dsq_out[...] = total
    leave.append(pltpu.make_async_copy(dsq_out, dsq_hbm, out_sem.at[NCH + 2]))
    leave.append(pltpu.make_async_copy(sq_out, sq_hbm, out_sem.at[NCH + 3]))
    leave[NCH + 2].start()

    for p in range(NPAY):
        take(send_sem.at[p], 15)
    for i in range(NXC):
        take(send_sem.at[NPAY + i], 15, SH)
        take(x_send.at[i], 12)
    for k in range(NCOT):
        take(d2d_send.at[k], 15)
    for k in range(NCH):
        three(gs.at[k], rs_send.at[k])
        three(ag.at[k], ag_send.at[k])
    three(ds, rs_send.at[NCH])
    three(dag, ag_send.at[NCH])
    pltpu.make_async_copy(all15, all15, q_send).wait()
    cot_pair.wait_send()
    x_pair.wait_send()
    ig_pair.wait_send()
    three(ag.at[NCH - 1], ag_recv.at[NCH - 1])
    leave[NCH - 1].start()
    all7 = sqr.at[pl.ds(0, 7)]
    pltpu.make_async_copy(all7, all7, r_send.at[3]).wait()
    pltpu.make_async_copy(all7, all7, r_recv.at[3]).wait()
    total = sqr[0]
    for k in range(1, 8):
        total = total + sqr[k]
    sq_out[...] = total
    leave[NCH + 3].start()
    for c in leave:
        c.wait()


def finish(ig, ag, dag, sq, dsq, ig_out, gg_out, ug_out, dg_out, gsq_out, usq_out, dsq_out):
    ig_out[...] = ig[...]
    for c in range(NCH):
        for j in range(4):
            v = ag[c, j].astype(F32)
            gg_out[32 * j : 32 * j + 32, c * CH : (c + 1) * CH] = v[0:32]
            ug_out[32 * j : 32 * j + 32, c * CH : (c + 1) * CH] = v[32:64]
    for k in range(FH // 128):
        v = jnp.concatenate(
            [dag[j, :, 128 * k : 128 * k + 128].astype(F32) for j in range(4)], axis=0
        )
        dg_out[128 * k : 128 * k + 128, :] = v.T
    gsq_out[...] = sq[0, 0:128]
    usq_out[...] = sq[0, 128:256]
    dsq_out[...] = dsq[0, :]


def on_device(layer_input, cotangent, gate_pre, up_pre, gate_weight, up_weight, down_weight):
    anyspec = pl.BlockSpec(memory_space=pl.ANY)
    vm = pl.BlockSpec(memory_space=pltpu.VMEM)
    dma = pltpu.SemaphoreType.DMA
    outs = pl.pallas_call(
        body,
        out_shape=(
            jax.ShapeDtypeStruct((HALF, 128), BF),
            jax.ShapeDtypeStruct((NCH, 4, 64, CH), BF),
            jax.ShapeDtypeStruct((4, 32, FH), BF),
            jax.ShapeDtypeStruct((1, 256), F32),
            jax.ShapeDtypeStruct((1, FH), F32),
        ),
        in_specs=[anyspec] * 7,
        out_specs=(anyspec,) * 5,
        scratch_shapes=[
            pltpu.VMEM((1, 256), F32),
            pltpu.VMEM((1, FH), F32),
            pltpu.VMEM((HALF, 128), BF),
            pltpu.VMEM((NCH, 4, 64, CH), BF),
            pltpu.VMEM((4, 32, FH), BF),
            dma((NCH + 4,)),
            pltpu.VMEM((16, TOK + FH, 128), BF),
            pltpu.VMEM((NCH, TOK, CH), BF),
            pltpu.VMEM((NCH, TOK, CH), BF),
            pltpu.VMEM((2, TP, FH), BF),
            pltpu.VMEM((2, TP, FH), BF),
            pltpu.VMEM((TP, FH), BF),
            pltpu.VMEM((TOK, 128), BF),
            pltpu.VMEM((128, TOK), BF),
            pltpu.VMEM((128, FH), F32),
            pltpu.VMEM((HALF, 128), F32),
            pltpu.VMEM((128, FH), BF),
            pltpu.VMEM((128, FH), BF),
            pltpu.VMEM((128, 2 * CH), F32),
            pltpu.VMEM((NCH, 4, 64, CH), BF),
            pltpu.VMEM((NCH, 4, 64, CH), BF),
            pltpu.VMEM((4, 32, FH), BF),
            pltpu.VMEM((4, 32, FH), BF),
            pltpu.VMEM((HALF, 128), BF),
            pltpu.VMEM((HALF, 128), BF),
            pltpu.VMEM((256, 128), F32),
            pltpu.VMEM((1, 256), F32),
            pltpu.VMEM((8, 1, 256), F32),
            pltpu.VMEM((1, FH), F32),
            pltpu.VMEM((16, 1, FH), F32),
            dma((NPAY + NXC,)),
            dma((NPAY + NXC, 6)),
            dma((NXC,)),
            dma((NXC,)),
            dma((NCOT,)),
            dma((NCOT,)),
            dma((5 + NXC,)),
            dma((2, 2)),
            dma((NCH + 1,)),
            dma((NCH + 1,)),
            dma((NCH + 1,)),
            dma((NCH + 1,)),
            dma,
            dma,
            dma((4,)),
            dma((4,)),
        ],
        compiler_params=pltpu.CompilerParams(
            collective_id=0, has_side_effects=True, vmem_limit_bytes=64000000
        ),
        name="backward",
    )(layer_input, cotangent, gate_pre, up_pre, gate_weight, up_weight, down_weight)
    return pl.pallas_call(
        finish,
        out_shape=(
            jax.ShapeDtypeStruct((HALF, 128), BF),
            jax.ShapeDtypeStruct((128, FH), F32),
            jax.ShapeDtypeStruct((128, FH), F32),
            jax.ShapeDtypeStruct((FH, 128), F32),
            jax.ShapeDtypeStruct((128,), F32),
            jax.ShapeDtypeStruct((128,), F32),
            jax.ShapeDtypeStruct((FH,), F32),
        ),
        in_specs=[vm] * 5,
        out_specs=(vm,) * 7,
        name="outputs",
    )(*outs)


def solution(mesh):
    return jax.shard_map(
        on_device,
        mesh=mesh,
        in_specs=(
            P(("rep", "fs"), "tp"),
            P(("rep", "fs"), "tp"),
            P("rep", "fs"),
            P("rep", "fs"),
            P("tp", "fs"),
            P("tp", "fs"),
            P("fs", "tp"),
        ),
        out_specs=(
            P(("rep", "fs"), "tp"),
            P("tp", "fs"),
            P("tp", "fs"),
            P("fs", "tp"),
            P("tp"),
            P("tp"),
            P("fs"),
        ),
        check_vma=False,
    )
```

```python
import math

import jax
import jax.numpy as jnp
from jax import lax
from jax.experimental import pallas as pl
from jax.experimental.pallas import tpu as pltpu
from jax.sharding import PartitionSpec as P

MESH = pl.DeviceIdType.MESH
BF = jnp.bfloat16
F32 = jnp.float32

TOK = 2560
HALF = 1280
FH = 1536
N = 256
CH = 256
NCH = FH // CH
NCOT = HALF // N
SH = CH // 4
NXC = 2
NPAY = NCOT + NCH - NXC
TM = 640
TS = 640
TP = 256


def body(
    x_hbm, cot_hbm, gate_hbm, up_hbm, gw_hbm, uw_hbm, dw_hbm,
    ig_hbm, ag_hbm, dag_hbm, sq_hbm, dsq_hbm,
    sq_out, dsq_out, ig_out, ag, dag, out_sem, allb, aa, cc, gbuf, ubuf, hid, xb, xt, dgt, ig, gw, uw,
    gacc, gs, rs, ds, dr, igs, igr, sqacc, sqs, sqr, dsqs, dsqr,
    send_sem, recv_sem, x_send, x_recv, d2d_send, d2d_recv, loc_sem, tile_sem,
    rs_send, rs_recv, ag_send, ag_recv, q_send, q_recv, r_send, r_recv,
):
    rep = lax.axis_index("rep")
    fs = lax.axis_index("fs")
    tp = lax.axis_index("tp")
    z, y = tp // 4, tp % 4
    sib = 1 - fs
    scale = 1.0 / math.sqrt(TOK * 4)

    def blk(dz, dy):
        return ((z + dz) % 4) * 4 + (y + dy) % 4

    mine = pl.multiple_of(fs * HALF, HALF)
    theirs = pl.multiple_of(sib * HALF, HALF)

    own_cot = pltpu.make_async_copy(cot_hbm, allb.at[tp, pl.ds(mine, HALF)], loc_sem.at[0])
    own_rows = [(CH * i + SH * rep, SH, 5 + i) for i in range(NXC)] + [(NXC * CH, FH - NXC * CH, 1)]
    own_dw = [
        pltpu.make_async_copy(
            dw_hbm.at[pl.ds(pl.multiple_of(r, SH), n)],
            allb.at[tp, pl.ds(pl.multiple_of(TOK + r, SH), n)],
            loc_sem.at[k],
        )
        for r, n, k in own_rows
    ]
    own_x = pltpu.make_async_copy(x_hbm, xb.at[pl.ds(mine, HALF)], loc_sem.at[2])
    own_gw = pltpu.make_async_copy(gw_hbm, gw, loc_sem.at[3])
    own_uw = pltpu.make_async_copy(uw_hbm, uw, loc_sem.at[4])
    own_cot.start()
    own_x.start()
    for c in own_dw:
        c.start()

    def tile_rows(i):
        return pl.multiple_of(((fs * 5 + i) % 10) * TP, TP)

    def loads(i):
        slot = i % 2
        r = tile_rows(i)
        return (
            pltpu.make_async_copy(gate_hbm.at[pl.ds(r, TP)], gbuf.at[slot], tile_sem.at[slot, 0]),
            pltpu.make_async_copy(up_hbm.at[pl.ds(r, TP)], ubuf.at[slot], tile_sem.at[slot, 1]),
        )

    for c in loads(0):
        c.start()
    for c in loads(1):
        c.start()
    own_gw.start()
    own_uw.start()

    barrier = pltpu.get_barrier_semaphore()
    for d in ((0, 1), (0, -1), (1, 0), (-1, 0)):
        pl.semaphore_signal(barrier, inc=1, device_id={"tp": blk(*d)}, device_id_type=MESH)
    for d in range(1, 4):
        peer = (rep + d) % 4
        pl.semaphore_signal(barrier, inc=1, device_id={"rep": peer}, device_id_type=MESH)
    pl.semaphore_signal(barrier, inc=1, device_id={"fs": sib}, device_id_type=MESH)
    pl.semaphore_wait(barrier, 8)

    def row0(p):
        w = (p + 11) // 16
        return 256 * p + w * (NXC * CH + HALF) + (1 - w) * fs * HALF

    def whole(p):
        return p, row0(p), N

    def share(i):
        return NPAY + i, TOK + CH * i + SH * rep, SH

    def put(pay, b, first, num, dz, dy, g):
        p, row, n = pay
        q = n // 4
        rows = pl.ds(pl.multiple_of(row + first * q, 16), num * q)
        ref = allb.at[b, rows]
        pltpu.make_async_remote_copy(
            src_ref=ref,
            dst_ref=ref,
            send_sem=send_sem.at[p],
            recv_sem=recv_sem.at[p, g],
            device_id={"tp": blk(dz, dy)},
            device_id_type=MESH,
        ).start()

    def take(sem, k, n=N):
        ref = allb.at[pl.ds(0, k), pl.ds(0, n)]
        pltpu.make_async_copy(ref, ref, sem).wait()

    def got(pay, g, k):
        take(recv_sem.at[pay[0], g], k, pay[2])

    def both_y(pay, b, g):
        put(pay, b, 0, 2, 0, 1, g)
        put(pay, b, 0, 2, 0, -1, g)

    def both_z(pay, b, g):
        put(pay, b, 2, 2, 1, 0, g)
        put(pay, b, 2, 2, -1, 0, g)

    def r0(pay):
        put(pay, tp, 0, 2, 1, 0, 0)
        put(pay, tp, 0, 2, -1, 0, 0)
        put(pay, tp, 2, 2, 0, 1, 0)
        put(pay, tp, 2, 2, 0, -1, 0)
        both_y(pay, tp, 2)
        both_z(pay, tp, 2)

    def r1(pay):
        got(pay, 0, 2)
        put(pay, blk(-1, 0), 0, 1, 1, 0, 1)
        put(pay, blk(1, 0), 1, 1, -1, 0, 1)
        put(pay, blk(0, -1), 2, 1, 0, 1, 1)
        put(pay, blk(0, 1), 3, 1, 0, -1, 1)
        for d in (-1, 1):
            both_y(pay, blk(d, 0), 2)
            both_z(pay, blk(0, d), 2)

    def r2(pay):
        got(pay, 1, 1)
        both_y(pay, blk(2, 0), 3)
        both_z(pay, blk(0, 2), 3)

    def onward(pay, d, g):
        put(pay, blk(d, -1), 0, 1, 0, 1, g)
        put(pay, blk(d, 1), 1, 1, 0, -1, g)
        put(pay, blk(-1, d), 2, 1, 1, 0, g)
        put(pay, blk(1, d), 3, 1, -1, 0, g)

    def r3(pay):
        got(pay, 2, 6)
        for d in (0, -1, 1):
            onward(pay, d, 4)

    def r4(pay):
        got(pay, 3, 2)
        onward(pay, 2, 5)

    def r5(pay):
        got(pay, 4, 3)
        got(pay, 5, 1)

    def over_rep(i):
        rows = pl.ds(pl.multiple_of(TOK + CH * i + SH * rep, SH), SH)
        ref = allb.at[pl.ds(0, 16), rows]
        for d in (1, 3, 2):
            pltpu.make_async_remote_copy(
                src_ref=ref,
                dst_ref=ref,
                send_sem=x_send.at[i],
                recv_sem=x_recv.at[i],
                device_id={"rep": (rep + d) % 4},
                device_id_type=MESH,
            ).start()

    NEAR = [(dz, dy) for dz in (0, 1, -1) for dy in (0, 1, -1) if (dz, dy) != (0, 0)]
    FAR = [(2, dy) for dy in (0, 1, -1, 2)] + [(dz, 2) for dz in (0, 1, -1)]

    def to_sibling(p, blocks):
        rows = pl.ds(pl.multiple_of(fs * HALF + N * p, N), N)
        for dz, dy in blocks:
            ref = allb.at[blk(dz, dy), rows]
            pltpu.make_async_remote_copy(
                src_ref=ref,
                dst_ref=ref,
                send_sem=d2d_send.at[p],
                recv_sem=d2d_recv.at[p],
                device_id={"fs": sib},
                device_id_type=MESH,
            ).start()

    def d2d(src, dst, k):
        return pltpu.make_async_remote_copy(
            src_ref=src,
            dst_ref=dst,
            send_sem=r_send.at[k],
            recv_sem=r_recv.at[k],
            device_id={"fs": sib},
            device_id_type=MESH,
        )

    def tile(i):
        slot = i % 2
        r = tile_rows(i)
        for c in loads(i):
            c.wait()

        def sub(k, carry):
            q = pl.multiple_of(k * 32, 32)
            for j in range(NCH):
                g = gbuf[slot, pl.ds(q, 32), j * CH : (j + 1) * CH].astype(F32)
                u = ubuf[slot, pl.ds(q, 32), j * CH : (j + 1) * CH].astype(F32)
                s = 1.0 / (1.0 + jnp.exp(-g))
                a = g * s
                hid[pl.ds(q, 32), j * CH : (j + 1) * CH] = (a * u).astype(BF)
                aa[j, pl.ds(pl.multiple_of(r + q, 32), 32), :] = a.astype(BF)
                cc[j, pl.ds(pl.multiple_of(r + q, 32), 32), :] = (
                    u * s * (1.0 + g * (1.0 - s))
                ).astype(BF)
            return carry

        lax.fori_loop(0, TP // 32, sub, 0)

        @pl.when(i < 8)
        def _():
            for c in loads(i + 2):
                c.start()

        ct = allb[tp, pl.ds(r, TP), :].astype(F32).T.astype(BF)
        dgt[...] += jnp.dot(ct, hid[...], preferred_element_type=F32)

    def transpose_x(i, carry):
        r = pl.multiple_of(i * 128, 128)
        v = xb[pl.ds(r, 128), :].astype(F32)
        xt[:, pl.ds(r, 128)] = v.T.astype(BF)
        return carry

    for c in own_dw:
        c.wait()
    shares = [share(i) for i in range(NXC)]
    for h in shares:
        r0(h)
    own_cot.wait()
    r0(whole(0))
    r0(whole(1))
    cot_pair = d2d(allb.at[tp, pl.ds(mine, HALF)], allb.at[tp, pl.ds(mine, HALF)], 0)
    cot_pair.start()
    own_x.wait()
    x_pair = d2d(xb.at[pl.ds(mine, HALF)], xb.at[pl.ds(mine, HALF)], 1)
    x_pair.start()
    own_gw.wait()
    own_uw.wait()
    dgt[...] = jnp.zeros_like(dgt)
    sqacc[...] = jnp.zeros_like(sqacc)
    tile(0)
    for h in shares:
        r1(h)
    r0(whole(2))
    r1(whole(0))
    tile(1)
    for h in shares:
        r2(h)
    for h in shares:
        r3(h)
    r0(whole(3))
    r1(whole(1))
    cot_pair.wait_recv()
    x_pair.wait_recv()
    lax.fori_loop(0, TOK // 128, transpose_x, 0)
    for h in shares:
        r4(h)
    r0(whole(4))
    tile(2)

    def first(k, carry):
        r2(whole(k))

        @pl.when(k + 2 < NCOT)
        def _():
            r1(whole(k + 2))

        tile(k + 3 + k // 3)

        @pl.when(k == 0)
        def _():
            for i, h in enumerate(shares):
                r5(h)
                over_rep(i)

        r3(whole(k))
        to_sibling(k, NEAR)

        @pl.when(k >= 1)
        def _():
            r4(whole(k - 1))

        @pl.when(k >= 2)
        def _():
            tile(2 * k + 2)
            r5(whole(k - 2))
            to_sibling(k - 2, FAR)

        return carry

    lax.fori_loop(0, NCOT - 1, first, 0)

    def scatter(src, dst, s_sem, r_sem):
        for d in (2, 1, 3):
            peer = (rep + d) % 4
            pltpu.make_async_remote_copy(
                src_ref=src.at[peer],
                dst_ref=dst.at[rep],
                send_sem=s_sem,
                recv_sem=r_sem,
                device_id={"rep": peer},
                device_id_type=MESH,
            ).start()

    def spread(buf, s_sem, r_sem):
        for d in (2, 1, 3):
            pltpu.make_async_remote_copy(
                src_ref=buf.at[rep],
                dst_ref=buf.at[rep],
                send_sem=s_sem,
                recv_sem=r_sem,
                device_id={"rep": (rep + d) % 4},
                device_id_type=MESH,
            ).start()

    def three(buf, sem):
        ref = buf.at[pl.ds(0, 3)]
        pltpu.make_async_copy(ref, ref, sem).wait()

    k = NCOT - 1
    r2(whole(k))
    tile(9)
    r3(whole(k))
    to_sibling(k, NEAR)
    r0(whole(k + 1))
    r4(whole(k - 1))
    r5(whole(k - 2))
    to_sibling(k - 2, FAR)
    r4(whole(k))
    r1(whole(k + 1))
    r0(whole(k + 2))
    r5(whole(k - 1))
    to_sibling(k - 1, FAR)
    r5(whole(k))
    to_sibling(k, FAR)
    r0(whole(k + 3))
    for j in range(4):
        ds[j] = (dgt[32 * j : 32 * j + 32, :] * scale).astype(BF)
    dr[rep] = ds[rep]
    take(x_recv.at[0], 12)
    for k in range(NCOT):
        take(d2d_recv.at[k], 15)

    def main_tile(c):
        fr = pl.ds(pl.multiple_of(TOK + c * CH, CH), CH)
        for i in range(TOK // TS):
            rows = pl.ds(i * TS, TS)
            lhs = jnp.concatenate([allb[k, rows, :] for k in range(16)], axis=1)
            rhs = jnp.concatenate([allb[k, fr, :] for k in range(16)], axis=1)
            hg = lax.dot_general(
                lhs, rhs, (((1,), (1,)), ((), ())), preferred_element_type=F32
            )
            cc[c, rows, :] = (hg * cc[c, rows, :].astype(F32)).astype(BF)
            aa[c, rows, :] = (hg * aa[c, rows, :].astype(F32)).astype(BF)

    def main_grads(c):
        gacc[:, 0:CH] = jnp.dot(xt[...], cc[c], preferred_element_type=F32)
        gacc[:, CH : 2 * CH] = jnp.dot(xt[...], aa[c], preferred_element_type=F32)

    def input_part(start):
        wts = jnp.concatenate([gw[...], uw[...]], axis=1)
        parts = []
        for i in range(2):
            rows = pl.ds(pl.multiple_of(start + i * TM, TM), TM)
            lhs = jnp.concatenate(
                [cc[c, rows, :] for c in range(NCH)] + [aa[c, rows, :] for c in range(NCH)],
                axis=1,
            )
            parts.append(
                lax.dot_general(lhs, wts, (((1,), (1,)), ((), ())), preferred_element_type=F32)
            )
        return parts

    def send_grads(c):
        for j in range(4):
            gs[c, j, 0:32, :] = (gacc[32 * j : 32 * j + 32, 0:CH] * scale).astype(BF)
            gs[c, j, 32:64, :] = (gacc[32 * j : 32 * j + 32, CH : 2 * CH] * scale).astype(BF)
        rs[c, rep] = gs[c, rep]
        scatter(gs.at[c], rs.at[c], rs_send.at[c], rs_recv.at[c])

    def reduce_grads(c):
        three(rs.at[c], rs_recv.at[c])
        v = rs[c, 0].astype(F32) + rs[c, 1].astype(F32)
        v = v + rs[c, 2].astype(F32) + rs[c, 3].astype(F32)
        ag[c, rep] = v.astype(BF)
        w = v * v
        w = w[:, 0:128] + w[:, 128:256]
        sqacc[pl.ds(pl.multiple_of(32 * rep, 32), 32), :] += w[0:32]
        sqacc[pl.ds(pl.multiple_of(128 + 32 * rep, 32), 32), :] += w[32:64]
    def spread_grads(c):
        spread(ag.at[c], ag_send.at[c], ag_recv.at[c])

    def reduce_down():
        three(dr, rs_recv.at[NCH])
        v = dr[0].astype(F32) + dr[1].astype(F32)
        v = v + dr[2].astype(F32) + dr[3].astype(F32)
        dag[rep] = v.astype(BF)
        spread(dag, ag_send.at[NCH], ag_recv.at[NCH])

    def finish_down():
        three(dag, ag_recv.at[NCH])
        for k in range(FH // 128):
            v = jnp.concatenate(
                [dag[j, :, 128 * k : 128 * k + 128].astype(F32) for j in range(4)], axis=0
            )
            dsqs[:, 128 * k : 128 * k + 128] = jnp.sum(v * v, axis=0, keepdims=True)

    def send_down_sq():
        dsqr[tp] = dsqs[...]
        for d in range(1, 16):
            pltpu.make_async_remote_copy(
                src_ref=dsqs,
                dst_ref=dsqr.at[tp],
                send_sem=q_send,
                recv_sem=q_recv,
                device_id={"tp": (tp + d) % 16},
                device_id_type=MESH,
            ).start()

    ig_pair = d2d(igs, igr, 2)

    def chunk(c, carry):
        k = NCOT + c

        @pl.when(c == 1)
        def _():
            take(x_recv.at[1], 12)
            scatter(ds, dr, rs_send.at[NCH], rs_recv.at[NCH])

        @pl.when((c >= 1) & (k - 1 < NPAY))
        def _():
            r4(whole(k - 1))

        def rounds(turn):
            @pl.when((k < NPAY) & turn)
            def _():
                r2(whole(k))

                @pl.when(k + 1 < NPAY)
                def _():
                    r1(whole(k + 1))

                @pl.when(c == 0)
                def _():
                    r0(whole(NPAY - 1))

        rounds((c >= 1) | (fs == 1))
        main_tile(c)
        rounds((c == 0) & (fs == 0))

        @pl.when(k < NPAY)
        def _():
            r3(whole(k))

        @pl.when(c == 3)
        def _():
            reduce_down()

        @pl.when(c == 5)
        def _():
            finish_down()
            send_down_sq()

        @pl.when(c >= 2)
        def _():
            reduce_grads(c - 2)
            spread_grads(c - 2)

        @pl.when((c >= 1) & (k - 1 < NPAY))
        def _():
            r5(whole(k - 1))

        main_grads(c)
        send_grads(c)
        return carry

    lax.fori_loop(0, NCH, chunk, 0)

    for i, v in enumerate(input_part(theirs)):
        igs[i * TM : (i + 1) * TM, :] = v.astype(BF)
    reduce_grads(NCH - 2)
    spread_grads(NCH - 2)
    ig_pair.start()
    reduce_grads(NCH - 1)
    sqs[...] = jnp.sum(sqacc[...].T, axis=0, keepdims=True)
    sqr[rep * 2 + fs] = sqs[...]
    for d in range(1, 8):
        other = {"rep": (rep + d // 2) % 4, "fs": (fs + d) % 2}
        pltpu.make_async_remote_copy(
            src_ref=sqs,
            dst_ref=sqr.at[rep * 2 + fs],
            send_sem=r_send.at[3],
            recv_sem=r_recv.at[3],
            device_id=other,
            device_id_type=MESH,
        ).start()
    spread_grads(NCH - 1)
    leave = [pltpu.make_async_copy(ag.at[k], ag_hbm.at[k], out_sem.at[k]) for k in range(NCH)]
    leave.append(pltpu.make_async_copy(dag, dag_hbm, out_sem.at[NCH]))
    leave.append(pltpu.make_async_copy(ig_out, ig_hbm, out_sem.at[NCH + 1]))
    leave[NCH].start()
    for k in range(NCH - 2):
        three(ag.at[k], ag_recv.at[k])
        leave[k].start()
    for i, v in enumerate(input_part(mine)):
        ig[i * TM : (i + 1) * TM, :] = v.astype(BF).astype(F32)
    ig_pair.wait_recv()
    ig_out[...] = (ig[...] + igr[...].astype(F32)).astype(BF)
    three(ag.at[NCH - 2], ag_recv.at[NCH - 2])
    leave[NCH - 2].start()
    leave[NCH + 1].start()
    all15 = dsqr.at[pl.ds(0, 15)]
    pltpu.make_async_copy(all15, all15, q_recv).wait()
    total = dsqr[0]
    for k in range(1, 16):
        total = total + dsqr[k]
    dsq_out[...] = total
    leave.append(pltpu.make_async_copy(dsq_out, dsq_hbm, out_sem.at[NCH + 2]))
    leave.append(pltpu.make_async_copy(sq_out, sq_hbm, out_sem.at[NCH + 3]))
    leave[NCH + 2].start()

    for p in range(NPAY):
        take(send_sem.at[p], 15)
    for i in range(NXC):
        take(send_sem.at[NPAY + i], 15, SH)
        take(x_send.at[i], 12)
    for k in range(NCOT):
        take(d2d_send.at[k], 15)
    for k in range(NCH):
        three(gs.at[k], rs_send.at[k])
        three(ag.at[k], ag_send.at[k])
    three(ds, rs_send.at[NCH])
    three(dag, ag_send.at[NCH])
    pltpu.make_async_copy(all15, all15, q_send).wait()
    cot_pair.wait_send()
    x_pair.wait_send()
    ig_pair.wait_send()
    three(ag.at[NCH - 1], ag_recv.at[NCH - 1])
    leave[NCH - 1].start()
    all7 = sqr.at[pl.ds(0, 7)]
    pltpu.make_async_copy(all7, all7, r_send.at[3]).wait()
    pltpu.make_async_copy(all7, all7, r_recv.at[3]).wait()
    total = sqr[0]
    for k in range(1, 8):
        total = total + sqr[k]
    sq_out[...] = total
    leave[NCH + 3].start()
    for c in leave:
        c.wait()


def finish(ig, ag, dag, sq, dsq, ig_out, gg_out, ug_out, dg_out, gsq_out, usq_out, dsq_out):
    ig_out[...] = ig[...]
    for c in range(NCH):
        for j in range(4):
            v = ag[c, j].astype(F32)
            gg_out[32 * j : 32 * j + 32, c * CH : (c + 1) * CH] = v[0:32]
            ug_out[32 * j : 32 * j + 32, c * CH : (c + 1) * CH] = v[32:64]
    for k in range(FH // 128):
        v = jnp.concatenate(
            [dag[j, :, 128 * k : 128 * k + 128].astype(F32) for j in range(4)], axis=0
        )
        dg_out[128 * k : 128 * k + 128, :] = v.T
    gsq_out[...] = sq[0, 0:128]
    usq_out[...] = sq[0, 128:256]
    dsq_out[...] = dsq[0, :]


def on_device(layer_input, cotangent, gate_pre, up_pre, gate_weight, up_weight, down_weight):
    anyspec = pl.BlockSpec(memory_space=pl.ANY)
    vm = pl.BlockSpec(memory_space=pltpu.VMEM)
    dma = pltpu.SemaphoreType.DMA
    outs = pl.pallas_call(
        body,
        out_shape=(
            jax.ShapeDtypeStruct((HALF, 128), BF),
            jax.ShapeDtypeStruct((NCH, 4, 64, CH), BF),
            jax.ShapeDtypeStruct((4, 32, FH), BF),
            jax.ShapeDtypeStruct((1, 256), F32),
            jax.ShapeDtypeStruct((1, FH), F32),
        ),
        in_specs=[anyspec] * 7,
        out_specs=(anyspec,) * 5,
        scratch_shapes=[
            pltpu.VMEM((1, 256), F32),
            pltpu.VMEM((1, FH), F32),
            pltpu.VMEM((HALF, 128), BF),
            pltpu.VMEM((NCH, 4, 64, CH), BF),
            pltpu.VMEM((4, 32, FH), BF),
            dma((NCH + 4,)),
            pltpu.VMEM((16, TOK + FH, 128), BF),
            pltpu.VMEM((NCH, TOK, CH), BF),
            pltpu.VMEM((NCH, TOK, CH), BF),
            pltpu.VMEM((2, TP, FH), BF),
            pltpu.VMEM((2, TP, FH), BF),
            pltpu.VMEM((TP, FH), BF),
            pltpu.VMEM((TOK, 128), BF),
            pltpu.VMEM((128, TOK), BF),
            pltpu.VMEM((128, FH), F32),
            pltpu.VMEM((HALF, 128), F32),
            pltpu.VMEM((128, FH), BF),
            pltpu.VMEM((128, FH), BF),
            pltpu.VMEM((128, 2 * CH), F32),
            pltpu.VMEM((NCH, 4, 64, CH), BF),
            pltpu.VMEM((NCH, 4, 64, CH), BF),
            pltpu.VMEM((4, 32, FH), BF),
            pltpu.VMEM((4, 32, FH), BF),
            pltpu.VMEM((HALF, 128), BF),
            pltpu.VMEM((HALF, 128), BF),
            pltpu.VMEM((256, 128), F32),
            pltpu.VMEM((1, 256), F32),
            pltpu.VMEM((8, 1, 256), F32),
            pltpu.VMEM((1, FH), F32),
            pltpu.VMEM((16, 1, FH), F32),
            dma((NPAY + NXC,)),
            dma((NPAY + NXC, 6)),
            dma((NXC,)),
            dma((NXC,)),
            dma((NCOT,)),
            dma((NCOT,)),
            dma((5 + NXC,)),
            dma((2, 2)),
            dma((NCH + 1,)),
            dma((NCH + 1,)),
            dma((NCH + 1,)),
            dma((NCH + 1,)),
            dma,
            dma,
            dma((4,)),
            dma((4,)),
        ],
        compiler_params=pltpu.CompilerParams(
            collective_id=0, has_side_effects=True, vmem_limit_bytes=64000000
        ),
        name="backward",
    )(layer_input, cotangent, gate_pre, up_pre, gate_weight, up_weight, down_weight)
    return pl.pallas_call(
        finish,
        out_shape=(
            jax.ShapeDtypeStruct((HALF, 128), BF),
            jax.ShapeDtypeStruct((128, FH), F32),
            jax.ShapeDtypeStruct((128, FH), F32),
            jax.ShapeDtypeStruct((FH, 128), F32),
            jax.ShapeDtypeStruct((128,), F32),
            jax.ShapeDtypeStruct((128,), F32),
            jax.ShapeDtypeStruct((FH,), F32),
        ),
        in_specs=[vm] * 5,
        out_specs=(vm,) * 7,
        name="outputs",
    )(*outs)


def solution(mesh):
    return jax.shard_map(
        on_device,
        mesh=mesh,
        in_specs=(
            P(("rep", "fs"), "tp"),
            P(("rep", "fs"), "tp"),
            P("rep", "fs"),
            P("rep", "fs"),
            P("tp", "fs"),
            P("tp", "fs"),
            P("fs", "tp"),
        ),
        out_specs=(
            P(("rep", "fs"), "tp"),
            P("tp", "fs"),
            P("tp", "fs"),
            P("fs", "tp"),
            P("tp"),
            P("tp"),
            P("fs"),
        ),
        check_vma=False,
    )
```

```python
import math

import jax
import jax.numpy as jnp
from jax import lax
from jax.experimental import pallas as pl
from jax.experimental.pallas import tpu as pltpu
from jax.sharding import PartitionSpec as P

MESH = pl.DeviceIdType.MESH
BF = jnp.bfloat16
F32 = jnp.float32

TOK = 2560
HALF = 1280
FH = 1536
N = 256
CH = 256
NCH = FH // CH
NCOT = HALF // N
SH = CH // 4
NXC = 2
NPAY = NCOT + NCH - NXC
TM = 640
TS = 640
TP = 256


def body(
    x_hbm, cot_hbm, gate_hbm, up_hbm, gw_hbm, uw_hbm, dw_hbm,
    ig_hbm, ag_hbm, dag_hbm, sq_hbm, dsq_hbm,
    sq_out, dsq_out, ig_out, ag, dag, out_sem, allb, aa, cc, gbuf, ubuf, hid, xb, xt, dgt, ig, gw, uw,
    gacc, gs, rs, ds, dr, igs, igr, sqacc, sqs, sqr, dsqs, dsqr,
    send_sem, recv_sem, x_send, x_recv, d2d_send, d2d_recv, loc_sem, tile_sem,
    rs_send, rs_recv, ag_send, ag_recv, q_send, q_recv, r_send, r_recv,
):
    rep = lax.axis_index("rep")
    fs = lax.axis_index("fs")
    tp = lax.axis_index("tp")
    z, y = tp // 4, tp % 4
    sib = 1 - fs
    scale = 1.0 / math.sqrt(TOK * 4)

    def blk(dz, dy):
        return ((z + dz) % 4) * 4 + (y + dy) % 4

    mine = pl.multiple_of(fs * HALF, HALF)
    theirs = pl.multiple_of(sib * HALF, HALF)

    own_cot = pltpu.make_async_copy(cot_hbm, allb.at[tp, pl.ds(mine, HALF)], loc_sem.at[0])
    own_rows = [(CH * i + SH * rep, SH, 5 + i) for i in range(NXC)] + [(NXC * CH, FH - NXC * CH, 1)]
    own_dw = [
        pltpu.make_async_copy(
            dw_hbm.at[pl.ds(pl.multiple_of(r, SH), n)],
            allb.at[tp, pl.ds(pl.multiple_of(TOK + r, SH), n)],
            loc_sem.at[k],
        )
        for r, n, k in own_rows
    ]
    own_x = pltpu.make_async_copy(x_hbm, xb.at[pl.ds(mine, HALF)], loc_sem.at[2])
    own_gw = pltpu.make_async_copy(gw_hbm, gw, loc_sem.at[3])
    own_uw = pltpu.make_async_copy(uw_hbm, uw, loc_sem.at[4])
    own_cot.start()
    own_x.start()
    for c in own_dw:
        c.start()

    def tile_rows(i):
        return pl.multiple_of(((fs * 5 + i) % 10) * TP, TP)

    def loads(i):
        slot = i % 2
        r = tile_rows(i)
        return (
            pltpu.make_async_copy(gate_hbm.at[pl.ds(r, TP)], gbuf.at[slot], tile_sem.at[slot, 0]),
            pltpu.make_async_copy(up_hbm.at[pl.ds(r, TP)], ubuf.at[slot], tile_sem.at[slot, 1]),
        )

    for c in loads(0):
        c.start()
    for c in loads(1):
        c.start()
    own_gw.start()
    own_uw.start()

    barrier = pltpu.get_barrier_semaphore()
    for d in ((0, 1), (0, -1), (1, 0), (-1, 0)):
        pl.semaphore_signal(barrier, inc=1, device_id={"tp": blk(*d)}, device_id_type=MESH)
    for d in range(1, 4):
        peer = (rep + d) % 4
        pl.semaphore_signal(barrier, inc=1, device_id={"rep": peer}, device_id_type=MESH)
    pl.semaphore_signal(barrier, inc=1, device_id={"fs": sib}, device_id_type=MESH)
    pl.semaphore_wait(barrier, 8)

    def row0(p):
        w = (p + 11) // 16
        return 256 * p + w * (NXC * CH + HALF) + (1 - w) * fs * HALF

    def whole(p):
        return p, row0(p), N

    def share(i):
        return NPAY + i, TOK + CH * i + SH * rep, SH

    def put(pay, b, first, num, dz, dy, g):
        p, row, n = pay
        q = n // 4
        rows = pl.ds(pl.multiple_of(row + first * q, 16), num * q)
        ref = allb.at[b, rows]
        pltpu.make_async_remote_copy(
            src_ref=ref,
            dst_ref=ref,
            send_sem=send_sem.at[p],
            recv_sem=recv_sem.at[p, g],
            device_id={"tp": blk(dz, dy)},
            device_id_type=MESH,
        ).start()

    def take(sem, k, n=N):
        ref = allb.at[pl.ds(0, k), pl.ds(0, n)]
        pltpu.make_async_copy(ref, ref, sem).wait()

    def got(pay, g, k):
        take(recv_sem.at[pay[0], g], k, pay[2])

    def both_y(pay, b, g):
        put(pay, b, 0, 2, 0, 1, g)
        put(pay, b, 0, 2, 0, -1, g)

    def both_z(pay, b, g):
        put(pay, b, 2, 2, 1, 0, g)
        put(pay, b, 2, 2, -1, 0, g)

    def r0(pay):
        put(pay, tp, 0, 2, 1, 0, 0)
        put(pay, tp, 0, 2, -1, 0, 0)
        put(pay, tp, 2, 2, 0, 1, 0)
        put(pay, tp, 2, 2, 0, -1, 0)
        both_y(pay, tp, 2)
        both_z(pay, tp, 2)

    def r1(pay):
        got(pay, 0, 2)
        put(pay, blk(-1, 0), 0, 1, 1, 0, 1)
        put(pay, blk(1, 0), 1, 1, -1, 0, 1)
        put(pay, blk(0, -1), 2, 1, 0, 1, 1)
        put(pay, blk(0, 1), 3, 1, 0, -1, 1)
        for d in (-1, 1):
            both_y(pay, blk(d, 0), 2)
            both_z(pay, blk(0, d), 2)

    def r2(pay):
        got(pay, 1, 1)
        both_y(pay, blk(2, 0), 3)
        both_z(pay, blk(0, 2), 3)

    def onward(pay, d, g):
        put(pay, blk(d, -1), 0, 1, 0, 1, g)
        put(pay, blk(d, 1), 1, 1, 0, -1, g)
        put(pay, blk(-1, d), 2, 1, 1, 0, g)
        put(pay, blk(1, d), 3, 1, -1, 0, g)

    def r3(pay):
        got(pay, 2, 6)
        for d in (0, -1, 1):
            onward(pay, d, 4)

    def r4(pay):
        got(pay, 3, 2)
        onward(pay, 2, 5)

    def r5(pay):
        got(pay, 4, 3)
        got(pay, 5, 1)

    def over_rep(i):
        rows = pl.ds(pl.multiple_of(TOK + CH * i + SH * rep, SH), SH)
        ref = allb.at[pl.ds(0, 16), rows]
        for d in (1, 3, 2):
            pltpu.make_async_remote_copy(
                src_ref=ref,
                dst_ref=ref,
                send_sem=x_send.at[i],
                recv_sem=x_recv.at[i],
                device_id={"rep": (rep + d) % 4},
                device_id_type=MESH,
            ).start()

    NEAR = [(dz, dy) for dz in (0, 1, -1) for dy in (0, 1, -1) if (dz, dy) != (0, 0)]
    FAR = [(2, dy) for dy in (0, 1, -1, 2)] + [(dz, 2) for dz in (0, 1, -1)]

    def to_sibling(p, blocks):
        rows = pl.ds(pl.multiple_of(fs * HALF + N * p, N), N)
        for dz, dy in blocks:
            ref = allb.at[blk(dz, dy), rows]
            pltpu.make_async_remote_copy(
                src_ref=ref,
                dst_ref=ref,
                send_sem=d2d_send.at[p],
                recv_sem=d2d_recv.at[p],
                device_id={"fs": sib},
                device_id_type=MESH,
            ).start()

    def d2d(src, dst, k):
        return pltpu.make_async_remote_copy(
            src_ref=src,
            dst_ref=dst,
            send_sem=r_send.at[k],
            recv_sem=r_recv.at[k],
            device_id={"fs": sib},
            device_id_type=MESH,
        )

    def tile(i):
        slot = i % 2
        r = tile_rows(i)
        for c in loads(i):
            c.wait()

        def sub(k, carry):
            q = pl.multiple_of(k * 32, 32)
            for j in range(NCH):
                g = gbuf[slot, pl.ds(q, 32), j * CH : (j + 1) * CH].astype(F32)
                u = ubuf[slot, pl.ds(q, 32), j * CH : (j + 1) * CH].astype(F32)
                s = 1.0 / (1.0 + jnp.exp(-g))
                a = g * s
                hid[pl.ds(q, 32), j * CH : (j + 1) * CH] = (a * u).astype(BF)
                aa[j, pl.ds(pl.multiple_of(r + q, 32), 32), :] = a.astype(BF)
                cc[j, pl.ds(pl.multiple_of(r + q, 32), 32), :] = (
                    u * s * (1.0 + g * (1.0 - s))
                ).astype(BF)
            return carry

        lax.fori_loop(0, TP // 32, sub, 0)

        @pl.when(i < 8)
        def _():
            for c in loads(i + 2):
                c.start()

        ct = allb[tp, pl.ds(r, TP), :].astype(F32).T.astype(BF)
        dgt[...] += jnp.dot(ct, hid[...], preferred_element_type=F32)

    def transpose_x(i, carry):
        r = pl.multiple_of(i * 128, 128)
        v = xb[pl.ds(r, 128), :].astype(F32)
        xt[:, pl.ds(r, 128)] = v.T.astype(BF)
        return carry

    for c in own_dw:
        c.wait()
    shares = [share(i) for i in range(NXC)]
    for h in shares:
        r0(h)
    own_cot.wait()
    r0(whole(0))
    r0(whole(1))
    cot_pair = d2d(allb.at[tp, pl.ds(mine, HALF)], allb.at[tp, pl.ds(mine, HALF)], 0)
    cot_pair.start()
    own_x.wait()
    x_pair = d2d(xb.at[pl.ds(mine, HALF)], xb.at[pl.ds(mine, HALF)], 1)
    x_pair.start()
    own_gw.wait()
    own_uw.wait()
    dgt[...] = jnp.zeros_like(dgt)
    sqacc[...] = jnp.zeros_like(sqacc)
    tile(0)
    for h in shares:
        r1(h)
    r0(whole(2))
    r1(whole(0))
    tile(1)
    for h in shares:
        r2(h)
    for h in shares:
        r3(h)
    r0(whole(3))
    r1(whole(1))
    cot_pair.wait_recv()
    x_pair.wait_recv()
    lax.fori_loop(0, TOK // 128, transpose_x, 0)
    for h in shares:
        r4(h)
    r0(whole(4))
    tile(2)

    def first(k, carry):
        r2(whole(k))

        @pl.when(k + 2 < NCOT)
        def _():
            r1(whole(k + 2))

        tile(k + 3 + k // 3)

        @pl.when(k == 0)
        def _():
            for i, h in enumerate(shares):
                r5(h)
                over_rep(i)

        r3(whole(k))
        to_sibling(k, NEAR)

        @pl.when(k >= 1)
        def _():
            r4(whole(k - 1))

        @pl.when(k >= 2)
        def _():
            tile(2 * k + 2)
            r5(whole(k - 2))
            to_sibling(k - 2, FAR)

        return carry

    lax.fori_loop(0, NCOT - 1, first, 0)

    def scatter(src, dst, s_sem, r_sem):
        for d in (2, 1, 3):
            peer = (rep + d) % 4
            pltpu.make_async_remote_copy(
                src_ref=src.at[peer],
                dst_ref=dst.at[rep],
                send_sem=s_sem,
                recv_sem=r_sem,
                device_id={"rep": peer},
                device_id_type=MESH,
            ).start()

    def spread(buf, s_sem, r_sem):
        for d in (2, 1, 3):
            pltpu.make_async_remote_copy(
                src_ref=buf.at[rep],
                dst_ref=buf.at[rep],
                send_sem=s_sem,
                recv_sem=r_sem,
                device_id={"rep": (rep + d) % 4},
                device_id_type=MESH,
            ).start()

    def three(buf, sem):
        ref = buf.at[pl.ds(0, 3)]
        pltpu.make_async_copy(ref, ref, sem).wait()

    k = NCOT - 1
    r2(whole(k))
    tile(9)
    r3(whole(k))
    to_sibling(k, NEAR)
    r0(whole(k + 1))
    r4(whole(k - 1))
    r5(whole(k - 2))
    to_sibling(k - 2, FAR)
    r4(whole(k))
    r1(whole(k + 1))
    r0(whole(k + 2))
    r5(whole(k - 1))
    to_sibling(k - 1, FAR)
    r5(whole(k))
    to_sibling(k, FAR)
    r0(whole(k + 3))
    for j in range(4):
        ds[j] = (dgt[32 * j : 32 * j + 32, :] * scale).astype(BF)
    dr[rep] = ds[rep]
    take(x_recv.at[0], 12)
    for k in range(NCOT):
        take(d2d_recv.at[k], 15)

    def main_tile(c):
        fr = pl.ds(pl.multiple_of(TOK + c * CH, CH), CH)
        for i in range(TOK // TS):
            rows = pl.ds(i * TS, TS)
            lhs = jnp.concatenate([allb[k, rows, :] for k in range(16)], axis=1)
            rhs = jnp.concatenate([allb[k, fr, :] for k in range(16)], axis=1)
            hg = lax.dot_general(
                lhs, rhs, (((1,), (1,)), ((), ())), preferred_element_type=F32
            )
            cc[c, rows, :] = (hg * cc[c, rows, :].astype(F32)).astype(BF)
            aa[c, rows, :] = (hg * aa[c, rows, :].astype(F32)).astype(BF)

    def main_grads(c):
        gacc[:, 0:CH] = jnp.dot(xt[...], cc[c], preferred_element_type=F32)
        gacc[:, CH : 2 * CH] = jnp.dot(xt[...], aa[c], preferred_element_type=F32)

    def input_part(start):
        wts = jnp.concatenate([gw[...], uw[...]], axis=1)
        parts = []
        for i in range(2):
            rows = pl.ds(pl.multiple_of(start + i * TM, TM), TM)
            lhs = jnp.concatenate(
                [cc[c, rows, :] for c in range(NCH)] + [aa[c, rows, :] for c in range(NCH)],
                axis=1,
            )
            parts.append(
                lax.dot_general(lhs, wts, (((1,), (1,)), ((), ())), preferred_element_type=F32)
            )
        return parts

    def send_grads(c):
        for j in range(4):
            gs[c, j, 0:32, :] = (gacc[32 * j : 32 * j + 32, 0:CH] * scale).astype(BF)
            gs[c, j, 32:64, :] = (gacc[32 * j : 32 * j + 32, CH : 2 * CH] * scale).astype(BF)
        rs[c, rep] = gs[c, rep]
        scatter(gs.at[c], rs.at[c], rs_send.at[c], rs_recv.at[c])

    def reduce_grads(c):
        three(rs.at[c], rs_recv.at[c])
        v = rs[c, 0].astype(F32) + rs[c, 1].astype(F32)
        v = v + rs[c, 2].astype(F32) + rs[c, 3].astype(F32)
        ag[c, rep] = v.astype(BF)
        w = v * v
        w = w[:, 0:128] + w[:, 128:256]
        sqacc[pl.ds(pl.multiple_of(32 * rep, 32), 32), :] += w[0:32]
        sqacc[pl.ds(pl.multiple_of(128 + 32 * rep, 32), 32), :] += w[32:64]
    def spread_grads(c):
        spread(ag.at[c], ag_send.at[c], ag_recv.at[c])

    def reduce_down():
        three(dr, rs_recv.at[NCH])
        v = dr[0].astype(F32) + dr[1].astype(F32)
        v = v + dr[2].astype(F32) + dr[3].astype(F32)
        dag[rep] = v.astype(BF)
        spread(dag, ag_send.at[NCH], ag_recv.at[NCH])

    def finish_down():
        three(dag, ag_recv.at[NCH])
        for k in range(FH // 128):
            v = jnp.concatenate(
                [dag[j, :, 128 * k : 128 * k + 128].astype(F32) for j in range(4)], axis=0
            )
            dsqs[:, 128 * k : 128 * k + 128] = jnp.sum(v * v, axis=0, keepdims=True)

    def send_down_sq():
        dsqr[tp] = dsqs[...]
        for d in range(1, 16):
            pltpu.make_async_remote_copy(
                src_ref=dsqs,
                dst_ref=dsqr.at[tp],
                send_sem=q_send,
                recv_sem=q_recv,
                device_id={"tp": (tp + d) % 16},
                device_id_type=MESH,
            ).start()

    ig_pair = d2d(igs, igr, 2)

    def chunk(c, carry):
        k = NCOT + c

        @pl.when(c == 1)
        def _():
            take(x_recv.at[1], 12)
            scatter(ds, dr, rs_send.at[NCH], rs_recv.at[NCH])

        @pl.when((c >= 1) & (k - 1 < NPAY))
        def _():
            r4(whole(k - 1))

        @pl.when(k < NPAY)
        def _():
            r2(whole(k))

        @pl.when(k + 1 < NPAY)
        def _():
            r1(whole(k + 1))

        @pl.when(c == 0)
        def _():
            r0(whole(NPAY - 1))

        main_tile(c)

        @pl.when(k < NPAY)
        def _():
            r3(whole(k))

        @pl.when(c == 3)
        def _():
            reduce_down()

        @pl.when(c == 5)
        def _():
            finish_down()
            send_down_sq()

        @pl.when(c >= 2)
        def _():
            reduce_grads(c - 2)
            spread_grads(c - 2)

        @pl.when((c >= 1) & (k - 1 < NPAY))
        def _():
            r5(whole(k - 1))

        main_grads(c)
        send_grads(c)
        return carry

    lax.fori_loop(0, NCH, chunk, 0)

    for i, v in enumerate(input_part(theirs)):
        igs[i * TM : (i + 1) * TM, :] = v.astype(BF)
    reduce_grads(NCH - 2)
    spread_grads(NCH - 2)
    ig_pair.start()
    reduce_grads(NCH - 1)
    sqs[...] = jnp.sum(sqacc[...].T, axis=0, keepdims=True)
    sqr[rep * 2 + fs] = sqs[...]
    for d in range(1, 8):
        other = {"rep": (rep + d // 2) % 4, "fs": (fs + d) % 2}
        pltpu.make_async_remote_copy(
            src_ref=sqs,
            dst_ref=sqr.at[rep * 2 + fs],
            send_sem=r_send.at[3],
            recv_sem=r_recv.at[3],
            device_id=other,
            device_id_type=MESH,
        ).start()
    spread_grads(NCH - 1)
    leave = [pltpu.make_async_copy(ag.at[k], ag_hbm.at[k], out_sem.at[k]) for k in range(NCH)]
    leave.append(pltpu.make_async_copy(dag, dag_hbm, out_sem.at[NCH]))
    leave.append(pltpu.make_async_copy(ig_out, ig_hbm, out_sem.at[NCH + 1]))
    leave[NCH].start()
    for k in range(NCH - 2):
        three(ag.at[k], ag_recv.at[k])
        leave[k].start()
    for i, v in enumerate(input_part(mine)):
        ig[i * TM : (i + 1) * TM, :] = v.astype(BF).astype(F32)
    ig_pair.wait_recv()
    ig_out[...] = (ig[...] + igr[...].astype(F32)).astype(BF)
    three(ag.at[NCH - 2], ag_recv.at[NCH - 2])
    leave[NCH - 2].start()
    leave[NCH + 1].start()
    all15 = dsqr.at[pl.ds(0, 15)]
    pltpu.make_async_copy(all15, all15, q_recv).wait()
    total = dsqr[0]
    for k in range(1, 16):
        total = total + dsqr[k]
    dsq_out[...] = total
    leave.append(pltpu.make_async_copy(dsq_out, dsq_hbm, out_sem.at[NCH + 2]))
    leave.append(pltpu.make_async_copy(sq_out, sq_hbm, out_sem.at[NCH + 3]))
    leave[NCH + 2].start()

    for p in range(NPAY):
        take(send_sem.at[p], 15)
    for i in range(NXC):
        take(send_sem.at[NPAY + i], 15, SH)
        take(x_send.at[i], 12)
    for k in range(NCOT):
        take(d2d_send.at[k], 15)
    for k in range(NCH):
        three(gs.at[k], rs_send.at[k])
        three(ag.at[k], ag_send.at[k])
    three(ds, rs_send.at[NCH])
    three(dag, ag_send.at[NCH])
    pltpu.make_async_copy(all15, all15, q_send).wait()
    cot_pair.wait_send()
    x_pair.wait_send()
    ig_pair.wait_send()
    three(ag.at[NCH - 1], ag_recv.at[NCH - 1])
    leave[NCH - 1].start()
    all7 = sqr.at[pl.ds(0, 7)]
    pltpu.make_async_copy(all7, all7, r_send.at[3]).wait()
    pltpu.make_async_copy(all7, all7, r_recv.at[3]).wait()
    total = sqr[0]
    for k in range(1, 8):
        total = total + sqr[k]
    sq_out[...] = total
    leave[NCH + 3].start()
    for c in leave:
        c.wait()


def finish(ig, ag, dag, sq, dsq, ig_out, gg_out, ug_out, dg_out, gsq_out, usq_out, dsq_out):
    ig_out[...] = ig[...]
    for c in range(NCH):
        for j in range(4):
            v = ag[c, j].astype(F32)
            gg_out[32 * j : 32 * j + 32, c * CH : (c + 1) * CH] = v[0:32]
            ug_out[32 * j : 32 * j + 32, c * CH : (c + 1) * CH] = v[32:64]
    for k in range(FH // 128):
        v = jnp.concatenate(
            [dag[j, :, 128 * k : 128 * k + 128].astype(F32) for j in range(4)], axis=0
        )
        dg_out[128 * k : 128 * k + 128, :] = v.T
    gsq_out[...] = sq[0, 0:128]
    usq_out[...] = sq[0, 128:256]
    dsq_out[...] = dsq[0, :]


def on_device(layer_input, cotangent, gate_pre, up_pre, gate_weight, up_weight, down_weight):
    anyspec = pl.BlockSpec(memory_space=pl.ANY)
    vm = pl.BlockSpec(memory_space=pltpu.VMEM)
    dma = pltpu.SemaphoreType.DMA
    outs = pl.pallas_call(
        body,
        out_shape=(
            jax.ShapeDtypeStruct((HALF, 128), BF),
            jax.ShapeDtypeStruct((NCH, 4, 64, CH), BF),
            jax.ShapeDtypeStruct((4, 32, FH), BF),
            jax.ShapeDtypeStruct((1, 256), F32),
            jax.ShapeDtypeStruct((1, FH), F32),
        ),
        in_specs=[anyspec] * 7,
        out_specs=(anyspec,) * 5,
        scratch_shapes=[
            pltpu.VMEM((1, 256), F32),
            pltpu.VMEM((1, FH), F32),
            pltpu.VMEM((HALF, 128), BF),
            pltpu.VMEM((NCH, 4, 64, CH), BF),
            pltpu.VMEM((4, 32, FH), BF),
            dma((NCH + 4,)),
            pltpu.VMEM((16, TOK + FH, 128), BF),
            pltpu.VMEM((NCH, TOK, CH), BF),
            pltpu.VMEM((NCH, TOK, CH), BF),
            pltpu.VMEM((2, TP, FH), BF),
            pltpu.VMEM((2, TP, FH), BF),
            pltpu.VMEM((TP, FH), BF),
            pltpu.VMEM((TOK, 128), BF),
            pltpu.VMEM((128, TOK), BF),
            pltpu.VMEM((128, FH), F32),
            pltpu.VMEM((HALF, 128), F32),
            pltpu.VMEM((128, FH), BF),
            pltpu.VMEM((128, FH), BF),
            pltpu.VMEM((128, 2 * CH), F32),
            pltpu.VMEM((NCH, 4, 64, CH), BF),
            pltpu.VMEM((NCH, 4, 64, CH), BF),
            pltpu.VMEM((4, 32, FH), BF),
            pltpu.VMEM((4, 32, FH), BF),
            pltpu.VMEM((HALF, 128), BF),
            pltpu.VMEM((HALF, 128), BF),
            pltpu.VMEM((256, 128), F32),
            pltpu.VMEM((1, 256), F32),
            pltpu.VMEM((8, 1, 256), F32),
            pltpu.VMEM((1, FH), F32),
            pltpu.VMEM((16, 1, FH), F32),
            dma((NPAY + NXC,)),
            dma((NPAY + NXC, 6)),
            dma((NXC,)),
            dma((NXC,)),
            dma((NCOT,)),
            dma((NCOT,)),
            dma((5 + NXC,)),
            dma((2, 2)),
            dma((NCH + 1,)),
            dma((NCH + 1,)),
            dma((NCH + 1,)),
            dma((NCH + 1,)),
            dma,
            dma,
            dma((4,)),
            dma((4,)),
        ],
        compiler_params=pltpu.CompilerParams(
            collective_id=0, has_side_effects=True, vmem_limit_bytes=64000000
        ),
        name="backward",
    )(layer_input, cotangent, gate_pre, up_pre, gate_weight, up_weight, down_weight)
    return pl.pallas_call(
        finish,
        out_shape=(
            jax.ShapeDtypeStruct((HALF, 128), BF),
            jax.ShapeDtypeStruct((128, FH), F32),
            jax.ShapeDtypeStruct((128, FH), F32),
            jax.ShapeDtypeStruct((FH, 128), F32),
            jax.ShapeDtypeStruct((128,), F32),
            jax.ShapeDtypeStruct((128,), F32),
            jax.ShapeDtypeStruct((FH,), F32),
        ),
        in_specs=[vm] * 5,
        out_specs=(vm,) * 7,
        name="outputs",
    )(*outs)


def solution(mesh):
    return jax.shard_map(
        on_device,
        mesh=mesh,
        in_specs=(
            P(("rep", "fs"), "tp"),
            P(("rep", "fs"), "tp"),
            P("rep", "fs"),
            P("rep", "fs"),
            P("tp", "fs"),
            P("tp", "fs"),
            P("fs", "tp"),
        ),
        out_specs=(
            P(("rep", "fs"), "tp"),
            P("tp", "fs"),
            P("tp", "fs"),
            P("fs", "tp"),
            P("tp"),
            P("tp"),
            P("fs"),
        ),
        check_vma=False,
    )
```

```python
import math

import jax
import jax.numpy as jnp
from jax import lax
from jax.experimental import pallas as pl
from jax.experimental.pallas import tpu as pltpu
from jax.sharding import PartitionSpec as P

MESH = pl.DeviceIdType.MESH
BF = jnp.bfloat16
F32 = jnp.float32

TOK = 2560
HALF = 1280
FH = 1536
N = 256
CH = 256
NCH = FH // CH
NCOT = HALF // N
SH = CH // 4
NXC = 2
NPAY = NCOT + NCH - NXC
TM = 640
TS = 640
TP = 256


def body(
    x_hbm, cot_hbm, gate_hbm, up_hbm, gw_hbm, uw_hbm, dw_hbm,
    ig_hbm, ag_hbm, dag_hbm, sq_hbm, dsq_hbm,
    sq_out, dsq_out, ig_out, ag, dag, out_sem, allb, aa, cc, gbuf, ubuf, hid, xb, xt, dgt, ig, gw, uw,
    gacc, gs, rs, ds, dr, igs, igr, sqacc, sqs, sqr, dsqs, dsqr,
    send_sem, recv_sem, x_send, x_recv, d2d_send, d2d_recv, loc_sem, tile_sem,
    rs_send, rs_recv, ag_send, ag_recv, q_send, q_recv, r_send, r_recv,
):
    rep = lax.axis_index("rep")
    fs = lax.axis_index("fs")
    tp = lax.axis_index("tp")
    z, y = tp // 4, tp % 4
    sib = 1 - fs
    scale = 1.0 / math.sqrt(TOK * 4)

    def blk(dz, dy):
        return ((z + dz) % 4) * 4 + (y + dy) % 4

    mine = pl.multiple_of(fs * HALF, HALF)
    theirs = pl.multiple_of(sib * HALF, HALF)

    own_cot = pltpu.make_async_copy(cot_hbm, allb.at[tp, pl.ds(mine, HALF)], loc_sem.at[0])
    own_rows = [(CH * i + SH * rep, SH, 5 + i) for i in range(NXC)] + [(NXC * CH, FH - NXC * CH, 1)]
    own_dw = [
        pltpu.make_async_copy(
            dw_hbm.at[pl.ds(pl.multiple_of(r, SH), n)],
            allb.at[tp, pl.ds(pl.multiple_of(TOK + r, SH), n)],
            loc_sem.at[k],
        )
        for r, n, k in own_rows
    ]
    own_x = pltpu.make_async_copy(x_hbm, xb.at[pl.ds(mine, HALF)], loc_sem.at[2])
    own_gw = pltpu.make_async_copy(gw_hbm, gw, loc_sem.at[3])
    own_uw = pltpu.make_async_copy(uw_hbm, uw, loc_sem.at[4])
    own_cot.start()
    own_x.start()
    for c in own_dw:
        c.start()

    def tile_rows(i):
        return pl.multiple_of(((fs * 5 + i) % 10) * TP, TP)

    def loads(i):
        slot = i % 2
        r = tile_rows(i)
        return (
            pltpu.make_async_copy(gate_hbm.at[pl.ds(r, TP)], gbuf.at[slot], tile_sem.at[slot, 0]),
            pltpu.make_async_copy(up_hbm.at[pl.ds(r, TP)], ubuf.at[slot], tile_sem.at[slot, 1]),
        )

    for c in loads(0):
        c.start()
    for c in loads(1):
        c.start()
    own_gw.start()
    own_uw.start()

    barrier = pltpu.get_barrier_semaphore()
    for d in ((0, 1), (0, -1), (1, 0), (-1, 0)):
        pl.semaphore_signal(barrier, inc=1, device_id={"tp": blk(*d)}, device_id_type=MESH)
    for d in range(1, 4):
        peer = (rep + d) % 4
        pl.semaphore_signal(barrier, inc=1, device_id={"rep": peer}, device_id_type=MESH)
    pl.semaphore_signal(barrier, inc=1, device_id={"fs": sib}, device_id_type=MESH)
    pl.semaphore_wait(barrier, 8)

    def row0(p):
        w = (p + 11) // 16
        return 256 * p + w * (NXC * CH + HALF) + (1 - w) * fs * HALF

    def whole(p):
        return p, row0(p), N

    def share(i):
        return NPAY + i, TOK + CH * i + SH * rep, SH

    def put(pay, b, first, num, dz, dy, g):
        p, row, n = pay
        q = n // 4
        rows = pl.ds(pl.multiple_of(row + first * q, 16), num * q)
        ref = allb.at[b, rows]
        pltpu.make_async_remote_copy(
            src_ref=ref,
            dst_ref=ref,
            send_sem=send_sem.at[p],
            recv_sem=recv_sem.at[p, g],
            device_id={"tp": blk(dz, dy)},
            device_id_type=MESH,
        ).start()

    def take(sem, k, n=N):
        ref = allb.at[pl.ds(0, k), pl.ds(0, n)]
        pltpu.make_async_copy(ref, ref, sem).wait()

    def got(pay, g, k):
        take(recv_sem.at[pay[0], g], k, pay[2])

    def both_y(pay, b, g):
        put(pay, b, 0, 2, 0, 1, g)
        put(pay, b, 0, 2, 0, -1, g)

    def both_z(pay, b, g):
        put(pay, b, 2, 2, 1, 0, g)
        put(pay, b, 2, 2, -1, 0, g)

    def r0(pay):
        put(pay, tp, 0, 2, 1, 0, 0)
        put(pay, tp, 0, 2, -1, 0, 0)
        put(pay, tp, 2, 2, 0, 1, 0)
        put(pay, tp, 2, 2, 0, -1, 0)
        both_y(pay, tp, 2)
        both_z(pay, tp, 2)

    def r1(pay):
        got(pay, 0, 2)
        put(pay, blk(-1, 0), 0, 1, 1, 0, 1)
        put(pay, blk(1, 0), 1, 1, -1, 0, 1)
        put(pay, blk(0, -1), 2, 1, 0, 1, 1)
        put(pay, blk(0, 1), 3, 1, 0, -1, 1)
        for d in (-1, 1):
            both_y(pay, blk(d, 0), 2)
            both_z(pay, blk(0, d), 2)

    def r2(pay):
        got(pay, 1, 1)
        both_y(pay, blk(2, 0), 3)
        both_z(pay, blk(0, 2), 3)

    def onward(pay, d, g):
        put(pay, blk(d, -1), 0, 1, 0, 1, g)
        put(pay, blk(d, 1), 1, 1, 0, -1, g)
        put(pay, blk(-1, d), 2, 1, 1, 0, g)
        put(pay, blk(1, d), 3, 1, -1, 0, g)

    def r3(pay):
        got(pay, 2, 6)
        for d in (0, -1, 1):
            onward(pay, d, 4)

    def r4(pay):
        got(pay, 3, 2)
        onward(pay, 2, 5)

    def r5(pay):
        got(pay, 4, 3)
        got(pay, 5, 1)

    def over_rep(i):
        rows = pl.ds(pl.multiple_of(TOK + CH * i + SH * rep, SH), SH)
        ref = allb.at[pl.ds(0, 16), rows]
        for d in (1, 3, 2):
            pltpu.make_async_remote_copy(
                src_ref=ref,
                dst_ref=ref,
                send_sem=x_send.at[i],
                recv_sem=x_recv.at[i],
                device_id={"rep": (rep + d) % 4},
                device_id_type=MESH,
            ).start()

    NEAR = [(dz, dy) for dz in (0, 1, -1) for dy in (0, 1, -1) if (dz, dy) != (0, 0)]
    FAR = [(2, dy) for dy in (0, 1, -1, 2)] + [(dz, 2) for dz in (0, 1, -1)]

    def to_sibling(p, blocks):
        rows = pl.ds(pl.multiple_of(fs * HALF + N * p, N), N)
        for dz, dy in blocks:
            ref = allb.at[blk(dz, dy), rows]
            pltpu.make_async_remote_copy(
                src_ref=ref,
                dst_ref=ref,
                send_sem=d2d_send.at[p],
                recv_sem=d2d_recv.at[p],
                device_id={"fs": sib},
                device_id_type=MESH,
            ).start()

    def d2d(src, dst, k):
        return pltpu.make_async_remote_copy(
            src_ref=src,
            dst_ref=dst,
            send_sem=r_send.at[k],
            recv_sem=r_recv.at[k],
            device_id={"fs": sib},
            device_id_type=MESH,
        )

    def tile(i):
        slot = i % 2
        r = tile_rows(i)
        for c in loads(i):
            c.wait()

        def sub(k, carry):
            q = pl.multiple_of(k * 32, 32)
            for j in range(NCH):
                g = gbuf[slot, pl.ds(q, 32), j * CH : (j + 1) * CH].astype(F32)
                u = ubuf[slot, pl.ds(q, 32), j * CH : (j + 1) * CH].astype(F32)
                s = 1.0 / (1.0 + jnp.exp(-g))
                a = g * s
                hid[pl.ds(q, 32), j * CH : (j + 1) * CH] = (a * u).astype(BF)
                aa[j, pl.ds(pl.multiple_of(r + q, 32), 32), :] = a.astype(BF)
                cc[j, pl.ds(pl.multiple_of(r + q, 32), 32), :] = (
                    u * s * (1.0 + g * (1.0 - s))
                ).astype(BF)
            return carry

        lax.fori_loop(0, TP // 32, sub, 0)

        @pl.when(i < 8)
        def _():
            for c in loads(i + 2):
                c.start()

        ct = allb[tp, pl.ds(r, TP), :].astype(F32).T.astype(BF)
        dgt[...] += jnp.dot(ct, hid[...], preferred_element_type=F32)

    def transpose_x(i, carry):
        r = pl.multiple_of(i * 128, 128)
        v = xb[pl.ds(r, 128), :].astype(F32)
        xt[:, pl.ds(r, 128)] = v.T.astype(BF)
        return carry

    for c in own_dw:
        c.wait()
    shares = [share(i) for i in range(NXC)]
    for h in shares:
        r0(h)
    own_cot.wait()
    r0(whole(0))
    r0(whole(1))
    cot_pair = d2d(allb.at[tp, pl.ds(mine, HALF)], allb.at[tp, pl.ds(mine, HALF)], 0)
    cot_pair.start()
    own_x.wait()
    x_pair = d2d(xb.at[pl.ds(mine, HALF)], xb.at[pl.ds(mine, HALF)], 1)
    x_pair.start()
    own_gw.wait()
    own_uw.wait()
    dgt[...] = jnp.zeros_like(dgt)
    sqacc[...] = jnp.zeros_like(sqacc)
    tile(0)
    for h in shares:
        r1(h)
    r0(whole(2))
    r1(whole(0))
    tile(1)
    for h in shares:
        r2(h)
    for h in shares:
        r3(h)
    r0(whole(3))
    r1(whole(1))
    cot_pair.wait_recv()
    x_pair.wait_recv()
    lax.fori_loop(0, TOK // 128, transpose_x, 0)
    for h in shares:
        r4(h)
    r0(whole(4))
    tile(2)

    def first(k, carry):
        r2(whole(k))

        @pl.when(k + 2 < NCOT)
        def _():
            r1(whole(k + 2))

        tile(k + 3 + k // 3)

        @pl.when(k == 0)
        def _():
            for i, h in enumerate(shares):
                r5(h)
                over_rep(i)

        r3(whole(k))
        to_sibling(k, NEAR)

        @pl.when(k >= 1)
        def _():
            r4(whole(k - 1))

        @pl.when(k >= 2)
        def _():
            tile(2 * k + 2)
            r5(whole(k - 2))
            to_sibling(k - 2, FAR)

        return carry

    lax.fori_loop(0, NCOT - 1, first, 0)

    def scatter(src, dst, s_sem, r_sem):
        for d in (2, 1, 3):
            peer = (rep + d) % 4
            pltpu.make_async_remote_copy(
                src_ref=src.at[peer],
                dst_ref=dst.at[rep],
                send_sem=s_sem,
                recv_sem=r_sem,
                device_id={"rep": peer},
                device_id_type=MESH,
            ).start()

    def spread(buf, s_sem, r_sem):
        for d in (2, 1, 3):
            pltpu.make_async_remote_copy(
                src_ref=buf.at[rep],
                dst_ref=buf.at[rep],
                send_sem=s_sem,
                recv_sem=r_sem,
                device_id={"rep": (rep + d) % 4},
                device_id_type=MESH,
            ).start()

    def three(buf, sem):
        ref = buf.at[pl.ds(0, 3)]
        pltpu.make_async_copy(ref, ref, sem).wait()

    k = NCOT - 1
    r2(whole(k))
    tile(9)
    r3(whole(k))
    to_sibling(k, NEAR)
    r0(whole(k + 1))
    r4(whole(k - 1))
    r5(whole(k - 2))
    to_sibling(k - 2, FAR)
    r4(whole(k))
    r5(whole(k - 1))
    to_sibling(k - 1, FAR)
    r1(whole(k + 1))
    r0(whole(k + 2))
    r5(whole(k))
    to_sibling(k, FAR)
    r0(whole(k + 3))
    for j in range(4):
        ds[j] = (dgt[32 * j : 32 * j + 32, :] * scale).astype(BF)
    dr[rep] = ds[rep]
    take(x_recv.at[0], 12)
    for k in range(NCOT):
        take(d2d_recv.at[k], 15)

    def main_tile(c):
        fr = pl.ds(pl.multiple_of(TOK + c * CH, CH), CH)
        for i in range(TOK // TS):
            rows = pl.ds(i * TS, TS)
            lhs = jnp.concatenate([allb[k, rows, :] for k in range(16)], axis=1)
            rhs = jnp.concatenate([allb[k, fr, :] for k in range(16)], axis=1)
            hg = lax.dot_general(
                lhs, rhs, (((1,), (1,)), ((), ())), preferred_element_type=F32
            )
            cc[c, rows, :] = (hg * cc[c, rows, :].astype(F32)).astype(BF)
            aa[c, rows, :] = (hg * aa[c, rows, :].astype(F32)).astype(BF)

    def main_grads(c):
        gacc[:, 0:CH] = jnp.dot(xt[...], cc[c], preferred_element_type=F32)
        gacc[:, CH : 2 * CH] = jnp.dot(xt[...], aa[c], preferred_element_type=F32)

    def input_part(start):
        wts = jnp.concatenate([gw[...], uw[...]], axis=1)
        parts = []
        for i in range(2):
            rows = pl.ds(pl.multiple_of(start + i * TM, TM), TM)
            lhs = jnp.concatenate(
                [cc[c, rows, :] for c in range(NCH)] + [aa[c, rows, :] for c in range(NCH)],
                axis=1,
            )
            parts.append(
                lax.dot_general(lhs, wts, (((1,), (1,)), ((), ())), preferred_element_type=F32)
            )
        return parts

    def send_grads(c):
        for j in range(4):
            gs[c, j, 0:32, :] = (gacc[32 * j : 32 * j + 32, 0:CH] * scale).astype(BF)
            gs[c, j, 32:64, :] = (gacc[32 * j : 32 * j + 32, CH : 2 * CH] * scale).astype(BF)
        rs[c, rep] = gs[c, rep]
        scatter(gs.at[c], rs.at[c], rs_send.at[c], rs_recv.at[c])

    def reduce_grads(c):
        three(rs.at[c], rs_recv.at[c])
        v = rs[c, 0].astype(F32) + rs[c, 1].astype(F32)
        v = v + rs[c, 2].astype(F32) + rs[c, 3].astype(F32)
        ag[c, rep] = v.astype(BF)
        w = v * v
        w = w[:, 0:128] + w[:, 128:256]
        sqacc[pl.ds(pl.multiple_of(32 * rep, 32), 32), :] += w[0:32]
        sqacc[pl.ds(pl.multiple_of(128 + 32 * rep, 32), 32), :] += w[32:64]
    def spread_grads(c):
        spread(ag.at[c], ag_send.at[c], ag_recv.at[c])

    def reduce_down():
        three(dr, rs_recv.at[NCH])
        v = dr[0].astype(F32) + dr[1].astype(F32)
        v = v + dr[2].astype(F32) + dr[3].astype(F32)
        dag[rep] = v.astype(BF)
        spread(dag, ag_send.at[NCH], ag_recv.at[NCH])

    def finish_down():
        three(dag, ag_recv.at[NCH])
        for k in range(FH // 128):
            v = jnp.concatenate(
                [dag[j, :, 128 * k : 128 * k + 128].astype(F32) for j in range(4)], axis=0
            )
            dsqs[:, 128 * k : 128 * k + 128] = jnp.sum(v * v, axis=0, keepdims=True)

    def send_down_sq():
        dsqr[tp] = dsqs[...]
        for d in range(1, 16):
            pltpu.make_async_remote_copy(
                src_ref=dsqs,
                dst_ref=dsqr.at[tp],
                send_sem=q_send,
                recv_sem=q_recv,
                device_id={"tp": (tp + d) % 16},
                device_id_type=MESH,
            ).start()

    ig_pair = d2d(igs, igr, 2)

    def chunk(c, carry):
        k = NCOT + c

        @pl.when(c == 1)
        def _():
            take(x_recv.at[1], 12)
            scatter(ds, dr, rs_send.at[NCH], rs_recv.at[NCH])

        @pl.when((c >= 1) & (k - 1 < NPAY))
        def _():
            r4(whole(k - 1))

        @pl.when(k < NPAY)
        def _():
            r2(whole(k))

        @pl.when(k + 1 < NPAY)
        def _():
            r1(whole(k + 1))

        @pl.when(c == 0)
        def _():
            r0(whole(NPAY - 1))

        main_tile(c)

        @pl.when(k < NPAY)
        def _():
            r3(whole(k))

        @pl.when(c == 3)
        def _():
            reduce_down()

        @pl.when(c == 5)
        def _():
            finish_down()
            send_down_sq()

        @pl.when(c >= 2)
        def _():
            reduce_grads(c - 2)
            spread_grads(c - 2)

        @pl.when((c >= 1) & (k - 1 < NPAY))
        def _():
            r5(whole(k - 1))

        main_grads(c)
        send_grads(c)
        return carry

    lax.fori_loop(0, NCH, chunk, 0)

    for i, v in enumerate(input_part(theirs)):
        igs[i * TM : (i + 1) * TM, :] = v.astype(BF)
    reduce_grads(NCH - 2)
    spread_grads(NCH - 2)
    ig_pair.start()
    reduce_grads(NCH - 1)
    sqs[...] = jnp.sum(sqacc[...].T, axis=0, keepdims=True)
    sqr[rep * 2 + fs] = sqs[...]
    for d in range(1, 8):
        other = {"rep": (rep + d // 2) % 4, "fs": (fs + d) % 2}
        pltpu.make_async_remote_copy(
            src_ref=sqs,
            dst_ref=sqr.at[rep * 2 + fs],
            send_sem=r_send.at[3],
            recv_sem=r_recv.at[3],
            device_id=other,
            device_id_type=MESH,
        ).start()
    spread_grads(NCH - 1)
    leave = [pltpu.make_async_copy(ag.at[k], ag_hbm.at[k], out_sem.at[k]) for k in range(NCH)]
    leave.append(pltpu.make_async_copy(dag, dag_hbm, out_sem.at[NCH]))
    leave.append(pltpu.make_async_copy(ig_out, ig_hbm, out_sem.at[NCH + 1]))
    leave[NCH].start()
    for k in range(NCH - 2):
        three(ag.at[k], ag_recv.at[k])
        leave[k].start()
    for i, v in enumerate(input_part(mine)):
        ig[i * TM : (i + 1) * TM, :] = v.astype(BF).astype(F32)
    ig_pair.wait_recv()
    ig_out[...] = (ig[...] + igr[...].astype(F32)).astype(BF)
    three(ag.at[NCH - 2], ag_recv.at[NCH - 2])
    leave[NCH - 2].start()
    leave[NCH + 1].start()
    all15 = dsqr.at[pl.ds(0, 15)]
    pltpu.make_async_copy(all15, all15, q_recv).wait()
    total = dsqr[0]
    for k in range(1, 16):
        total = total + dsqr[k]
    dsq_out[...] = total
    leave.append(pltpu.make_async_copy(dsq_out, dsq_hbm, out_sem.at[NCH + 2]))
    leave.append(pltpu.make_async_copy(sq_out, sq_hbm, out_sem.at[NCH + 3]))
    leave[NCH + 2].start()

    for p in range(NPAY):
        take(send_sem.at[p], 15)
    for i in range(NXC):
        take(send_sem.at[NPAY + i], 15, SH)
        take(x_send.at[i], 12)
    for k in range(NCOT):
        take(d2d_send.at[k], 15)
    for k in range(NCH):
        three(gs.at[k], rs_send.at[k])
        three(ag.at[k], ag_send.at[k])
    three(ds, rs_send.at[NCH])
    three(dag, ag_send.at[NCH])
    pltpu.make_async_copy(all15, all15, q_send).wait()
    cot_pair.wait_send()
    x_pair.wait_send()
    ig_pair.wait_send()
    three(ag.at[NCH - 1], ag_recv.at[NCH - 1])
    leave[NCH - 1].start()
    all7 = sqr.at[pl.ds(0, 7)]
    pltpu.make_async_copy(all7, all7, r_send.at[3]).wait()
    pltpu.make_async_copy(all7, all7, r_recv.at[3]).wait()
    total = sqr[0]
    for k in range(1, 8):
        total = total + sqr[k]
    sq_out[...] = total
    leave[NCH + 3].start()
    for c in leave:
        c.wait()


def finish(ig, ag, dag, sq, dsq, ig_out, gg_out, ug_out, dg_out, gsq_out, usq_out, dsq_out):
    ig_out[...] = ig[...]
    for c in range(NCH):
        for j in range(4):
            v = ag[c, j].astype(F32)
            gg_out[32 * j : 32 * j + 32, c * CH : (c + 1) * CH] = v[0:32]
            ug_out[32 * j : 32 * j + 32, c * CH : (c + 1) * CH] = v[32:64]
    for k in range(FH // 128):
        v = jnp.concatenate(
            [dag[j, :, 128 * k : 128 * k + 128].astype(F32) for j in range(4)], axis=0
        )
        dg_out[128 * k : 128 * k + 128, :] = v.T
    gsq_out[...] = sq[0, 0:128]
    usq_out[...] = sq[0, 128:256]
    dsq_out[...] = dsq[0, :]


def on_device(layer_input, cotangent, gate_pre, up_pre, gate_weight, up_weight, down_weight):
    anyspec = pl.BlockSpec(memory_space=pl.ANY)
    vm = pl.BlockSpec(memory_space=pltpu.VMEM)
    dma = pltpu.SemaphoreType.DMA
    outs = pl.pallas_call(
        body,
        out_shape=(
            jax.ShapeDtypeStruct((HALF, 128), BF),
            jax.ShapeDtypeStruct((NCH, 4, 64, CH), BF),
            jax.ShapeDtypeStruct((4, 32, FH), BF),
            jax.ShapeDtypeStruct((1, 256), F32),
            jax.ShapeDtypeStruct((1, FH), F32),
        ),
        in_specs=[anyspec] * 7,
        out_specs=(anyspec,) * 5,
        scratch_shapes=[
            pltpu.VMEM((1, 256), F32),
            pltpu.VMEM((1, FH), F32),
            pltpu.VMEM((HALF, 128), BF),
            pltpu.VMEM((NCH, 4, 64, CH), BF),
            pltpu.VMEM((4, 32, FH), BF),
            dma((NCH + 4,)),
            pltpu.VMEM((16, TOK + FH, 128), BF),
            pltpu.VMEM((NCH, TOK, CH), BF),
            pltpu.VMEM((NCH, TOK, CH), BF),
            pltpu.VMEM((2, TP, FH), BF),
            pltpu.VMEM((2, TP, FH), BF),
            pltpu.VMEM((TP, FH), BF),
            pltpu.VMEM((TOK, 128), BF),
            pltpu.VMEM((128, TOK), BF),
            pltpu.VMEM((128, FH), F32),
            pltpu.VMEM((HALF, 128), F32),
            pltpu.VMEM((128, FH), BF),
            pltpu.VMEM((128, FH), BF),
            pltpu.VMEM((128, 2 * CH), F32),
            pltpu.VMEM((NCH, 4, 64, CH), BF),
            pltpu.VMEM((NCH, 4, 64, CH), BF),
            pltpu.VMEM((4, 32, FH), BF),
            pltpu.VMEM((4, 32, FH), BF),
            pltpu.VMEM((HALF, 128), BF),
            pltpu.VMEM((HALF, 128), BF),
            pltpu.VMEM((256, 128), F32),
            pltpu.VMEM((1, 256), F32),
            pltpu.VMEM((8, 1, 256), F32),
            pltpu.VMEM((1, FH), F32),
            pltpu.VMEM((16, 1, FH), F32),
            dma((NPAY + NXC,)),
            dma((NPAY + NXC, 6)),
            dma((NXC,)),
            dma((NXC,)),
            dma((NCOT,)),
            dma((NCOT,)),
            dma((5 + NXC,)),
            dma((2, 2)),
            dma((NCH + 1,)),
            dma((NCH + 1,)),
            dma((NCH + 1,)),
            dma((NCH + 1,)),
            dma,
            dma,
            dma((4,)),
            dma((4,)),
        ],
        compiler_params=pltpu.CompilerParams(
            collective_id=0, has_side_effects=True, vmem_limit_bytes=64000000
        ),
        name="backward",
    )(layer_input, cotangent, gate_pre, up_pre, gate_weight, up_weight, down_weight)
    return pl.pallas_call(
        finish,
        out_shape=(
            jax.ShapeDtypeStruct((HALF, 128), BF),
            jax.ShapeDtypeStruct((128, FH), F32),
            jax.ShapeDtypeStruct((128, FH), F32),
            jax.ShapeDtypeStruct((FH, 128), F32),
            jax.ShapeDtypeStruct((128,), F32),
            jax.ShapeDtypeStruct((128,), F32),
            jax.ShapeDtypeStruct((FH,), F32),
        ),
        in_specs=[vm] * 5,
        out_specs=(vm,) * 7,
        name="outputs",
    )(*outs)


def solution(mesh):
    return jax.shard_map(
        on_device,
        mesh=mesh,
        in_specs=(
            P(("rep", "fs"), "tp"),
            P(("rep", "fs"), "tp"),
            P("rep", "fs"),
            P("rep", "fs"),
            P("tp", "fs"),
            P("tp", "fs"),
            P("fs", "tp"),
        ),
        out_specs=(
            P(("rep", "fs"), "tp"),
            P("tp", "fs"),
            P("tp", "fs"),
            P("fs", "tp"),
            P("tp"),
            P("tp"),
            P("fs"),
        ),
        check_vma=False,
    )
```
